256 devices in a mesh: ep: 64 (over z, x, core), tp: 4 (over y).
Axes of the slice: x: 4, y: 4, z: 8, core: 2. Of those that a mesh axis runs over, the one named last changes fastest.
Arguments:
- conv_value: bfloat16 [65536, 1024], P('ep', 'tp'), may hold values from -600 to 600
- conv_gate: bfloat16 [65536, 1024], P('ep', 'tp'), may hold values from -8 to 8
- depth_weight: float32 [31, 1024], replicated, may hold values from -1 to 1
- norm_gain: float32 [1024], replicated, may hold values from 0.1 to 1.9
- norm_shift: float32 [1024], replicated, may hold values from -3 to 3
- conv_out_weight: bfloat16 [1024, 2048], P('tp'), may hold values from -0.1875 to 0.1875
- moe_input: bfloat16 [98304, 2048], P(('ep', 'tp')), may hold values from -6 to 6
- moe_gain: float32 [2048], replicated, may hold values from 0.1 to 1.9
- route_experts: int32 [98304, 2], P(('ep', 'tp')), may hold values from 0 to 63, as said below
- route_scores: float32 [98304, 2], P(('ep', 'tp')), may hold values from -8 to 8
- expert_gate: bfloat16 [64, 2048, 512], P('ep'), may hold values from -0.125 to 0.125
- expert_up: bfloat16 [64, 2048, 512], P('ep'), may hold values from -0.125 to 0.125
- expert_down: bfloat16 [64, 512, 2048], P('ep'), may hold values from -1 to 1
Outputs:
- conv_out: bfloat16 [65536, 2048], P(('ep', 'tp'))
- moe_out: bfloat16 [98304, 2048], P(('ep', 'tp'))
The draws below stay inside these ranges and needn't reach their ends.
Inputs may be any that keep to these rules, and one draw needn't show every extreme that they name: `route_experts`: each row names two different experts that lie in one group of 16 consecutive experts.
All inputs are finite; a program needn't handle non-finite values.
Results may differ from the reference program's by a relative error of at most 0.009.
Values may be sent and summed in bfloat16 or wider, within the bound.
A program may use at most 128 MiB of HBM per device.

```python
import jax
import jax.numpy as jnp
from jax import lax

D = 2048
CONV = 1024
FF = 512
KERNEL = 31
GROUPS = 4
TOP = 2
TOK_B = 384
EXPERTS = 64
GROUP_EXP = 16
CAP = 18
TOKENS_A = 65536
TOKENS_B = 98304
N_EP = 64
N_TP = 4


def draw_conv_value(key, part):
    keys = jax.random.split(jax.random.fold_in(key, 31), 2)
    column_scale = 10.0 ** (jnp.arange(CONV, dtype=jnp.float32) / CONV)
    base = jnp.clip(jax.random.normal(keys[0], (TOKENS_A, CONV), jnp.float32), -4.0, 4.0)
    row_scale = 10.0 ** jax.random.uniform(keys[1], (TOKENS_A, 1), jnp.float32)
    return (base * row_scale * column_scale[None, :]).astype(jnp.bfloat16)


def group_order(key):
    return jax.random.permutation(key, GROUP_EXP)


def draw_route_experts(key, part):
    keys = jax.random.split(jax.random.fold_in(key, 17), 7)
    order_groups = jax.random.permutation(keys[0], GROUPS)
    group_pick = jnp.minimum(jax.random.randint(keys[1], (TOKENS_B,), 0, GROUPS), jax.random.randint(keys[2], (TOKENS_B,), 0, GROUPS))
    group_id = order_groups[group_pick]
    orders = jax.vmap(group_order)(jax.random.split(keys[3], GROUPS))
    first_pick = jnp.minimum(jax.random.randint(keys[4], (TOKENS_B,), 0, GROUP_EXP), jax.random.randint(keys[5], (TOKENS_B,), 0, GROUP_EXP))
    second_pick = (first_pick + 1 + jax.random.randint(keys[6], (TOKENS_B,), 0, GROUP_EXP - 1)) % GROUP_EXP
    first = group_id * GROUP_EXP + orders[group_id, first_pick]
    second = group_id * GROUP_EXP + orders[group_id, second_pick]
    return jnp.stack([first, second], axis=1).astype(jnp.int32)


def shard_levels(rng, dims, shards, smallest, top_value):
    def one(position, shards_of):
        steps = jax.random.uniform(jax.random.fold_in(jax.random.fold_in(rng, 6), position), (shards_of,), jnp.float32, smallest / len(shards), top_value / len(shards))
        return jnp.repeat(jnp.exp(steps), dims[position] // shards_of).reshape((-1,) + (1,) * (len(dims) - position - 1))

    gain = one(*shards[0])
    for cut in shards[1:]:
        gain = gain * one(*cut)
    return gain


def normal_values(key, dims, deviation, reach, cuts=(), kind=jnp.bfloat16):
    result = jax.random.normal(key, dims, jnp.float32) * deviation
    if len(cuts) > 0:
        result = shard_levels(key, dims, cuts, -0.22, 0.18) * result
    return jnp.clip(result, min=-reach, max=reach).astype(kind)


def setup_inputs(seed: int = 0) -> dict:
    arg_keys = jax.random.split(jax.random.key(seed), 14)
    conv_value = draw_conv_value(jax.random.fold_in(arg_keys[13], 71), 0)
    conv_gate = normal_values(arg_keys[1], (TOKENS_A, CONV), 1.5, 8.0, ((0, 64), (1, 4)))
    depth_weight = normal_values(arg_keys[2], (KERNEL, CONV), KERNEL ** -0.5, 1.0, (), jnp.float32)
    norm_gain = jnp.clip(1.0 + 0.18 * jax.random.normal(arg_keys[3], (CONV,), jnp.float32), 0.1, 1.9)
    norm_shift = normal_values(arg_keys[4], (CONV,), 0.5, 3.0, (), jnp.float32)
    conv_out_weight = normal_values(arg_keys[5], (CONV, D), CONV ** -0.5, 0.1875, ((0, 4),))
    moe_input = normal_values(arg_keys[6], (TOKENS_B, D), 1.0, 6.0, ((0, 256),))
    moe_gain = jnp.clip(1.0 + 0.18 * jax.random.normal(arg_keys[7], (D,), jnp.float32), 0.1, 1.9)
    route_experts = draw_route_experts(jax.random.fold_in(arg_keys[13], 71), 0)
    route_scores = normal_values(arg_keys[9], (TOKENS_B, TOP), 1.5, 8.0, ((0, 256),), jnp.float32)
    expert_gate = normal_values(arg_keys[10], (EXPERTS, D, FF), D ** -0.5, 0.125, ((0, 64),))
    expert_up = normal_values(arg_keys[11], (EXPERTS, D, FF), D ** -0.5, 0.125, ((0, 64),))
    expert_down = normal_values(arg_keys[12], (EXPERTS, FF, D), (FF // 16) ** -0.5, 1.0, ((0, 64),))
    return dict(conv_value=conv_value, conv_gate=conv_gate, depth_weight=depth_weight, norm_gain=norm_gain, norm_shift=norm_shift, conv_out_weight=conv_out_weight, moe_input=moe_input, moe_gain=moe_gain, route_experts=route_experts, route_scores=route_scores, expert_gate=expert_gate, expert_up=expert_up, expert_down=expert_down)


def conv_part(conv_value, conv_gate, depth_weight, norm_gain, norm_shift, conv_out_weight):
    gated = (conv_value.astype(jnp.float32) * jax.nn.sigmoid(conv_gate.astype(jnp.float32))).astype(jnp.bfloat16)
    padded = jnp.concatenate([jnp.zeros((KERNEL - 1, CONV), jnp.bfloat16), gated], 0).astype(jnp.float32)
    filtered = jnp.zeros((TOKENS_A, CONV), jnp.float32)
    for offset in range(KERNEL):
        filtered = filtered + depth_weight[offset] * padded[offset:offset + TOKENS_A]
    center = lax.optimization_barrier(jnp.mean(filtered, axis=-1, keepdims=True))
    spread = lax.optimization_barrier(jnp.mean(filtered * filtered, axis=-1, keepdims=True)) - center * center
    normed = (filtered - center) * lax.rsqrt(spread + 1e-05) * norm_gain + norm_shift
    activated = jax.nn.silu(normed).astype(jnp.bfloat16)
    block_width = CONV // N_TP
    summed = jnp.zeros((TOKENS_A, D), jnp.float32)
    for column_block in range(N_TP):
        low = column_block * block_width
        partial_value = jnp.dot(activated[:, low:low + block_width], conv_out_weight[low:low + block_width], preferred_element_type=jnp.float32).astype(jnp.bfloat16)
        summed = summed + partial_value.astype(jnp.float32)
    return summed.astype(jnp.bfloat16)

def moe_part(moe_input, moe_gain, route_experts, route_scores, expert_gate, expert_up, expert_down):
    widened = moe_input.astype(jnp.float32)
    normal_in = (widened * lax.rsqrt(lax.optimization_barrier(jnp.mean(widened * widened, axis=-1, keepdims=True)) + 1e-06) * moe_gain).astype(jnp.bfloat16)
    sources = N_EP * N_TP
    chosen = route_experts.reshape(sources, TOK_B * TOP)
    onehot = (chosen[:, :, None] == jnp.arange(EXPERTS, dtype=jnp.int32)[None, None, :]).astype(jnp.int32)
    slot_rank = lax.optimization_barrier(jnp.sum(jnp.cumsum(onehot, axis=1) * onehot, axis=-1)) - 1
    within_cap = slot_rank < CAP
    source_ids = jnp.arange(sources, dtype=jnp.int32)[:, None]
    token_index = source_ids * TOK_B + jnp.arange(TOK_B * TOP, dtype=jnp.int32)[None, :] // TOP
    per_expert = sources * CAP
    slot_index = jnp.where(within_cap, chosen * per_expert + source_ids * CAP + slot_rank, EXPERTS * per_expert).astype(jnp.int32)
    slot_token = jnp.full((EXPERTS * per_expert,), TOKENS_B, jnp.int32).at[slot_index.reshape(-1)].set(token_index.reshape(-1), mode='drop')
    group_gate = jax.nn.sigmoid(route_scores[:, 0])
    weights = jnp.stack([group_gate * jax.nn.sigmoid(route_scores[:, 1]), group_gate * jax.nn.sigmoid(-route_scores[:, 1])], axis=-1)
    slot_weight = jnp.zeros((EXPERTS * per_expert,), jnp.float32).at[slot_index.reshape(-1)].set(weights.reshape(-1), mode='drop')
    padded_in = jnp.concatenate([normal_in, jnp.zeros((1, D), jnp.bfloat16)], 0)

    def apply_expert(summed, inputs):
        gate_matrix, up_matrix, down_matrix, tokens_here, weight_here = inputs
        picked_rows = padded_in[tokens_here]
        gate_act = jnp.dot(picked_rows, gate_matrix, preferred_element_type=jnp.float32)
        up_act = jnp.dot(picked_rows, up_matrix, preferred_element_type=jnp.float32)
        inner = (jax.nn.silu(gate_act) * up_act).astype(jnp.bfloat16)
        expert_rows = jnp.dot(inner, down_matrix, preferred_element_type=jnp.float32).astype(jnp.bfloat16)
        summed = summed.at[tokens_here].add(weight_here[:, None] * expert_rows.astype(jnp.float32), mode='drop')
        return (summed, None)
    summed, _ = lax.scan(apply_expert, jnp.zeros((TOKENS_B, D), jnp.float32), (expert_gate, expert_up, expert_down, slot_token.reshape(EXPERTS, per_expert), slot_weight.reshape(EXPERTS, per_expert)))
    return summed.astype(jnp.bfloat16)

def reference(conv_value, conv_gate, depth_weight, norm_gain, norm_shift, conv_out_weight, moe_input, moe_gain, route_experts, route_scores, expert_gate, expert_up, expert_down):
    conv_out = conv_part(conv_value, conv_gate, depth_weight, norm_gain, norm_shift, conv_out_weight)
    moe_out = moe_part(moe_input, moe_gain, route_experts, route_scores, expert_gate, expert_up, expert_down)
    return (conv_out, moe_out)
```

```python
import functools

import jax
import jax.numpy as jnp
from jax import lax
from jax.experimental import pallas as pl
from jax.experimental.pallas import tpu as pltpu
from jax.sharding import PartitionSpec as P

CONV = 1024
TOP = 2
MESH = pl.DeviceIdType.MESH
NZ, NX, NC, NY = 8, 4, 2, 4
MAIN = 16
REM = 2
CHUNKS = 24
LAG = 10
OFFSETS = [
    (1, 0), (3, 0), (0, 1), (0, 3), (1, 1), (3, 3), (1, 3), (3, 1),
    (2, 0), (0, 2), (2, 2), (1, 2), (3, 2), (2, 1), (2, 3),
]


def passed_along(x, axis, by):
    peers = lax.axis_size(axis)
    pairs = [(i, i + by) for i in range(peers) if 0 <= i + by < peers]
    return lax.ppermute(x, axis, pairs)


def conv_half(conv_value, conv_gate, depth_weight, norm_gain, norm_shift, conv_out_weight):
    channels = conv_value.shape[1]
    length = conv_value.shape[0]
    first_col = lax.axis_index("tp") * channels
    taps = lax.dynamic_slice_in_dim(depth_weight, first_col, channels, 1)
    gains = lax.dynamic_slice_in_dim(norm_gain, first_col, channels, 0)
    shifts = lax.dynamic_slice_in_dim(norm_shift, first_col, channels, 0)
    gated = (conv_value.astype(jnp.float32) * jax.nn.sigmoid(conv_gate.astype(jnp.float32))).astype(
        jnp.bfloat16
    )
    reach = taps.shape[0] - 1
    earlier = passed_along(gated[length - reach :], "ep", 1)
    padded = jnp.concatenate([earlier, gated], 0).astype(jnp.float32)
    filtered = taps[0] * padded[0:length]
    for offset in range(1, reach + 1):
        filtered = filtered + taps[offset] * padded[offset : offset + length]
    sums, squares = lax.psum(
        (jnp.sum(filtered, axis=1), jnp.sum(filtered * filtered, axis=1)), "tp"
    )
    center = (sums / CONV)[:, None]
    spread = (squares / CONV)[:, None] - center * center
    normed = (filtered - center) * lax.rsqrt(spread + 1e-05) * gains + shifts
    activated = jax.nn.silu(normed).astype(jnp.bfloat16)
    partial_value = jnp.dot(activated, conv_out_weight, preferred_element_type=jnp.float32)
    return lax.psum_scatter(
        partial_value.astype(jnp.bfloat16).astype(jnp.float32).astype(jnp.bfloat16),
        "tp",
        scatter_dimension=0,
        tiled=True,
    )


def slot_of(expert, rank):
    high = expert // 8
    block = ((expert // 2) % 4) * NY + high % 4
    order = (expert % 2) * 2 + high // 4
    main = (block * 64 + order * MAIN).astype(jnp.float32) + rank
    rest = (1024 + block * 8 + order * REM).astype(jnp.float32) + (rank - MAIN)
    return jnp.where(rank < MAIN, main, jnp.where(rank < MAIN + REM, rest, -1.0))


def moe_kernel(
    x_hbm, gain, rt, rc, scores, wg_hbm, wu_hbm, wd_hbm, out,
    w, xn, sm, sr, rm, rr, bm, br, hg, hu, inner, rx, orx, acc,
    xsem, avail, share, foreign, ring_sent, sib_sent,
    d_sent, d_recv, r_sent, r_recv,
):
    f32, bf16 = jnp.float32, jnp.bfloat16
    ep = lax.axis_index("ep")
    y = lax.axis_index("tp")
    z, x, c = ep // 8, (ep // 2) % 4, ep % 2
    me = x * NY + y
    dd = (z - y + 8) % 4
    dist = jnp.where(c == 0, dd, (4 - dd) % 4)
    h_low = ((z - dd - y + 8) % 8) // 4
    hs = jnp.where((c == 0) | (dd == 0), h_low, 1 - h_low)

    def device(zz, xx, cc):
        return (zz * NX + xx) * NC + cc

    along = jnp.where(c == 0, (z + 1) % NZ, (z + NZ - 1) % NZ)
    ring_to = (device(along, x, c), y)
    sibling = (device(z, x, 1 - c), y)

    load_x = pltpu.make_async_copy(x_hbm, xn, xsem)
    load_x.start()

    @pl.when(dist == 0)
    def _():
        for part, ref in enumerate((wg_hbm, wu_hbm)):
            for j in range(8):
                pltpu.make_async_copy(
                    ref.at[0, pl.ds((j // 2) * 512, 512), pl.ds((j % 2) * 256, 256)],
                    w.at[hs, c, part * 8 + j],
                    avail.at[c * CHUNKS + part * 8 + j],
                ).start()
        for j in range(8):
            pltpu.make_async_copy(
                wd_hbm.at[0, :, pl.ds(j * 256, 256)],
                w.at[hs, c, 16 + j],
                avail.at[c * CHUNKS + 16 + j],
            ).start()

    barrier = pltpu.get_barrier_semaphore()
    peers = [(device(z, (x + dx) % NX, c), (y + dy) % NY) for dx, dy in OFFSETS]
    peers += [(device((z + 1) % NZ, x, c), y), (device((z + NZ - 1) % NZ, x, c), y), sibling]
    for peer in peers:
        pl.semaphore_signal(barrier, inc=1, device_id=peer, device_id_type=MESH)
    pl.semaphore_wait(barrier, len(peers))

    def ring_copy(n, sem):
        ref = w.at[hs, n // CHUNKS, n % CHUNKS]
        return pltpu.make_async_remote_copy(
            src_ref=ref, dst_ref=ref, send_sem=ring_sent, recv_sem=sem.at[n],
            device_id=ring_to, device_id_type=MESH,
        )

    def sib_copy(h, n, sem):
        ref = w.at[h, n // CHUNKS, n % CHUNKS]
        return pltpu.make_async_remote_copy(
            src_ref=ref, dst_ref=ref, send_sem=sib_sent, recv_sem=sem.at[n],
            device_id=sibling, device_id_type=MESH,
        )

    def own(n):
        ring_copy(n, avail).wait_recv()

        @pl.when(dist < 3)
        def _():
            ring_copy(n, avail).start()

        @pl.when((dist == 3) & (n % 2 == c))
        def _():
            ring_copy(n, foreign).start()

        @pl.when(dist > 0)
        def _():
            sib_copy(hs, n, share).start()

        @pl.when((dist == 0) & (n // CHUNKS == c))
        def _():
            sib_copy(hs, n, avail).start()

    def outer(n):
        @pl.when((dist == 0) & (n % 2 == c))
        def _():
            ring_copy(n, foreign).wait_recv()
            sib_copy(1 - hs, n, share).start()

    def pump(n):
        if isinstance(n, int):
            if n < 2 * CHUNKS:
                own(n)
            if n >= LAG:
                outer(n - LAG)
            return

        @pl.when(n < 2 * CHUNKS)
        def _():
            own(n)

        @pl.when(n >= LAG)
        def _():
            outer(n - LAG)

    def pumps(low, high):
        def body(n, carry):
            pump(n)
            return carry

        lax.fori_loop(low, high, body, 0)

    pump(0)

    tokens = xn.shape[0]
    first, second = rt[0:1, :], rt[1:2, :]
    ids = lax.broadcasted_iota(jnp.int32, (64, tokens), 0)
    hit0, hit1 = ids == first, ids == second
    both = jnp.where(hit0 | hit1, 1.0, 0.0).astype(bf16)
    row_t = lax.broadcasted_iota(jnp.int32, (tokens, tokens), 0)
    col_t = lax.broadcasted_iota(jnp.int32, (tokens, tokens), 1)
    earlier = jnp.where(row_t < col_t, 1.0, 0.0).astype(bf16)
    counts = jnp.dot(both, earlier, preferred_element_type=f32)
    slot0 = slot_of(first, jnp.sum(jnp.where(hit0, counts, 0.0), axis=0, keepdims=True))
    slot1 = slot_of(second, jnp.sum(jnp.where(hit1, counts, 0.0), axis=0, keepdims=True))
    first_c, second_c = rc[:, 0:1], rc[:, 1:2]
    ids_c = lax.broadcasted_iota(jnp.int32, (tokens, 64), 1)
    hit0_c, hit1_c = ids_c == first_c, ids_c == second_c
    both_c = jnp.where(hit0_c | hit1_c, 1.0, 0.0).astype(bf16)
    earlier_c = jnp.where(row_t > col_t, 1.0, 0.0).astype(bf16)
    counts_c = jnp.dot(earlier_c, both_c, preferred_element_type=f32)
    slot0_c = slot_of(first_c, jnp.sum(jnp.where(hit0_c, counts_c, 0.0), axis=1, keepdims=True))
    slot1_c = slot_of(second_c, jnp.sum(jnp.where(hit1_c, counts_c, 0.0), axis=1, keepdims=True))
    pump(1)

    load_x.wait()

    def norm(b, carry):
        rows = pl.ds(pl.multiple_of(b * 64, 64), 64)
        wide = xn[rows, :].astype(f32)
        square = jnp.mean(wide * wide, axis=-1, keepdims=True)
        xn[rows, :] = (wide * lax.rsqrt(square + 1e-06) * gain[...]).astype(bf16)
        return carry

    for part in range(3):
        lax.fori_loop(part * 2, part * 2 + 2, norm, 0)
        pump(2 + part)

    def picked(base, count):
        at = (lax.broadcasted_iota(jnp.int32, (count, tokens), 0) + base).astype(f32)
        return jnp.where((at == slot0) | (at == slot1), 1.0, 0.0).astype(bf16)

    def gather(g, carry):
        choose = picked(g * 256, 256)

        def cols(q, carry):
            at = pl.ds(pl.multiple_of(q * 512, 512), 512)
            rows = jnp.dot(choose, xn[:, at], preferred_element_type=f32).astype(bf16)
            sm[pl.ds(g * 4, 4), :, at] = rows.reshape(4, 64, 512)
            return carry

        lax.fori_loop(0, 4, cols, 0)
        pump(5 + g)
        return carry

    lax.fori_loop(0, 4, gather, 0)
    choose = picked(1024, 128)

    def gather_rest(q, carry):
        at = pl.ds(pl.multiple_of(q * 512, 512), 512)
        rows = jnp.dot(choose, xn[:, at], preferred_element_type=f32)
        sr[:, :, at] = rows.reshape(16, 8, 512).astype(bf16)
        return carry

    lax.fori_loop(0, 4, gather_rest, 0)

    def block_at(k, sign):
        dx, dy = OFFSETS[k]
        xx, yy = (x + sign * dx + NX) % NX, (y + sign * dy + NY) % NY
        return xx * NY + yy, (device(z, xx, c), yy)

    def dispatch(k, part):
        block, peer = block_at(k, 1)
        if part < 2:
            src, dst = sm.at[block, pl.ds(part * 32, 32)], rm.at[me, pl.ds(part * 32, 32)]
        else:
            src, dst = sr.at[block], rr.at[me]
        return pltpu.make_async_remote_copy(
            src_ref=src, dst_ref=dst, send_sem=d_sent.at[part, k], recv_sem=d_recv.at[part, k],
            device_id=peer, device_id_type=MESH,
        )

    for part in range(3):
        for k in range(15):
            dispatch(k, part).start()
    rm[me] = sm[me]
    rr[me] = sr[me]

    pumps(9, 24)

    for part in range(3):
        for k in range(15):
            dispatch(k, part).wait_recv()
    rx[...] = rr[...].astype(f32).reshape(128, 2048).astype(bf16)
    hg[...] = jnp.zeros_like(hg)
    hu[...] = jnp.zeros_like(hu)

    def rows_of(cc, h, at):
        main = rm[:, cc * 32 + h * MAIN : cc * 32 + (h + 1) * MAIN, at]
        return jnp.concatenate([main.reshape(256, main.shape[2]), rx[:, at]], axis=0)

    order_in_rest = (lax.broadcasted_iota(jnp.int32, (128, 256), 0) % 8) // REM

    def ffn(cc, j):
        n = cc * CHUNKS + j

        @pl.when((dist > 0) | (n % 2 != c))
        def _():
            sib_copy(hs, n, share).wait_recv()

        at_k = pl.ds(pl.multiple_of(((j % 8) // 2) * 512, 512), 512)
        at_n = pl.ds(pl.multiple_of((j % 2) * 256, 256), 256)
        at_o = pl.ds(pl.multiple_of((j % 8) * 256, 256), 256)
        for h in range(2):

            @pl.when(j < 8)
            def _(h=h):
                hg[h, :, at_n] += jnp.dot(
                    rows_of(cc, h, at_k), w[h, cc, j], preferred_element_type=f32
                )

            @pl.when((j >= 8) & (j < 16))
            def _(h=h):
                hu[h, :, at_n] += jnp.dot(
                    rows_of(cc, h, at_k), w[h, cc, j], preferred_element_type=f32
                )

            @pl.when(j == 15)
            def _(h=h):
                gate = hg[h]
                inner[h] = (jax.nn.silu(gate) * hu[h]).astype(bf16)
                hg[h] = jnp.zeros_like(gate)
                hu[h] = jnp.zeros_like(gate)

            @pl.when(j >= 16)
            def _(h=h):
                rows = jnp.dot(inner[h], w[h, cc, j], preferred_element_type=f32)
                rm[:, cc * 32 + h * MAIN : cc * 32 + (h + 1) * MAIN, at_o] = (
                    rows[:256].astype(bf16).reshape(16, MAIN, 256)
                )
                mine = order_in_rest == cc * 2 + h
                orx[:, at_o] = jnp.where(mine, rows[256:], orx[:, at_o])

    def phase0(n, carry):
        pump(n)
        ffn(0, 2 * (n - 24))
        ffn(0, 2 * (n - 24) + 1)
        return carry

    lax.fori_loop(24, 36, phase0, 0)

    def back(k, part):
        block, peer = block_at(k, -1)
        if part < 2:
            src, dst = rm.at[block, pl.ds(part * 32, 32)], bm.at[me, pl.ds(part * 32, 32)]
        else:
            src, dst = rr.at[block], br.at[me]
        return pltpu.make_async_remote_copy(
            src_ref=src, dst_ref=dst, send_sem=r_sent.at[part, k], recv_sem=r_recv.at[part, k],
            device_id=peer, device_id_type=MESH,
        )

    for k in range(15):
        back(k, 0).start()
    bm[me, 0:32] = rm[me, 0:32]

    def phase1(n, carry):
        pump(n)
        j = n - LAG - CHUNKS

        @pl.when(n < 38)
        def _():
            ffn(1, 2 * (n - 36))
            ffn(1, 2 * (n - 36) + 1)

        @pl.when(n >= 38)
        def _():
            ffn(1, j)

        return carry

    lax.fori_loop(36, 2 * CHUNKS + LAG, phase1, 0)

    rr[...] = orx[...].reshape(16, 8, 2048).astype(bf16)
    for part in (1, 2):
        for k in range(15):
            back(k, part).start()
    bm[me, 32:64] = rm[me, 32:64]
    br[me] = rr[me]

    group = jax.nn.sigmoid(scores[:, 0:1])
    weight0 = group * jax.nn.sigmoid(scores[:, 1:2])
    weight1 = group * jax.nn.sigmoid(-scores[:, 1:2])

    def chosen(slot, cc):
        at = lax.broadcasted_iota(jnp.int32, (tokens, 512), 1)
        main = ((at // 32) * 64 + cc * 32 + at % 32).astype(f32)
        hits = jnp.where(main == slot, 1.0, 0.0).astype(bf16)
        if cc == 0:
            return hits
        rest = (lax.broadcasted_iota(jnp.int32, (tokens, 128), 1) + 1024).astype(f32)
        return jnp.concatenate([hits, jnp.where(rest == slot, 1.0, 0.0).astype(bf16)], axis=1)

    for k in range(15):
        back(k, 0).wait_recv()
    pick0, pick1 = chosen(slot0_c, 0), chosen(slot1_c, 0)

    def combine0(q, carry):
        at = pl.ds(pl.multiple_of(q * 512, 512), 512)
        rows = bm[:, 0:32, at].reshape(512, 512)
        acc[:, at] = weight0 * jnp.dot(
            pick0, rows, preferred_element_type=f32
        ) + weight1 * jnp.dot(pick1, rows, preferred_element_type=f32)
        return carry

    lax.fori_loop(0, 4, combine0, 0)

    for part in (1, 2):
        for k in range(15):
            back(k, part).wait_recv()
    pick0b, pick1b = chosen(slot0_c, 1), chosen(slot1_c, 1)

    def combine1(q, carry):
        at = pl.ds(pl.multiple_of(q * 512, 512), 512)
        rest = br[:, :, at].astype(f32).reshape(128, 512).astype(bf16)
        rows = jnp.concatenate([bm[:, 32:64, at].reshape(512, 512), rest], axis=0)
        total = acc[:, at] + (
            weight0 * jnp.dot(pick0b, rows, preferred_element_type=f32)
            + weight1 * jnp.dot(pick1b, rows, preferred_element_type=f32)
        )
        out[:, at] = total.astype(bf16)
        return carry

    lax.fori_loop(0, 4, combine1, 0)

    for part in range(3):
        for k in range(15):
            dispatch(k, part).wait_send()
            back(k, part).wait_send()

    def sent(n, carry):
        @pl.when((dist < 3) | (n % 2 == c))
        def _():
            ring_copy(n, avail).wait_send()

        sib_copy(hs, n, share).wait_send()
        return carry

    lax.fori_loop(0, 2 * CHUNKS, sent, 0)


def moe_half(moe_input, moe_gain, route_experts, route_scores, expert_gate, expert_up, expert_down):
    bf16, f32 = jnp.bfloat16, jnp.float32
    rows, width = moe_input.shape
    hbm = pl.BlockSpec(memory_space=pl.ANY)
    vmem = pl.BlockSpec(memory_space=pltpu.VMEM)
    dma = pltpu.SemaphoreType.DMA
    return pl.pallas_call(
        moe_kernel,
        out_shape=jax.ShapeDtypeStruct((rows, width), bf16),
        in_specs=[hbm, vmem, vmem, vmem, vmem, hbm, hbm, hbm],
        out_specs=vmem,
        scratch_shapes=[
            pltpu.VMEM((2, 2, CHUNKS, 512, 256), bf16),
            pltpu.VMEM((rows, width), bf16),
            pltpu.VMEM((16, 64, width), bf16),
            pltpu.VMEM((16, 8, width), bf16),
            pltpu.VMEM((16, 64, width), bf16),
            pltpu.VMEM((16, 8, width), bf16),
            pltpu.VMEM((16, 64, width), bf16),
            pltpu.VMEM((16, 8, width), bf16),
            pltpu.VMEM((2, 384, 512), f32),
            pltpu.VMEM((2, 384, 512), f32),
            pltpu.VMEM((2, 384, 512), bf16),
            pltpu.VMEM((128, width), bf16),
            pltpu.VMEM((128, width), f32),
            pltpu.VMEM((rows, width), f32),
            dma,
            dma((2 * CHUNKS,)),
            dma((2 * CHUNKS,)),
            dma((2 * CHUNKS,)),
            dma,
            dma,
            dma((3, 15)),
            dma((3, 15)),
            dma((3, 15)),
            dma((3, 15)),
        ],
        compiler_params=pltpu.CompilerParams(
            collective_id=0, has_side_effects=True, vmem_limit_bytes=66_000_000
        ),
        name="experts",
    )(
        moe_input,
        moe_gain.reshape(1, width),
        route_experts.T,
        route_experts,
        route_scores,
        expert_gate,
        expert_up,
        expert_down,
    )


def on_device(
    conv_value,
    conv_gate,
    depth_weight,
    norm_gain,
    norm_shift,
    conv_out_weight,
    moe_input,
    moe_gain,
    route_experts,
    route_scores,
    expert_gate,
    expert_up,
    expert_down,
):
    conv_out = conv_half(
        conv_value, conv_gate, depth_weight, norm_gain, norm_shift, conv_out_weight
    )
    moe_out = moe_half(
        moe_input, moe_gain, route_experts, route_scores, expert_gate, expert_up, expert_down
    )
    return (conv_out, moe_out)


def solution(mesh):
    in_specs = (
        P("ep", "tp"),
        P("ep", "tp"),
        P(),
        P(),
        P(),
        P("tp", None),
        P(("ep", "tp"), None),
        P(),
        P(("ep", "tp"), None),
        P(("ep", "tp"), None),
        P("ep", None, None),
        P("ep", None, None),
        P("ep", None, None),
    )
    out_specs = (P(("ep", "tp"), None), P(("ep", "tp"), None))
    return jax.shard_map(
        on_device, mesh=mesh, in_specs=in_specs, out_specs=out_specs, check_vma=False
    )
```

```python
import jax
import jax.numpy as jnp
from jax import lax
from jax.experimental import pallas as pl
from jax.experimental.pallas import tpu as pltpu
from jax.sharding import PartitionSpec as P

MESH = pl.DeviceIdType.MESH
NZ, NX, NC, NY = 8, 4, 2, 4
CONV = 1024
KERNEL = 31
HALO = 32
MAIN = 16
REM = 2
CHUNKS = 24
TOTAL = 2 * CHUNKS
HOP = 2
FAR = 4 * HOP + 1
START = 28
OFFSETS = [
    (1, 0), (3, 0), (0, 1), (0, 3), (1, 1), (3, 3), (1, 3), (3, 1),
    (2, 0), (0, 2), (2, 2), (1, 2), (3, 2), (2, 1), (2, 3),
]


def slot_of(expert, rank):
    high = expert // 8
    block = ((expert // 2) % 4) * NY + high % 4
    order = (expert % 2) * 2 + high // 4
    main = (block * 64 + order * MAIN).astype(jnp.float32) + rank
    rest = (1024 + block * 8 + order * REM).astype(jnp.float32) + (rank - MAIN)
    return jnp.where(rank < MAIN, main, jnp.where(rank < MAIN + REM, rest, -1.0))


def eye(n):
    return lax.broadcasted_iota(jnp.int32, (n, n), 0) == lax.broadcasted_iota(jnp.int32, (n, n), 1)


def to_column(row, n):
    pieces = []
    for at in range(0, n, 128):
        spread = jnp.where(eye(128), row[:, at : at + 128], 0.0)
        pieces.append(jnp.sum(spread, axis=1, keepdims=True))
    return pieces[0] if len(pieces) == 1 else jnp.concatenate(pieces, axis=0)


def to_row(column):
    return jnp.sum(jnp.where(eye(128), column, 0.0), axis=0, keepdims=True)


def kernel(
    value_hbm, gate_hbm, taps_hbm, gain_c, shift_c, cw_hbm,
    x_hbm, gain, table, wg_hbm, wu_hbm, wd_hbm,
    conv_out, out,
    w, xn, sm, sr, rm, rr, bm, br, hg, hu, inner, rx, orx, acc,
    val, gat, taps, pad, filt, act, acts, cw, window, halo_out, halo_in, stat, stats,
    load, avail, share, foreign, ring_sent, sib_sent,
    d_sent, d_recv, r_sent, r_recv, q_sent, q_recv,
    halo_sem, stat_sent, stat_recv, act_sent, act_recv, cw_sent, cw_recv, cs_sent, cs_recv,
):
    f32, bf16 = jnp.float32, jnp.bfloat16
    ep = lax.axis_index("ep")
    y = lax.axis_index("tp")
    z, x, c = ep // 8, (ep // 2) % 4, ep % 2
    me = x * NY + y
    dd = (z - y + 8) % 4
    dist = jnp.where(c == 0, dd, (4 - dd) % 4)
    h_low = ((z - dd - y + 8) % 8) // 4
    hs = jnp.where((c == 0) | (dd == 0), h_low, 1 - h_low)

    def device(zz, xx, cc):
        return (zz * NX + xx) * NC + cc

    along = jnp.where(c == 0, (z + 1) % NZ, (z + NZ - 1) % NZ)
    ring_to = (device(along, x, c), y)
    sibling = (device(z, x, 1 - c), y)
    my_cols = pl.ds(pl.multiple_of(y * 256, 256), 256)

    loads = [
        pltpu.make_async_copy(value_hbm, val, load.at[0]),
        pltpu.make_async_copy(gate_hbm, gat, load.at[1]),
        pltpu.make_async_copy(x_hbm, xn, load.at[2]),
        pltpu.make_async_copy(taps_hbm.at[:, my_cols], taps, load.at[3]),
        pltpu.make_async_copy(cw_hbm, cw.at[y], load.at[4]),
    ]

    @pl.when(dist == 0)
    def _():
        for part, ref in enumerate((wg_hbm, wu_hbm)):
            for j in range(8):
                pltpu.make_async_copy(
                    ref.at[0, pl.ds((j // 2) * 512, 512), pl.ds((j % 2) * 256, 256)],
                    w.at[hs, c, part * 8 + j],
                    avail.at[c * CHUNKS + part * 8 + j],
                ).start()
        for j in range(8):
            pltpu.make_async_copy(
                wd_hbm.at[0, :, pl.ds(j * 256, 256)],
                w.at[hs, c, 16 + j],
                avail.at[c * CHUNKS + 16 + j],
            ).start()

    for copy in loads:
        copy.start()

    with jax.named_scope("s_barrier"):
        barrier = pltpu.get_barrier_semaphore()
        peers = [(device(z, (x + dx) % NX, c), (y + dy) % NY) for dx, dy in OFFSETS]
        peers += [(device((z + 1) % NZ, x, c), y), (device((z + NZ - 1) % NZ, x, c), y), sibling]
        peers += [((ep + 1) % 64, y), ((ep + 63) % 64, y)]
        for peer in peers:
            pl.semaphore_signal(barrier, inc=1, device_id=peer, device_id_type=MESH)
        pl.semaphore_wait(barrier, len(peers))

    def ring_copy(n, sem):
        ref = w.at[hs, n // CHUNKS, n % CHUNKS]
        return pltpu.make_async_remote_copy(
            src_ref=ref, dst_ref=ref, send_sem=ring_sent, recv_sem=sem.at[n],
            device_id=ring_to, device_id_type=MESH,
        )

    def sib_copy(h, n, sem):
        ref = w.at[h, n // CHUNKS, n % CHUNKS]
        return pltpu.make_async_remote_copy(
            src_ref=ref, dst_ref=ref, send_sem=sib_sent, recv_sem=sem.at[n],
            device_id=sibling, device_id_type=MESH,
        )

    def own(n):
        ring_copy(n, avail).wait_recv()

        @pl.when(dist < 3)
        def _():
            ring_copy(n, avail).start()

        @pl.when((dist == 3) & (n % 2 == c))
        def _():
            ring_copy(n, foreign).start()

        @pl.when(dist > 0)
        def _():
            sib_copy(hs, n, share).start()

        @pl.when((dist == 0) & (n // CHUNKS == c))
        def _():
            sib_copy(hs, n, avail).start()

    def step(p):
        n = p - HOP * dist
        m = p - FAR

        @pl.when((n >= 0) & (n < TOTAL))
        def _():
            own(n)

        @pl.when((dist == 0) & (m >= 0) & (m < TOTAL) & (m % 2 == c))
        def _():
            ring_copy(m, foreign).wait_recv()
            sib_copy(1 - hs, m, share).start()

    step(0)

    with jax.named_scope("s_gated"):
        loads[0].wait()
        loads[1].wait()

        def gated(b, carry):
            rows = pl.ds(pl.multiple_of(b * 128, 128), 128)
            wide = val[rows, :].astype(f32) * jax.nn.sigmoid(gat[rows, :].astype(f32))
            pad[pl.ds(pl.multiple_of(HALO + b * 128, 32), 128), :] = wide.astype(bf16).astype(f32)
            return carry

        lax.fori_loop(0, 8, gated, 0)
        halo_out[...] = pad[1024 : 1024 + HALO, :].astype(bf16)
        halo = pltpu.make_async_remote_copy(
            src_ref=halo_out, dst_ref=halo_in, send_sem=halo_sem.at[0], recv_sem=halo_sem.at[1],
            device_id=((ep + 1) % 64, y), device_id_type=MESH,
        )
        halo.start()

    step(1)

    with jax.named_scope("s_route"):
        tokens = xn.shape[0]
        first, second = table[0:1, :].astype(jnp.int32), table[1:2, :].astype(jnp.int32)
        ids = lax.broadcasted_iota(jnp.int32, (64, tokens), 0)
        hit0, hit1 = ids == first, ids == second
        both = jnp.where(hit0 | hit1, 1.0, 0.0).astype(bf16)
        row_t = lax.broadcasted_iota(jnp.int32, (tokens, tokens), 0)
        col_t = lax.broadcasted_iota(jnp.int32, (tokens, tokens), 1)
        earlier = jnp.where(row_t < col_t, 1.0, 0.0).astype(bf16)
        counts = jnp.dot(both, earlier, preferred_element_type=f32)
        slot0 = slot_of(first, jnp.sum(jnp.where(hit0, counts, 0.0), axis=0, keepdims=True))
        slot1 = slot_of(second, jnp.sum(jnp.where(hit1, counts, 0.0), axis=0, keepdims=True))

    with jax.named_scope("s_norm"):
        loads[2].wait()

        def norm(b, carry):
            rows = pl.ds(pl.multiple_of(b * 64, 64), 64)
            wide = xn[rows, :].astype(f32)
            square = jnp.mean(wide * wide, axis=-1, keepdims=True)
            xn[rows, :] = (wide * lax.rsqrt(square + 1e-06) * gain[...]).astype(bf16)
            return carry

        lax.fori_loop(0, 6, norm, 0)
    step(2)

    def picked(base, count):
        at = (lax.broadcasted_iota(jnp.int32, (count, tokens), 0) + base).astype(f32)
        return jnp.where((at == slot0) | (at == slot1), 1.0, 0.0).astype(bf16)

    def gather(g, carry):
        choose = picked(g * 256, 256)

        def cols(q, carry):
            at = pl.ds(pl.multiple_of(q * 512, 512), 512)
            rows = jnp.dot(choose, xn[:, at], preferred_element_type=f32).astype(bf16)
            sm[pl.ds(g * 4, 4), :, at] = rows.reshape(4, 64, 512)
            return carry

        lax.fori_loop(0, 4, cols, 0)

        @pl.when(g % 2 == 1)
        def _():
            step(3 + g // 2)

        return carry

    with jax.named_scope("s_gather"):
        lax.fori_loop(0, 4, gather, 0)
        choose = picked(1024, 128)

        def gather_rest(q, carry):
            at = pl.ds(pl.multiple_of(q * 512, 512), 512)
            rows = jnp.dot(choose, xn[:, at], preferred_element_type=f32)
            sr[:, :, at] = rows.reshape(16, 8, 512).astype(bf16)
            return carry

        lax.fori_loop(0, 4, gather_rest, 0)

    def block_at(k, sign):
        dx, dy = OFFSETS[k]
        xx, yy = (x + sign * dx + NX) % NX, (y + sign * dy + NY) % NY
        return xx * NY + yy, (device(z, xx, c), yy)

    def dispatch(k, part):
        block, peer = block_at(k, 1)
        if part < 2:
            src, dst = sm.at[block, pl.ds(part * 32, 32)], rm.at[me, pl.ds(part * 32, 32)]
        else:
            src, dst = sr.at[block], rr.at[me]
        return pltpu.make_async_remote_copy(
            src_ref=src, dst_ref=dst, send_sem=d_sent.at[part, k], recv_sem=d_recv.at[part, k],
            device_id=peer, device_id_type=MESH,
        )

    with jax.named_scope("s_dispatch"):
        for part in range(3):
            for k in range(15):
                dispatch(k, part).start()
        rm[me] = sm[me]
        rr[me] = sr[me]

    with jax.named_scope("s_filter"):
        halo.wait_recv()
        pad[0:HALO, :] = jnp.where(ep > 0, halo_in[...].astype(f32), 0.0)
        loads[3].wait()

        def filter_block(b, carry):
            step(5 + b)
            base = pl.multiple_of(b * 128, 128)
            window[...] = pad[pl.ds(base, 128 + HALO), :]
            total = None
            for k in range(KERNEL):
                low = HALO - KERNEL + 1 + k
                term = taps[k : k + 1, :] * window[low : low + 128, :]
                total = term if total is None else total + term
            filt[pl.ds(base, 128), :] = total
            stat[y, pl.ds(b, 1), :] = to_row(jnp.sum(total, axis=1, keepdims=True))
            stat[y, pl.ds(8 + b, 1), :] = to_row(jnp.sum(total * total, axis=1, keepdims=True))
            return carry

        lax.fori_loop(0, 8, filter_block, 0)

    def near(k):
        yy = (y + k) % NY
        return yy, (ep, yy)

    def stat_copy(k):
        return pltpu.make_async_remote_copy(
            src_ref=stat.at[y], dst_ref=stat.at[y], send_sem=stat_sent.at[k], recv_sem=stat_recv.at[k],
            device_id=near(k)[1], device_id_type=MESH,
        )

    def act_copy(k):
        yy, peer = near(k)
        return pltpu.make_async_remote_copy(
            src_ref=act.at[pl.ds(pl.multiple_of(yy * 256, 256), 256)], dst_ref=acts.at[y],
            send_sem=act_sent.at[k], recv_sem=act_recv.at[k], device_id=peer, device_id_type=MESH,
        )

    half = pl.ds(pl.multiple_of(c * 128, 128), 128)

    def cw_copy(k):
        return pltpu.make_async_remote_copy(
            src_ref=cw.at[y, half], dst_ref=cw.at[y, half], send_sem=cw_sent.at[k],
            recv_sem=cw_recv.at[k], device_id=near(k)[1], device_id_type=MESH,
        )

    def cs_copy(k):
        yy = (y + NY - k) % NY
        return pltpu.make_async_remote_copy(
            src_ref=cw.at[yy, half], dst_ref=cw.at[yy, half], send_sem=cs_sent.at[k],
            recv_sem=cs_recv.at[k], device_id=sibling, device_id_type=MESH,
        )

    loads[4].wait()
    for k in (1, 3, 2):
        stat_copy(k).start()
    for k in (1, 3, 2):
        cw_copy(k).start()

    def only_step(p, carry):
        step(p)
        return carry

    with jax.named_scope("s_pumps"):
        lax.fori_loop(13, START, only_step, 0)

    with jax.named_scope("s_wait_rows"):
        for part in range(3):
            for k in range(15):
                dispatch(k, part).wait_recv()
        rx[...] = rr[...].astype(f32).reshape(128, 2048).astype(bf16)
        hg[...] = jnp.zeros_like(hg)
        hu[...] = jnp.zeros_like(hu)

    with jax.named_scope("s_wait_stat"):
        for k in (1, 3, 2):
            stat_copy(k).wait_recv()
        stats[...] = (stat[0] + stat[1]) + (stat[2] + stat[3])

    order_in_rest = (lax.broadcasted_iota(jnp.int32, (128, 256), 0) % 8) // REM

    def ffn(f, carry):
        cc, j = f // CHUNKS, f % CHUNKS

        @pl.when((dist > 0) | (f % 2 != c))
        def _():
            sib_copy(hs, f, share).wait_recv()

        at_k = pl.ds(pl.multiple_of(((j % 8) // 2) * 512, 512), 512)
        at_n = pl.ds(pl.multiple_of((j % 2) * 256, 256), 256)
        at_o = pl.ds(pl.multiple_of((j % 8) * 256, 256), 256)
        for h in range(2):
            at_r = pl.ds(pl.multiple_of(cc * 32 + h * MAIN, MAIN), MAIN)

            def product(h=h, at_r=at_r):
                rows = jnp.concatenate([rm[:, at_r, at_k].reshape(256, 512), rx[:, at_k]], axis=0)
                return jnp.dot(rows, w[h, cc, j], preferred_element_type=f32)

            @pl.when(j < 8)
            def _(h=h):
                hg[h, :, at_n] += product()

            @pl.when((j >= 8) & (j < 16))
            def _(h=h):
                hu[h, :, at_n] += product()

            @pl.when(j == 15)
            def _(h=h):
                gate = hg[h]
                inner[h] = (jax.nn.silu(gate) * hu[h]).astype(bf16)
                hg[h] = jnp.zeros_like(gate)
                hu[h] = jnp.zeros_like(gate)

            @pl.when(j >= 16)
            def _(h=h, at_r=at_r):
                rows = jnp.dot(inner[h], w[h, cc, j], preferred_element_type=f32)
                rm[:, at_r, at_o] = rows[:256].astype(bf16).reshape(16, MAIN, 256)
                mine = order_in_rest == cc * 2 + h
                orx[:, at_o] = jnp.where(mine, rows[256:], orx[:, at_o])

        return carry

    def activate(b):
        rows = pl.ds(pl.multiple_of(b * 128, 128), 128)
        center = to_column(stats[pl.ds(b, 1), :], 128) / CONV
        spread = to_column(stats[pl.ds(8 + b, 1), :], 128) / CONV - center * center
        normed = (filt[rows, :] - center) * lax.rsqrt(spread + 1e-05) * gain_c[:, my_cols] + shift_c[
            :, my_cols
        ]
        act[rows, :] = jax.nn.silu(normed).astype(bf16)

    def phase0(p, carry):
        step(p)
        activate(p - START)
        return lax.fori_loop(3 * (p - START), 3 * (p - START) + 3, ffn, carry)

    with jax.named_scope("s_phase0"):
        lax.fori_loop(START, START + 8, phase0, 0)

    def back(k):
        block, peer = block_at(k, -1)
        return pltpu.make_async_remote_copy(
            src_ref=rm.at[block, pl.ds(0, 32)], dst_ref=bm.at[me, pl.ds(0, 32)],
            send_sem=r_sent.at[k], recv_sem=r_recv.at[k], device_id=peer, device_id_type=MESH,
        )

    with jax.named_scope("s_back0"):
        for k in (1, 3, 2):
            act_copy(k).start()
        acts[y] = act[my_cols, :]
        for k in range(15):
            back(k).start()
        bm[me, 0:32] = rm[me, 0:32]

    def conv_part(q):
        at = pl.ds(pl.multiple_of(q * 512, 512), 512)
        total = None
        for b in range(4):
            term = jnp.dot(acts[b], cw[b, :, at], preferred_element_type=f32).astype(bf16).astype(f32)
            total = term if total is None else total + term
        conv_out[:, at] = total.astype(bf16)

    def phase1(p, carry):
        step(p)

        @pl.when(p == START + 9)
        def _():
            for k in (1, 3, 2):
                cw_copy(k).wait_recv()
                cs_copy(k).start()

        @pl.when(p == START + 11)
        def _():
            for k in (1, 3, 2):
                act_copy(k).wait_recv()
                cs_copy(k).wait_recv()

        @pl.when((p >= START + 12) & (p < START + 16))
        def _():
            conv_part(p - START - 12)

        low = jnp.where(p < START + 11, CHUNKS + 2 * (p - START - 8), p - FAR)
        high = jnp.where(p < START + 11, low + 2, low + 1)
        lax.fori_loop(low, high, ffn, 0)
        return carry

    def quarter(k, q, main):
        block, peer = block_at(k, -1)
        at = pl.ds(q * 512, 512)
        if main:
            src, dst = rm.at[block, pl.ds(32, 32), at], bm.at[me, pl.ds(32, 32), at]
        else:
            src, dst = rr.at[block, :, at], br.at[me, :, at]
        return pltpu.make_async_remote_copy(
            src_ref=src, dst_ref=dst, send_sem=q_sent.at[q, 1 - main, k],
            recv_sem=q_recv.at[q, 1 - main, k], device_id=peer, device_id_type=MESH,
        )

    with jax.named_scope("s_phase1"):
        last = TOTAL + FAR

        def tail(p, carry):
            phase1(p, carry)
            for q in range(4):

                @pl.when(p == last - 7 + 2 * q)
                def _(q=q):
                    at = slice(q * 512, q * 512 + 512)
                    rr[:, :, at] = orx[:, at].reshape(16, 8, 512).astype(bf16)
                    for main in (1, 0):
                        for k in range(15):
                            quarter(k, q, main).start()
                    bm[me, 32:64, at] = rm[me, 32:64, at]
                    br[me, :, at] = rr[me, :, at]

            return carry

        lax.fori_loop(START + 8, last, tail, 0)

    with jax.named_scope("s_combine0"):
        slot0_c, slot1_c = to_column(slot0, tokens), to_column(slot1, tokens)
        group = jax.nn.sigmoid(table[2:3, :])
        weight0 = to_column(group * jax.nn.sigmoid(table[3:4, :]), tokens)
        weight1 = to_column(group * jax.nn.sigmoid(-table[3:4, :]), tokens)

        def chosen(slot, cc):
            at = lax.broadcasted_iota(jnp.int32, (tokens, 512), 1)
            main = ((at // 32) * 64 + cc * 32 + at % 32).astype(f32)
            hits = jnp.where(main == slot, 1.0, 0.0).astype(bf16)
            if cc == 0:
                return hits
            rest = (lax.broadcasted_iota(jnp.int32, (tokens, 128), 1) + 1024).astype(f32)
            return jnp.concatenate([hits, jnp.where(rest == slot, 1.0, 0.0).astype(bf16)], axis=1)

        for k in range(15):
            back(k).wait_recv()
        pick0, pick1 = chosen(slot0_c, 0), chosen(slot1_c, 0)

        def combine0(q, carry):
            at = pl.ds(pl.multiple_of(q * 512, 512), 512)
            rows = bm[:, 0:32, at].reshape(512, 512)
            acc[:, at] = weight0 * jnp.dot(
                pick0, rows, preferred_element_type=f32
            ) + weight1 * jnp.dot(pick1, rows, preferred_element_type=f32)
            return carry

        lax.fori_loop(0, 4, combine0, 0)

    with jax.named_scope("s_combine1"):
        pick0b, pick1b = chosen(slot0_c, 1), chosen(slot1_c, 1)
        for q in range(4):
            for main in (1, 0):
                for k in range(15):
                    quarter(k, q, main).wait_recv()
            at = slice(q * 512, q * 512 + 512)
            rest = br[:, :, at].astype(f32).reshape(128, 512).astype(bf16)
            rows = jnp.concatenate([bm[:, 32:64, at].reshape(512, 512), rest], axis=0)
            total = acc[:, at] + (
                weight0 * jnp.dot(pick0b, rows, preferred_element_type=f32)
                + weight1 * jnp.dot(pick1b, rows, preferred_element_type=f32)
            )
            out[:, at] = total.astype(bf16)

    with jax.named_scope("s_sent"):
        halo.wait_send()
        for k in (1, 3, 2):
            stat_copy(k).wait_send()
            act_copy(k).wait_send()
            cw_copy(k).wait_send()
            cs_copy(k).wait_send()
        for k in range(15):
            for part in range(3):
                dispatch(k, part).wait_send()
            back(k).wait_send()
            for q in range(4):
                for main in (1, 0):
                    quarter(k, q, main).wait_send()

        def sent(n, carry):
            @pl.when((dist < 3) | (n % 2 == c))
            def _():
                ring_copy(n, avail).wait_send()

            sib_copy(hs, n, share).wait_send()
            return carry

        lax.fori_loop(0, TOTAL, sent, 0)


def on_device(
    conv_value,
    conv_gate,
    depth_weight,
    norm_gain,
    norm_shift,
    conv_out_weight,
    moe_input,
    moe_gain,
    route_experts,
    route_scores,
    expert_gate,
    expert_up,
    expert_down,
):
    bf16, f32 = jnp.bfloat16, jnp.float32
    rows, width = moe_input.shape
    span, channels = conv_value.shape
    table = jnp.concatenate([route_experts.T.astype(f32), route_scores.T], axis=0)
    hbm = pl.BlockSpec(memory_space=pl.ANY)
    vmem = pl.BlockSpec(memory_space=pltpu.VMEM)
    dma = pltpu.SemaphoreType.DMA
    return pl.pallas_call(
        kernel,
        out_shape=(
            jax.ShapeDtypeStruct((span // NY, width), bf16),
            jax.ShapeDtypeStruct((rows, width), bf16),
        ),
        in_specs=[hbm, hbm, hbm, vmem, vmem, hbm, hbm, vmem, vmem, hbm, hbm, hbm],
        out_specs=(vmem, vmem),
        scratch_shapes=[
            pltpu.VMEM((2, 2, CHUNKS, 512, 256), bf16),
            pltpu.VMEM((rows, width), bf16),
            pltpu.VMEM((16, 64, width), bf16),
            pltpu.VMEM((16, 8, width), bf16),
            pltpu.VMEM((16, 64, width), bf16),
            pltpu.VMEM((16, 8, width), bf16),
            pltpu.VMEM((16, 64, width), bf16),
            pltpu.VMEM((16, 8, width), bf16),
            pltpu.VMEM((2, 384, 512), f32),
            pltpu.VMEM((2, 384, 512), f32),
            pltpu.VMEM((2, 384, 512), bf16),
            pltpu.VMEM((128, width), bf16),
            pltpu.VMEM((128, width), f32),
            pltpu.VMEM((rows, width), f32),
            pltpu.VMEM((span, channels), bf16),
            pltpu.VMEM((span, channels), bf16),
            pltpu.VMEM((KERNEL, channels), f32),
            pltpu.VMEM((HALO + span, channels), f32),
            pltpu.VMEM((span, channels), f32),
            pltpu.VMEM((span, channels), bf16),
            pltpu.VMEM((NY, span // NY, channels), bf16),
            pltpu.VMEM((NY, channels, width), bf16),
            pltpu.VMEM((128 + HALO, channels), f32),
            pltpu.VMEM((HALO, channels), bf16),
            pltpu.VMEM((HALO, channels), bf16),
            pltpu.VMEM((NY, 16, 128), f32),
            pltpu.VMEM((16, 128), f32),
            dma((5,)),
            dma((TOTAL,)),
            dma((TOTAL,)),
            dma((TOTAL,)),
            dma,
            dma,
            dma((3, 15)),
            dma((3, 15)),
            dma((15,)),
            dma((15,)),
            dma((4, 2, 15)),
            dma((4, 2, 15)),
            dma((2,)),
            dma((4,)),
            dma((4,)),
            dma((4,)),
            dma((4,)),
            dma((4,)),
            dma((4,)),
            dma((4,)),
            dma((4,)),
        ],
        compiler_params=pltpu.CompilerParams(
            collective_id=0, has_side_effects=True, vmem_limit_bytes=67_000_000
        ),
        name="both",
    )(
        conv_value,
        conv_gate,
        depth_weight,
        norm_gain.reshape(1, CONV),
        norm_shift.reshape(1, CONV),
        conv_out_weight,
        moe_input,
        moe_gain.reshape(1, width),
        table,
        expert_gate,
        expert_up,
        expert_down,
    )


def solution(mesh):
    in_specs = (
        P("ep", "tp"),
        P("ep", "tp"),
        P(),
        P(),
        P(),
        P("tp", None),
        P(("ep", "tp"), None),
        P(),
        P(("ep", "tp"), None),
        P(("ep", "tp"), None),
        P("ep", None, None),
        P("ep", None, None),
        P("ep", None, None),
    )
    out_specs = (P(("ep", "tp"), None), P(("ep", "tp"), None))
    return jax.shard_map(
        on_device, mesh=mesh, in_specs=in_specs, out_specs=out_specs, check_vma=False
    )
```

```python
import jax
import jax.numpy as jnp
from jax import lax
from jax.experimental import pallas as pl
from jax.experimental.pallas import tpu as pltpu
from jax.sharding import PartitionSpec as P

MESH = pl.DeviceIdType.MESH
NZ, NX, NC, NY = 8, 4, 2, 4
CONV = 1024
KERNEL = 31
HALO = 32
MAIN = 16
REM = 2
PIECE = 256
CHUNKS = 48
TOTAL = 2 * CHUNKS
HOP = 4
FAR = 3 * HOP + 3
OUTER = 4 * HOP + 2
START = 50
MIDDLE = START + 16
LAST = TOTAL + FAR
OFFSETS = [
    (1, 0), (3, 0), (0, 1), (0, 3), (1, 1), (3, 3), (1, 3), (3, 1),
    (2, 0), (0, 2), (2, 2), (1, 2), (3, 2), (2, 1), (2, 3),
]


def slot_of(expert, rank, z, c):
    high = expert // 8
    yy = high % 4
    block = ((expert // 2) % 4) * NY + yy
    hops = (z - yy + 8) % 4
    below = ((z - hops - yy + 8) % 8) // 4
    other = jnp.where(high // 4 == below, 0, 1)
    flip = (other + jnp.where(hops == 0, c, 0)) % 2
    half = jnp.where(flip == 0, expert % 2, 1 - expert % 2)
    order = half * 2 + other
    main = (block * 64 + order * MAIN).astype(jnp.float32) + rank
    rest = (1024 + block * 8 + order * REM).astype(jnp.float32) + (rank - MAIN)
    return jnp.where(rank < MAIN, main, jnp.where(rank < MAIN + REM, rest, -1.0))


def eye(n):
    return lax.broadcasted_iota(jnp.int32, (n, n), 0) == lax.broadcasted_iota(jnp.int32, (n, n), 1)


def to_column(row, n):
    pieces = []
    for at in range(0, n, 128):
        spread = jnp.where(eye(128), row[:, at : at + 128], 0.0)
        pieces.append(jnp.sum(spread, axis=1, keepdims=True))
    return pieces[0] if len(pieces) == 1 else jnp.concatenate(pieces, axis=0)


def to_row(column):
    return jnp.sum(jnp.where(eye(128), column, 0.0), axis=0, keepdims=True)


def kernel(
    value_hbm, gate_hbm, taps_hbm, gain_c, shift_c, cw_hbm,
    x_hbm, gain, experts, scores, wg_hbm, wu_hbm, wd_hbm,
    conv_out, out,
    w, xn, sm, sr, rm, rr, bm, br, hidden, inner, rx, orx,
    val, gat, taps, pad, acts, cw, window, halo_out, halo_in, stat, stats,
    load, avail, share, foreign, ring_sent, sib_sent,
    d_sent, d_recv, r_sent, r_recv, q_sent, q_recv,
    halo_sem, stat_sent, stat_recv, act_sent, act_recv, cw_sent, cw_recv, cs_sent, cs_recv,
):
    f32, bf16 = jnp.float32, jnp.bfloat16
    ep = lax.axis_index("ep")
    y = lax.axis_index("tp")
    z, x, c = ep // 8, (ep // 2) % 4, ep % 2
    me = x * NY + y
    dd = (z - y + 8) % 4
    dist = jnp.where(c == 0, dd, (4 - dd) % 4)
    h_low = ((z - dd - y + 8) % 8) // 4
    hs = jnp.where((c == 0) | (dd == 0), h_low, 1 - h_low)

    def device(zz, xx, cc):
        return (zz * NX + xx) * NC + cc

    along = jnp.where(c == 0, (z + 1) % NZ, (z + NZ - 1) % NZ)
    ring_to = (device(along, x, c), y)
    sibling = (device(z, x, 1 - c), y)
    my_cols = pl.ds(pl.multiple_of(y * 256, 256), 256)

    loads = [
        pltpu.make_async_copy(value_hbm, val, load.at[0]),
        pltpu.make_async_copy(gate_hbm, gat, load.at[1]),
        pltpu.make_async_copy(x_hbm, xn, load.at[2]),
        pltpu.make_async_copy(taps_hbm.at[:, my_cols], taps, load.at[3]),
        pltpu.make_async_copy(cw_hbm, cw.at[y], load.at[4]),
    ]

    @pl.when(dist == 0)
    def _():
        def native(i, src):
            dst = w.at[hs, c, pl.ds(i * PIECE, PIECE)]
            pltpu.make_async_copy(src, dst, avail.at[c * CHUNKS + i]).start()

        for i in range(CHUNKS):
            ref = wg_hbm if i < 16 else wu_hbm if i < 32 else wd_hbm
            block, row = (i // 8 % 2, i % 8) if i < 32 else ((i - 32) // 2, i % 2)
            native(i, ref.at[0, pl.ds(row * PIECE, PIECE), pl.ds(block * 256, 256)])

    for copy in loads:
        copy.start()

    barrier = pltpu.get_barrier_semaphore()
    peers = [(device(z, (x + dx) % NX, c), (y + dy) % NY) for dx, dy in OFFSETS]
    peers += [(device((z + 1) % NZ, x, c), y), (device((z + NZ - 1) % NZ, x, c), y), sibling]
    peers += [((ep + 1) % 64, y), ((ep + 63) % 64, y)]
    for peer in peers:
        pl.semaphore_signal(barrier, inc=1, device_id=peer, device_id_type=MESH)

    def ring_copy(n, sem):
        ref = w.at[hs, n // CHUNKS, pl.ds(pl.multiple_of(n % CHUNKS * PIECE, PIECE), PIECE)]
        return pltpu.make_async_remote_copy(
            src_ref=ref, dst_ref=ref, send_sem=ring_sent, recv_sem=sem.at[n],
            device_id=ring_to, device_id_type=MESH,
        )

    def sib_copy(h, n, sem):
        ref = w.at[h, n // CHUNKS, pl.ds(pl.multiple_of(n % CHUNKS * PIECE, PIECE), PIECE)]
        return pltpu.make_async_remote_copy(
            src_ref=ref, dst_ref=ref, send_sem=sib_sent, recv_sem=sem.at[n],
            device_id=sibling, device_id_type=MESH,
        )

    def expert_at(n):
        return jnp.where(c == 0, n, (n + CHUNKS) % TOTAL)

    def own(n):
        i = expert_at(n)
        ring_copy(i, avail).wait_recv()

        @pl.when(dist < 3)
        def _():
            ring_copy(i, avail).start()

        @pl.when((dist == 3) & (n < CHUNKS))
        def _():
            ring_copy(i, foreign).start()

        @pl.when(dist > 0)
        def _():
            sib_copy(hs, i, share).start()

        @pl.when((dist == 0) & (i // CHUNKS == c))
        def _():
            sib_copy(hs, i, avail).start()

    def step(p):
        n = p - HOP * dist
        m = p - OUTER

        @pl.when((n >= 0) & (n < TOTAL))
        def _():
            own(n)

        @pl.when((dist == 0) & (m >= 0) & (m < CHUNKS))
        def _():
            i = expert_at(m)
            ring_copy(i, foreign).wait_recv()
            sib_copy(1 - hs, i, share).start()

    with jax.named_scope("s_gated"):
        loads[0].wait()
        loads[1].wait()

        def gated(b, carry):
            rows = pl.ds(pl.multiple_of(b * 128, 128), 128)
            wide = val[rows, :].astype(f32) * jax.nn.sigmoid(gat[rows, :].astype(f32))
            pad[pl.ds(pl.multiple_of(HALO + b * 128, 32), 128), :] = wide.astype(bf16).astype(f32)
            return carry

        lax.fori_loop(0, 8, gated, 0)
        halo_out[...] = pad[1024 : 1024 + HALO, :].astype(bf16)

        halo = pltpu.make_async_remote_copy(
            src_ref=halo_out, dst_ref=halo_in, send_sem=halo_sem.at[0], recv_sem=halo_sem.at[1],
            device_id=((ep + 1) % 64, y), device_id_type=MESH,
        )
    with jax.named_scope("s_route"):
        tokens = xn.shape[0]
        first, second = experts[0:1, :], experts[1:2, :]
        ids = lax.broadcasted_iota(jnp.int32, (64, tokens), 0)
        hit0, hit1 = ids == first, ids == second
        both = jnp.where(hit0 | hit1, 1.0, 0.0).astype(bf16)
        row_t = lax.broadcasted_iota(jnp.int32, (tokens, tokens), 0)
        col_t = lax.broadcasted_iota(jnp.int32, (tokens, tokens), 1)
        earlier = jnp.where(row_t < col_t, 1.0, 0.0).astype(bf16)
        counts = jnp.dot(both, earlier, preferred_element_type=f32)
        slot0 = slot_of(first, jnp.sum(jnp.where(hit0, counts, 0.0), axis=0, keepdims=True), z, c)
        slot1 = slot_of(second, jnp.sum(jnp.where(hit1, counts, 0.0), axis=0, keepdims=True), z, c)

    with jax.named_scope("s_norm"):
        loads[2].wait()

        def norm(b, carry):
            rows = pl.ds(pl.multiple_of(b * 64, 64), 64)
            wide = xn[rows, :].astype(f32)
            square = jnp.mean(wide * wide, axis=-1, keepdims=True)
            xn[rows, :] = (wide * lax.rsqrt(square + 1e-06) * gain[...]).astype(bf16)
            return carry

        lax.fori_loop(0, 6, norm, 0)

    with jax.named_scope("s_barrier"):
        pl.semaphore_wait(barrier, len(peers))
    halo.start()
    step(0)

    def picked(base, count):
        at = (lax.broadcasted_iota(jnp.int32, (count, tokens), 0) + base).astype(f32)
        return jnp.where((at == slot0) | (at == slot1), 1.0, 0.0).astype(bf16)

    def gather(g, carry):
        choose = picked(g * 256, 256)

        def cols(q, carry):
            at = pl.ds(pl.multiple_of(q * 512, 512), 512)
            rows = jnp.dot(choose, xn[:, at], preferred_element_type=f32).astype(bf16)
            sm[pl.ds(g * 4, 4), :, at] = rows.reshape(4, 64, 512)
            return carry

        lax.fori_loop(0, 4, cols, 0)

        step(1 + g)
        return carry

    with jax.named_scope("s_gather"):
        lax.fori_loop(0, 4, gather, 0)
        choose = picked(1024, 128)

        def gather_rest(q, carry):
            at = pl.ds(pl.multiple_of(q * 512, 512), 512)
            rows = jnp.dot(choose, xn[:, at], preferred_element_type=f32)
            sr[:, :, at] = rows.reshape(16, 8, 512).astype(bf16)
            return carry

        lax.fori_loop(0, 4, gather_rest, 0)

    def block_at(k, sign):
        dx, dy = OFFSETS[k]
        xx, yy = (x + sign * dx + NX) % NX, (y + sign * dy + NY) % NY
        return xx * NY + yy, (device(z, xx, c), yy)

    def dispatch(k, part):
        block, peer = block_at(k, 1)
        if part < 2:
            src, dst = sm.at[block, pl.ds(part * 32, 32)], rm.at[me, pl.ds(part * 32, 32)]
        else:
            src, dst = sr.at[block], rr.at[me]
        return pltpu.make_async_remote_copy(
            src_ref=src, dst_ref=dst, send_sem=d_sent.at[part, k], recv_sem=d_recv.at[part, k],
            device_id=peer, device_id_type=MESH,
        )

    with jax.named_scope("s_dispatch"):
        for part in range(3):
            for k in range(15):
                dispatch(k, part).start()
        rm[me] = sm[me]
        rr[me] = sr[me]

    with jax.named_scope("s_filter"):
        halo.wait_recv()
        pad[0:HALO, :] = jnp.where(ep > 0, halo_in[...].astype(f32), 0.0)
        loads[3].wait()

        def filter_block(b, carry):
            step(5 + 2 * b)
            step(6 + 2 * b)
            base = pl.multiple_of(b * 128, 128)
            window[...] = pad[pl.ds(base, 128 + HALO), :]
            total = None
            for k in range(KERNEL):
                low = HALO - KERNEL + 1 + k
                term = taps[k : k + 1, :] * window[low : low + 128, :]
                total = term if total is None else total + term
            pad[pl.ds(base, 128), :] = total
            stat[y, pl.ds(b, 1), :] = to_row(jnp.sum(total, axis=1, keepdims=True))
            stat[y, pl.ds(8 + b, 1), :] = to_row(jnp.sum(total * total, axis=1, keepdims=True))
            return carry

        lax.fori_loop(0, 8, filter_block, 0)

    def near(k):
        yy = (y + k) % NY
        return yy, (ep, yy)

    def stat_copy(k):
        return pltpu.make_async_remote_copy(
            src_ref=stat.at[y], dst_ref=stat.at[y], send_sem=stat_sent.at[k], recv_sem=stat_recv.at[k],
            device_id=near(k)[1], device_id_type=MESH,
        )

    def act_copy(k):
        yy, peer = near(k)
        return pltpu.make_async_remote_copy(
            src_ref=val.at[pl.ds(pl.multiple_of(yy * 256, 256), 256)], dst_ref=acts.at[y],
            send_sem=act_sent.at[k], recv_sem=act_recv.at[k], device_id=peer, device_id_type=MESH,
        )

    half = pl.ds(pl.multiple_of(c * 128, 128), 128)

    def cw_copy(k):
        return pltpu.make_async_remote_copy(
            src_ref=cw.at[y, half], dst_ref=cw.at[y, half], send_sem=cw_sent.at[k],
            recv_sem=cw_recv.at[k], device_id=near(k)[1], device_id_type=MESH,
        )

    def cs_copy(k):
        yy = (y + NY - k) % NY
        return pltpu.make_async_remote_copy(
            src_ref=cw.at[yy, half], dst_ref=cw.at[yy, half], send_sem=cs_sent.at[k],
            recv_sem=cs_recv.at[k], device_id=sibling, device_id_type=MESH,
        )

    loads[4].wait()
    for k in (1, 3, 2):
        stat_copy(k).start()
    for k in (1, 3, 2):
        cw_copy(k).start()

    def only_step(p, carry):
        step(p)
        return carry

    with jax.named_scope("s_pumps"):
        lax.fori_loop(21, START, only_step, 0)

    with jax.named_scope("s_wait_rows"):
        for part in range(3):
            for k in range(15):
                dispatch(k, part).wait_recv()
        rx[...] = rr[...].astype(f32).reshape(128, 2048).astype(bf16)

    with jax.named_scope("s_wait_stat"):
        for k in (1, 3, 2):
            stat_copy(k).wait_recv()
        stats[...] = (stat[0] + stat[1]) + (stat[2] + stat[3])

    order_in_rest = (lax.broadcasted_iota(jnp.int32, (128, 256), 0) % 8) // REM

    def of_half(half, s):
        e_low = jnp.where((dist == 0) & (c == 1), 1 - half, half)
        return jnp.where(s == 0, h_low, 1 - h_low), jnp.where(s == 0, e_low, 1 - e_low)

    def shared(half, low, count):
        others = jnp.where(dist == 0, 1 - c, jnp.where(c == 0, 1 - half, half))

        def wait(i, carry):
            sib_copy(hs, others * CHUNKS + i, share).wait_recv()
            return carry

        @pl.when((dist > 0) | (half == 0))
        def _():
            lax.fori_loop(low, low + count, wait, 0)

    def rows_at(half, s):
        return pl.ds(pl.multiple_of(half * 32 + s * MAIN, MAIN), MAIN)

    def gate_up(half, block, s):
        @pl.when(s == 0)
        def _():
            shared(half, block * 8, 8)

        h, e = of_half(half, s)
        rows = jnp.concatenate([rm[:, rows_at(half, s), :].reshape(256, 2048), rx[...]], axis=0)
        weight = w[h, e, pl.ds(pl.multiple_of(block * 2048, 2048), 2048), :]
        at = pl.ds(pl.multiple_of(block * 256, 256), 256)
        hidden[s, :, at] = jnp.dot(rows, weight, preferred_element_type=f32)

        @pl.when(block == 3)
        def _():
            inner[s] = (jax.nn.silu(hidden[s, :, 0:512]) * hidden[s, :, 512:1024]).astype(bf16)

    def down(half, block):
        shared(half, 32 + block * 2, 2)
        at = pl.ds(pl.multiple_of(block * 256, 256), 256)
        for s in range(2):
            h, e = of_half(half, s)
            weight = w[h, e, pl.ds(pl.multiple_of(8192 + block * 512, 512), 512), :]
            rows = jnp.dot(inner[s], weight, preferred_element_type=f32)
            rm[:, rows_at(half, s), at] = rows[:256].astype(bf16).reshape(16, MAIN, 256)
            here = order_in_rest == half * 2 + s
            orx[:, at] = jnp.where(here, rows[256:], orx[:, at])

    def activate(b):
        rows = pl.ds(pl.multiple_of(b * 128, 128), 128)
        center = to_column(stats[pl.ds(b, 1), :], 128) / CONV
        spread = to_column(stats[pl.ds(8 + b, 1), :], 128) / CONV - center * center
        normed = (pad[rows, :] - center) * lax.rsqrt(spread + 1e-05) * gain_c[:, my_cols] + shift_c[
            :, my_cols
        ]
        val[rows, :] = jax.nn.silu(normed).astype(bf16)

    def phase0(p, carry):
        step(p)

        @pl.when(p < START + 8)
        def _():
            activate(p - START)
            gate_up(0, (p - START) // 2, (p - START) % 2)

        @pl.when(p == START + 8)
        def _():
            for k in (1, 3, 2):
                act_copy(k).start()
            acts[y] = val[my_cols, :]

        @pl.when(p >= START + 8)
        def _():
            down(0, p - START - 8)

        return carry

    with jax.named_scope("s_phase0"):
        lax.fori_loop(START, MIDDLE, phase0, 0)

    def back(k):
        block, peer = block_at(k, -1)
        return pltpu.make_async_remote_copy(
            src_ref=rm.at[block, pl.ds(0, 32)], dst_ref=bm.at[me, pl.ds(0, 32)],
            send_sem=r_sent.at[k], recv_sem=r_recv.at[k], device_id=peer, device_id_type=MESH,
        )

    with jax.named_scope("s_back0"):
        for k in range(15):
            back(k).start()
        bm[me, 0:32] = rm[me, 0:32]

    def conv_part(q):
        at = pl.ds(pl.multiple_of(q * 512, 512), 512)
        total = None
        for b in range(4):
            term = jnp.dot(acts[b], cw[b, :, at], preferred_element_type=f32).astype(bf16).astype(f32)
            total = term if total is None else total + term
        conv_out[:, at] = total.astype(bf16)

    slot0_c, slot1_c = to_column(slot0, tokens), to_column(slot1, tokens)
    group = jax.nn.sigmoid(scores[0:1, :])
    weight0 = to_column(group * jax.nn.sigmoid(scores[1:2, :]), tokens)
    weight1 = to_column(group * jax.nn.sigmoid(-scores[1:2, :]), tokens)

    def chosen(slot, half):
        at = lax.broadcasted_iota(jnp.int32, (tokens, 512), 1)
        main = ((at // 32) * 64 + half * 32 + at % 32).astype(f32)
        hits = jnp.where(main == slot, 1.0, 0.0).astype(bf16)
        if half == 0:
            return hits
        rest = (lax.broadcasted_iota(jnp.int32, (tokens, 128), 1) + 1024).astype(f32)
        return jnp.concatenate([hits, jnp.where(rest == slot, 1.0, 0.0).astype(bf16)], axis=1)

    def combine0(q):
        at = pl.ds(pl.multiple_of(q * 512, 512), 512)
        kept = pl.ds(pl.multiple_of(q % 2 * 512, 512), 512)
        rows = bm[:, 0:32, at].reshape(512, 512)
        pick0, pick1 = chosen(slot0_c, 0), chosen(slot1_c, 0)
        hidden[q // 2, :, kept] = weight0 * jnp.dot(
            pick0, rows, preferred_element_type=f32
        ) + weight1 * jnp.dot(pick1, rows, preferred_element_type=f32)

    def phase1(p, carry):
        step(p)

        @pl.when(p == MIDDLE + 2)
        def _():
            for k in (1, 3, 2):
                cw_copy(k).wait_recv()
                cs_copy(k).start()

        @pl.when(p == MIDDLE + 6)
        def _():
            for k in (1, 3, 2):
                act_copy(k).wait_recv()
                cs_copy(k).wait_recv()

        @pl.when((p >= MIDDLE + 9) & (p < MIDDLE + 13))
        def _():
            conv_part(p - MIDDLE - 9)

        ready = p - FAR - CHUNKS + 1

        @pl.when((ready >= 8) & (ready < 34) & (ready % 8 < 2))
        def _():
            gate_up(1, ready // 8 - 1, ready % 8)

        @pl.when((ready >= 34) & (ready % 2 == 0))
        def _():
            down(1, (ready - 34) // 2)

        @pl.when(ready == 35)
        def _():
            for k in range(15):
                back(k).wait_recv()

        @pl.when((ready >= 35) & (ready % 2 == 1) & (ready < 43))
        def _():
            combine0((ready - 35) // 2)

        return carry

    def quarter(k, q, main):
        block, peer = block_at(k, -1)
        at = pl.ds(q * 512, 512)
        if main:
            src, dst = rm.at[block, pl.ds(32, 32), at], bm.at[me, pl.ds(32, 32), at]
        else:
            src, dst = rr.at[block, :, at], br.at[me, :, at]
        return pltpu.make_async_remote_copy(
            src_ref=src, dst_ref=dst, send_sem=q_sent.at[q, 1 - main, k],
            recv_sem=q_recv.at[q, 1 - main, k], device_id=peer, device_id_type=MESH,
        )

    with jax.named_scope("s_phase1"):
        def tail(p, carry):
            phase1(p, carry)
            for q in range(4):

                @pl.when(p == LAST - 13 + 4 * q)
                def _(q=q):
                    at = slice(q * 512, q * 512 + 512)
                    rr[:, :, at] = orx[:, at].reshape(16, 8, 512).astype(bf16)
                    for main in (1, 0):
                        for k in range(15):
                            quarter(k, q, main).start()
                    bm[me, 32:64, at] = rm[me, 32:64, at]
                    br[me, :, at] = rr[me, :, at]

            return carry

        lax.fori_loop(MIDDLE, LAST, tail, 0)

    with jax.named_scope("s_combine1"):
        pick0b, pick1b = chosen(slot0_c, 1), chosen(slot1_c, 1)
        for q in range(4):
            for main in (1, 0):
                for k in range(15):
                    quarter(k, q, main).wait_recv()
            at = slice(q * 512, q * 512 + 512)
            rest = br[:, :, at].astype(f32).reshape(128, 512).astype(bf16)
            rows = jnp.concatenate([bm[:, 32:64, at].reshape(512, 512), rest], axis=0)
            total = hidden[q // 2, :, q % 2 * 512 : q % 2 * 512 + 512] + (
                weight0 * jnp.dot(pick0b, rows, preferred_element_type=f32)
                + weight1 * jnp.dot(pick1b, rows, preferred_element_type=f32)
            )
            out[:, at] = total.astype(bf16)

    with jax.named_scope("s_sent"):
        halo.wait_send()
        for k in (1, 3, 2):
            stat_copy(k).wait_send()
            act_copy(k).wait_send()
            cw_copy(k).wait_send()
            cs_copy(k).wait_send()
        for k in range(15):
            for part in range(3):
                dispatch(k, part).wait_send()
            back(k).wait_send()
            for q in range(4):
                for main in (1, 0):
                    quarter(k, q, main).wait_send()

        def sent(n, carry):
            @pl.when((dist < 3) | (n < CHUNKS))
            def _():
                ring_copy(n, avail).wait_send()

            sib_copy(hs, n, share).wait_send()
            return carry

        lax.fori_loop(0, TOTAL, sent, 0)


def on_device(
    conv_value,
    conv_gate,
    depth_weight,
    norm_gain,
    norm_shift,
    conv_out_weight,
    moe_input,
    moe_gain,
    route_experts,
    route_scores,
    expert_gate,
    expert_up,
    expert_down,
):
    bf16, f32 = jnp.bfloat16, jnp.float32
    rows, width = moe_input.shape
    span, channels = conv_value.shape
    hbm = pl.BlockSpec(memory_space=pl.ANY)
    vmem = pl.BlockSpec(memory_space=pltpu.VMEM)
    dma = pltpu.SemaphoreType.DMA
    return pl.pallas_call(
        kernel,
        out_shape=(
            jax.ShapeDtypeStruct((span // NY, width), bf16),
            jax.ShapeDtypeStruct((rows, width), bf16),
        ),
        in_specs=[hbm, hbm, hbm, vmem, vmem, hbm, hbm, vmem, vmem, vmem, hbm, hbm, hbm],
        out_specs=(vmem, vmem),
        scratch_shapes=[
            pltpu.VMEM((2, 2, CHUNKS * PIECE, 256), bf16),
            pltpu.VMEM((rows, width), bf16),
            pltpu.VMEM((16, 64, width), bf16),
            pltpu.VMEM((16, 8, width), bf16),
            pltpu.VMEM((16, 64, width), bf16),
            pltpu.VMEM((16, 8, width), bf16),
            pltpu.VMEM((16, 64, width), bf16),
            pltpu.VMEM((16, 8, width), bf16),
            pltpu.VMEM((2, 384, 1024), f32),
            pltpu.VMEM((2, 384, 512), bf16),
            pltpu.VMEM((128, width), bf16),
            pltpu.VMEM((128, width), f32),
            pltpu.VMEM((span, channels), bf16),
            pltpu.VMEM((span, channels), bf16),
            pltpu.VMEM((KERNEL, channels), f32),
            pltpu.VMEM((HALO + span, channels), f32),
            pltpu.VMEM((NY, span // NY, channels), bf16),
            pltpu.VMEM((NY, channels, width), bf16),
            pltpu.VMEM((128 + HALO, channels), f32),
            pltpu.VMEM((HALO, channels), bf16),
            pltpu.VMEM((HALO, channels), bf16),
            pltpu.VMEM((NY, 16, 128), f32),
            pltpu.VMEM((16, 128), f32),
            dma((5,)),
            dma((TOTAL,)),
            dma((TOTAL,)),
            dma((TOTAL,)),
            dma,
            dma,
            dma((3, 15)),
            dma((3, 15)),
            dma((15,)),
            dma((15,)),
            dma((4, 2, 15)),
            dma((4, 2, 15)),
            dma((2,)),
            dma((4,)),
            dma((4,)),
            dma((4,)),
            dma((4,)),
            dma((4,)),
            dma((4,)),
            dma((4,)),
            dma((4,)),
        ],
        compiler_params=pltpu.CompilerParams(
            collective_id=0, has_side_effects=True, vmem_limit_bytes=67_000_000
        ),
        name="both",
    )(
        conv_value,
        conv_gate,
        depth_weight,
        norm_gain.reshape(1, CONV),
        norm_shift.reshape(1, CONV),
        conv_out_weight,
        moe_input,
        moe_gain.reshape(1, width),
        route_experts.T,
        route_scores.T,
        expert_gate,
        expert_up,
        expert_down,
    )


def solution(mesh):
    in_specs = (
        P("ep", "tp"),
        P("ep", "tp"),
        P(),
        P(),
        P(),
        P("tp", None),
        P(("ep", "tp"), None),
        P(),
        P(("ep", "tp"), None),
        P(("ep", "tp"), None),
        P("ep", None, None),
        P("ep", None, None),
        P("ep", None, None),
    )
    out_specs = (P(("ep", "tp"), None), P(("ep", "tp"), None))
    return jax.shard_map(
        on_device, mesh=mesh, in_specs=in_specs, out_specs=out_specs, check_vma=False
    )
```

```python
import jax
import jax.numpy as jnp
from jax import lax
from jax.experimental import pallas as pl
from jax.experimental.pallas import tpu as pltpu
from jax.sharding import PartitionSpec as P

MESH = pl.DeviceIdType.MESH
NZ, NX, NC, NY = 8, 4, 2, 4
CONV = 1024
KERNEL = 31
HALO = 32
MAIN = 16
REM = 2
PIECE = 256
CHUNKS = 48
TOTAL = 2 * CHUNKS
HOP = 4
FAR = 3 * HOP + 3
OUTER = 4 * HOP + 2
START = 50
MIDDLE = START + 16
LAST = TOTAL + FAR
OFFSETS = [
    (1, 0), (3, 0), (0, 1), (0, 3), (1, 1), (3, 3), (1, 3), (3, 1),
    (2, 0), (0, 2), (2, 2), (1, 2), (3, 2), (2, 1), (2, 3),
]


def slot_of(expert, rank, z, c):
    high = expert // 8
    yy = high % 4
    block = ((expert // 2) % 4) * NY + yy
    hops = (z - yy + 8) % 4
    below = ((z - hops - yy + 8) % 8) // 4
    other = jnp.where(high // 4 == below, 0, 1)
    flip = (other + jnp.where(hops == 0, c, 0)) % 2
    half = jnp.where(flip == 0, expert % 2, 1 - expert % 2)
    order = half * 2 + other
    main = (block * 64 + order * MAIN).astype(jnp.float32) + rank
    rest = (1024 + block * 8 + order * REM).astype(jnp.float32) + (rank - MAIN)
    return jnp.where(rank < MAIN, main, jnp.where(rank < MAIN + REM, rest, -1.0))


def eye(n):
    return lax.broadcasted_iota(jnp.int32, (n, n), 0) == lax.broadcasted_iota(jnp.int32, (n, n), 1)


def to_column(row, n):
    pieces = []
    for at in range(0, n, 128):
        spread = jnp.where(eye(128), row[:, at : at + 128], 0.0)
        pieces.append(jnp.sum(spread, axis=1, keepdims=True))
    return pieces[0] if len(pieces) == 1 else jnp.concatenate(pieces, axis=0)


def to_row(column):
    return jnp.sum(jnp.where(eye(128), column, 0.0), axis=0, keepdims=True)


def kernel(
    value_hbm, gate_hbm, taps_hbm, gain_c_hbm, shift_c_hbm, cw_hbm,
    x_hbm, gain_hbm, experts_hbm, scores_hbm, wg_hbm, wu_hbm, wd_hbm,
    conv_out, out,
    w, xn, sm, sr, rm, sx, bm, rest_out, rest_in, hidden, inner, rx, orx,
    val, gat, taps, gain_c, shift_c, gain, experts, scores,
    pad, acts, cw, window, halo_out, halo_in, stat, stats,
    load, native, avail, share, ring_sent, sib_sent,
    d_sent, d_recv, r_sent, r_recv, q_sent, q_recv,
    halo_sem, stat_sem, act_sem, cw_sem, cs_sem,
):
    f32, bf16 = jnp.float32, jnp.bfloat16
    ep = lax.axis_index("ep")
    y = lax.axis_index("tp")
    z, x, c = ep // 8, (ep // 2) % 4, ep % 2
    me = x * NY + y
    dd = (z - y + 8) % 4
    dist = jnp.where(c == 0, dd, (4 - dd) % 4)
    h_low = ((z - dd - y + 8) % 8) // 4
    hs = jnp.where((c == 0) | (dd == 0), h_low, 1 - h_low)

    def device(zz, xx, cc):
        return (zz * NX + xx) * NC + cc

    along = jnp.where(c == 0, (z + 1) % NZ, (z + NZ - 1) % NZ)
    ring_to = (device(along, x, c), y)
    sibling = (device(z, x, 1 - c), y)
    my_cols = pl.ds(pl.multiple_of(y * 256, 256), 256)

    loads = [
        pltpu.make_async_copy(value_hbm, val, load.at[0]),
        pltpu.make_async_copy(gate_hbm, gat, load.at[1]),
        pltpu.make_async_copy(x_hbm, xn, load.at[2]),
        pltpu.make_async_copy(taps_hbm.at[:, my_cols], taps, load.at[3]),
        pltpu.make_async_copy(cw_hbm, cw.at[y], load.at[4]),
        pltpu.make_async_copy(gain_c_hbm.at[:, my_cols], gain_c, load.at[5]),
        pltpu.make_async_copy(shift_c_hbm.at[:, my_cols], shift_c, load.at[6]),
        pltpu.make_async_copy(gain_hbm, gain, load.at[7]),
        pltpu.make_async_copy(experts_hbm, experts, load.at[8]),
        pltpu.make_async_copy(scores_hbm, scores, load.at[9]),
    ]

    @pl.when(dist == 0)
    def _():
        for i in range(CHUNKS):
            ref = wg_hbm if i < 16 else wu_hbm if i < 32 else wd_hbm
            block, row = (i // 8 % 2, i % 8) if i < 32 else ((i - 32) // 2, i % 2)
            pltpu.make_async_copy(
                ref.at[0, pl.ds(row * PIECE, PIECE), pl.ds(block * 256, 256)],
                w.at[hs, c, pl.ds(i * PIECE, PIECE)],
                native.at[i // 8],
            ).start()

    for copy in loads:
        copy.start()

    barrier = pltpu.get_barrier_semaphore()
    peers = [(device(z, (x + dx) % NX, c), (y + dy) % NY) for dx, dy in OFFSETS]
    peers += [(device((z + 1) % NZ, x, c), y), (device((z + NZ - 1) % NZ, x, c), y), sibling]
    peers += [((ep + 1) % 64, y), ((ep + 63) % 64, y)]
    for peer in peers:
        pl.semaphore_signal(barrier, inc=1, device_id=peer, device_id_type=MESH)

    def arrived(ref, sem):
        pltpu.make_async_copy(ref, ref, sem).wait()

    def piece(h, i):
        return w.at[h, i // CHUNKS, pl.ds(pl.multiple_of(i % CHUNKS * PIECE, PIECE), PIECE)]

    def ring_copy(i):
        return pltpu.make_async_remote_copy(
            src_ref=piece(hs, i), dst_ref=piece(hs, i), send_sem=ring_sent, recv_sem=avail.at[i],
            device_id=ring_to, device_id_type=MESH,
        )

    def sib_copy(h, i, sem):
        return pltpu.make_async_remote_copy(
            src_ref=piece(h, i), dst_ref=piece(h, i), send_sem=sib_sent, recv_sem=sem,
            device_id=sibling, device_id_type=MESH,
        )

    def share_of(i):
        j = i % CHUNKS
        return share.at[i // CHUNKS * 12 + jnp.where(j < 32, j // 8, 4 + (j - 32) // 2)]

    def expert_at(n):
        return jnp.where(c == 0, n, (n + CHUNKS) % TOTAL)

    def own(n):
        i = expert_at(n)
        mine = (dist == 0) & (i // CHUNKS == c)

        @pl.when(mine & (i % 8 == 0))
        def _():
            arrived(w.at[hs, c, pl.ds(0, 8 * PIECE)], native.at[i % CHUNKS // 8])

        @pl.when(jnp.logical_not(mine))
        def _():
            ring_copy(i).wait_recv()

        @pl.when((dist < 3) | (n < CHUNKS))
        def _():
            ring_copy(i).start()

        @pl.when(dist > 0)
        def _():
            sib_copy(hs, i, share_of(i)).start()

        @pl.when(mine)
        def _():
            sib_copy(hs, i, avail.at[i]).start()

    def step(p):
        n = p - HOP * dist
        m = p - OUTER

        @pl.when((n >= 0) & (n < TOTAL))
        def _():
            own(n)

        @pl.when((dist == 0) & (m >= 0) & (m < CHUNKS))
        def _():
            i = expert_at(m)
            ring_copy(i).wait_recv()
            sib_copy(1 - hs, i, share_of(i)).start()

    with jax.named_scope("s_gated"):
        loads[0].wait()
        loads[1].wait()

        def gated(b, carry):
            rows = pl.ds(pl.multiple_of(b * 128, 128), 128)
            wide = val[rows, :].astype(f32) * jax.nn.sigmoid(gat[rows, :].astype(f32))
            pad[pl.ds(pl.multiple_of(HALO + b * 128, 32), 128), :] = wide.astype(bf16).astype(f32)
            return carry

        lax.fori_loop(0, 8, gated, 0)
        halo_out[...] = pad[1024 : 1024 + HALO, :].astype(bf16)

        halo = pltpu.make_async_remote_copy(
            src_ref=halo_out, dst_ref=halo_in, send_sem=halo_sem.at[0], recv_sem=halo_sem.at[1],
            device_id=((ep + 1) % 64, y), device_id_type=MESH,
        )
    with jax.named_scope("s_route"):
        tokens = xn.shape[0]
        loads[8].wait()
        loads[9].wait()
        first, second = experts[0:1, :], experts[1:2, :]
        ids = lax.broadcasted_iota(jnp.int32, (64, tokens), 0)
        hit0, hit1 = ids == first, ids == second
        both = jnp.where(hit0 | hit1, 1.0, 0.0).astype(bf16)
        row_t = lax.broadcasted_iota(jnp.int32, (tokens, tokens), 0)
        col_t = lax.broadcasted_iota(jnp.int32, (tokens, tokens), 1)
        earlier = jnp.where(row_t < col_t, 1.0, 0.0).astype(bf16)
        counts = jnp.dot(both, earlier, preferred_element_type=f32)
        slot0 = slot_of(first, jnp.sum(jnp.where(hit0, counts, 0.0), axis=0, keepdims=True), z, c)
        slot1 = slot_of(second, jnp.sum(jnp.where(hit1, counts, 0.0), axis=0, keepdims=True), z, c)

    with jax.named_scope("s_norm"):
        loads[2].wait()
        loads[7].wait()

        def norm(b, carry):
            rows = pl.ds(pl.multiple_of(b * 64, 64), 64)
            wide = xn[rows, :].astype(f32)
            square = jnp.mean(wide * wide, axis=-1, keepdims=True)
            xn[rows, :] = (wide * lax.rsqrt(square + 1e-06) * gain[...]).astype(bf16)
            return carry

        lax.fori_loop(0, 6, norm, 0)

    with jax.named_scope("s_barrier"):
        pl.semaphore_wait(barrier, len(peers))
    halo.start()
    step(0)

    def picked(base, count):
        at = (lax.broadcasted_iota(jnp.int32, (count, tokens), 0) + base).astype(f32)
        return jnp.where((at == slot0) | (at == slot1), 1.0, 0.0).astype(bf16)

    def gather(g, carry):
        choose = picked(g * 256, 256)

        def cols(q, carry):
            at = pl.ds(pl.multiple_of(q * 512, 512), 512)
            rows = jnp.dot(choose, xn[:, at], preferred_element_type=f32).astype(bf16)
            sm[pl.ds(g * 4, 4), :, at] = rows.reshape(4, 64, 512)
            return carry

        lax.fori_loop(0, 4, cols, 0)

        step(1 + g)
        return carry

    with jax.named_scope("s_gather"):
        lax.fori_loop(0, 4, gather, 0)
        choose = picked(1024, 128)

        def gather_rest(q, carry):
            at = pl.ds(pl.multiple_of(q * 512, 512), 512)
            rows = jnp.dot(choose, xn[:, at], preferred_element_type=f32)
            sr[:, :, at] = rows.reshape(16, 8, 512).astype(bf16)
            return carry

        lax.fori_loop(0, 4, gather_rest, 0)

    def block_at(k, sign):
        dx, dy = OFFSETS[k]
        xx, yy = (x + sign * dx + NX) % NX, (y + sign * dy + NY) % NY
        return xx * NY + yy, (device(z, xx, c), yy)

    def dispatch(k, part):
        block, peer = block_at(k, 1)
        if part < 2:
            src, dst = sm.at[block, pl.ds(part * 32, 32)], rm.at[me, pl.ds(part * 32, 32)]
        else:
            src, dst = sr.at[block], sx.at[me]
        return pltpu.make_async_remote_copy(
            src_ref=src, dst_ref=dst, send_sem=d_sent.at[part // 2], recv_sem=d_recv.at[part],
            device_id=peer, device_id_type=MESH,
        )

    with jax.named_scope("s_dispatch"):
        for part in range(3):
            for k in range(15):
                dispatch(k, part).start()
        rm[me] = sm[me]
        sx[me] = sr[me]

    with jax.named_scope("s_filter"):
        halo.wait_recv()
        pad[0:HALO, :] = jnp.where(ep > 0, halo_in[...].astype(f32), 0.0)
        loads[3].wait()

        def filter_block(b, carry):
            step(5 + 2 * b)
            step(6 + 2 * b)
            base = pl.multiple_of(b * 128, 128)
            window[...] = pad[pl.ds(base, 128 + HALO), :]
            total = None
            for k in range(KERNEL):
                low = HALO - KERNEL + 1 + k
                term = taps[k : k + 1, :] * window[low : low + 128, :]
                total = term if total is None else total + term
            pad[pl.ds(base, 128), :] = total
            stat[y, pl.ds(b, 1), :] = to_row(jnp.sum(total, axis=1, keepdims=True))
            stat[y, pl.ds(8 + b, 1), :] = to_row(jnp.sum(total * total, axis=1, keepdims=True))
            return carry

        lax.fori_loop(0, 8, filter_block, 0)

    def near(k):
        yy = (y + k) % NY
        return yy, (ep, yy)

    def stat_copy(k):
        return pltpu.make_async_remote_copy(
            src_ref=stat.at[y], dst_ref=stat.at[y], send_sem=stat_sem.at[0], recv_sem=stat_sem.at[1],
            device_id=near(k)[1], device_id_type=MESH,
        )

    def act_copy(k):
        yy, peer = near(k)
        return pltpu.make_async_remote_copy(
            src_ref=val.at[pl.ds(pl.multiple_of(yy * 256, 256), 256)], dst_ref=acts.at[y],
            send_sem=act_sem.at[0], recv_sem=act_sem.at[1], device_id=peer, device_id_type=MESH,
        )

    half = pl.ds(pl.multiple_of(c * 128, 128), 128)

    def cw_copy(k):
        return pltpu.make_async_remote_copy(
            src_ref=cw.at[y, half], dst_ref=cw.at[y, half], send_sem=cw_sem.at[0],
            recv_sem=cw_sem.at[1], device_id=near(k)[1], device_id_type=MESH,
        )

    def cs_copy(k):
        yy = (y + NY - k) % NY
        return pltpu.make_async_remote_copy(
            src_ref=cw.at[yy, half], dst_ref=cw.at[yy, half], send_sem=cs_sem.at[0],
            recv_sem=cs_sem.at[1], device_id=sibling, device_id_type=MESH,
        )

    loads[4].wait()
    for k in (1, 3, 2):
        stat_copy(k).start()
    for k in (1, 3, 2):
        cw_copy(k).start()

    def only_step(p, carry):
        step(p)
        return carry

    with jax.named_scope("s_pumps"):
        lax.fori_loop(21, START, only_step, 0)

    with jax.named_scope("s_wait_rows"):
        for part in range(2):
            arrived(rm.at[pl.ds(0, 15), pl.ds(0, 32)], d_recv.at[part])
        arrived(sx.at[pl.ds(0, 15)], d_recv.at[2])
        rx[...] = sx[...].astype(f32).reshape(128, 2048).astype(bf16)

    with jax.named_scope("s_wait_stat"):
        arrived(stat.at[pl.ds(0, 3)], stat_sem.at[1])
        loads[5].wait()
        loads[6].wait()
        stats[...] = (stat[0] + stat[1]) + (stat[2] + stat[3])

    order_in_rest = (lax.broadcasted_iota(jnp.int32, (128, 256), 0) % 8) // REM

    def of_half(half, s):
        e_low = jnp.where((dist == 0) & (c == 1), 1 - half, half)
        return jnp.where(s == 0, h_low, 1 - h_low), jnp.where(s == 0, e_low, 1 - e_low)

    def shared(half, low, count):
        others = jnp.where(dist == 0, 1 - c, jnp.where(c == 0, 1 - half, half))

        @pl.when((dist > 0) | (half == 0))
        def _():
            arrived(w.at[hs, 0, pl.ds(0, count * PIECE)], share_of(others * CHUNKS + low))

    def rows_at(half, s):
        return pl.ds(pl.multiple_of(half * 32 + s * MAIN, MAIN), MAIN)

    def gate_up(half, block, s):
        @pl.when(s == 0)
        def _():
            shared(half, block * 8, 8)

        h, e = of_half(half, s)
        rows = jnp.concatenate([rm[:, rows_at(half, s), :].reshape(256, 2048), rx[...]], axis=0)
        weight = w[h, e, pl.ds(pl.multiple_of(block * 2048, 2048), 2048), :]
        at = pl.ds(pl.multiple_of(block * 256, 256), 256)
        hidden[s, :, at] = jnp.dot(rows, weight, preferred_element_type=f32)

        @pl.when(block == 3)
        def _():
            inner[s] = (jax.nn.silu(hidden[s, :, 0:512]) * hidden[s, :, 512:1024]).astype(bf16)

    def down(half, block):
        shared(half, 32 + block * 2, 2)
        at = pl.ds(pl.multiple_of(block * 256, 256), 256)
        for s in range(2):
            h, e = of_half(half, s)
            weight = w[h, e, pl.ds(pl.multiple_of(8192 + block * 512, 512), 512), :]
            rows = jnp.dot(inner[s], weight, preferred_element_type=f32)
            rm[:, rows_at(half, s), at] = rows[:256].astype(bf16).reshape(16, MAIN, 256)
            here = order_in_rest == half * 2 + s
            orx[:, at] = jnp.where(here, rows[256:], orx[:, at])

    def activate(b):
        rows = pl.ds(pl.multiple_of(b * 128, 128), 128)
        center = to_column(stats[pl.ds(b, 1), :], 128) / CONV
        spread = to_column(stats[pl.ds(8 + b, 1), :], 128) / CONV - center * center
        normed = (pad[rows, :] - center) * lax.rsqrt(spread + 1e-05) * gain_c[...] + shift_c[...]
        val[rows, :] = jax.nn.silu(normed).astype(bf16)

    def phase0(p, carry):
        step(p)

        @pl.when(p < START + 8)
        def _():
            activate(p - START)
            gate_up(0, (p - START) // 2, (p - START) % 2)

        @pl.when(p == START + 8)
        def _():
            for k in (1, 3, 2):
                act_copy(k).start()
            acts[y] = val[my_cols, :]

        @pl.when(p >= START + 8)
        def _():
            down(0, p - START - 8)

        return carry

    with jax.named_scope("s_phase0"):
        lax.fori_loop(START, MIDDLE, phase0, 0)

    def back(k, main):
        block, peer = block_at(k, -1)
        if main:
            src, dst = rm.at[block, pl.ds(0, 32)], bm.at[me, pl.ds(0, 32)]
        else:
            src, dst = rest_out.at[0, block], rest_in.at[0, me]
        return pltpu.make_async_remote_copy(
            src_ref=src, dst_ref=dst, send_sem=r_sent.at[1 - main], recv_sem=r_recv.at[1 - main],
            device_id=peer, device_id_type=MESH,
        )

    low_rows = lax.broadcasted_iota(jnp.int32, (128, 256), 0) % 8 < 4

    def fold(half, block):
        left = slice(block * 256, block * 256 + 256)
        right = slice(1024 + block * 256, 1280 + block * 256)
        if half == 0:
            rows = jnp.where(low_rows, orx[:, left], pltpu.roll(orx[:, right], 4, 0))
        else:
            rows = jnp.where(low_rows, pltpu.roll(orx[:, left], 124, 0), orx[:, right])
        rest_out[half, :, :, left] = rows.reshape(16, 8, 256).astype(bf16)

    with jax.named_scope("s_back0"):
        for k in range(15):
            back(k, 1).start()
        for block in range(4):
            fold(0, block)
        for k in range(15):
            back(k, 0).start()
        bm[me, 0:32] = rm[me, 0:32]
        rest_in[0, me] = rest_out[0, me]

    def conv_part(q):
        at = pl.ds(pl.multiple_of(q * 512, 512), 512)
        total = None
        for b in range(4):
            term = jnp.dot(acts[b], cw[b, :, at], preferred_element_type=f32).astype(bf16).astype(f32)
            total = term if total is None else total + term
        conv_out[:, at] = total.astype(bf16)

    slot0_c, slot1_c = to_column(slot0, tokens), to_column(slot1, tokens)
    group = jax.nn.sigmoid(scores[0:1, :])
    weight0 = to_column(group * jax.nn.sigmoid(scores[1:2, :]), tokens)
    weight1 = to_column(group * jax.nn.sigmoid(-scores[1:2, :]), tokens)

    def chosen_main(slot, half):
        at = lax.broadcasted_iota(jnp.int32, (tokens, 512), 1)
        main = ((at // 32) * 64 + half * 32 + at % 32).astype(f32)
        return jnp.where(main == slot, 1.0, 0.0).astype(bf16)

    def chosen_rest(slot, half, right):
        at = lax.broadcasted_iota(jnp.int32, (tokens, 128), 1)
        name = 1024 + at + 4 * (half - right)
        here = (at % 8 >= 4) == (right > 0)
        return jnp.where(here & (name.astype(f32) == slot), 1.0, 0.0).astype(bf16)

    def rest_rows(half, at):
        return rest_in[half, :, :, at].astype(f32).reshape(128, 512).astype(bf16)

    def weighted(pick0, pick1, rows):
        return weight0 * jnp.dot(pick0, rows, preferred_element_type=f32) + weight1 * jnp.dot(
            pick1, rows, preferred_element_type=f32
        )

    def combine0(q):
        at = pl.ds(pl.multiple_of(q * 512, 512), 512)
        kept = pl.ds(pl.multiple_of(q % 2 * 512, 512), 512)
        rows = jnp.concatenate([bm[:, 0:32, at].reshape(512, 512), rest_rows(0, kept)], axis=0)
        picks = [
            jnp.concatenate([chosen_main(slot, 0), chosen_rest(slot, 0, q // 2)], axis=1)
            for slot in (slot0_c, slot1_c)
        ]
        hidden[q // 2, :, kept] = weighted(picks[0], picks[1], rows)

    def phase1(p, carry):
        step(p)

        @pl.when(p == MIDDLE + 2)
        def _():
            arrived(cw.at[pl.ds(0, 3), pl.ds(0, 128)], cw_sem.at[1])
            for k in (1, 3, 2):
                cs_copy(k).start()

        @pl.when(p == MIDDLE + 6)
        def _():
            arrived(acts.at[pl.ds(0, 3)], act_sem.at[1])
            arrived(cw.at[pl.ds(0, 3), pl.ds(0, 128)], cs_sem.at[1])

        @pl.when((p >= MIDDLE + 9) & (p < MIDDLE + 13))
        def _():
            conv_part(p - MIDDLE - 9)

        ready = p - FAR - CHUNKS + 1

        @pl.when((ready >= 8) & (ready < 34) & (ready % 8 < 2))
        def _():
            gate_up(1, ready // 8 - 1, ready % 8)

        @pl.when((ready >= 34) & (ready % 2 == 0))
        def _():
            down(1, (ready - 34) // 2)

        @pl.when(ready == 35)
        def _():
            arrived(bm.at[pl.ds(0, 15), pl.ds(0, 32)], r_recv.at[0])
            arrived(rest_in.at[0, pl.ds(0, 15)], r_recv.at[1])

        @pl.when((ready >= 35) & (ready % 2 == 1) & (ready < 43))
        def _():
            combine0((ready - 35) // 2)

        return carry

    def column(k, block, main):
        source, peer = block_at(k, -1)
        at = pl.ds((block if main else block - 4) * 256, 256)
        if main:
            src, dst = rm.at[source, pl.ds(32, 32), at], bm.at[me, pl.ds(32, 32), at]
        else:
            src, dst = rest_out.at[1, source, :, at], rest_in.at[1, me, :, at]
        return pltpu.make_async_remote_copy(
            src_ref=src, dst_ref=dst, send_sem=q_sent.at[1 - main],
            recv_sem=q_recv.at[block + 4 * (1 - main)], device_id=peer, device_id_type=MESH,
        )

    with jax.named_scope("s_phase1"):

        def tail(p, carry):
            phase1(p, carry)
            for block in range(8):

                @pl.when(p == LAST - 15 + 2 * block)
                def _(block=block):
                    at = slice(block * 256, block * 256 + 256)
                    for k in range(15):
                        column(k, block, 1).start()
                    bm[me, 32:64, at] = rm[me, 32:64, at]
                    if block >= 4:
                        fold(1, block - 4)
                        for k in range(15):
                            column(k, block, 0).start()
                        at = slice(block * 256 - 1024, block * 256 - 768)
                        rest_in[1, me, :, at] = rest_out[1, me, :, at]

            return carry

        lax.fori_loop(MIDDLE, LAST, tail, 0)

    with jax.named_scope("s_combine1"):
        pick0, pick1 = chosen_main(slot0_c, 1), chosen_main(slot1_c, 1)
        for q in range(4):
            for block in (2 * q, 2 * q + 1):
                at = slice(block * 256, block * 256 + 256)
                arrived(bm.at[pl.ds(0, 15), pl.ds(32, 32), pl.ds(block * 256, 256)], q_recv.at[block])
            at = slice(q * 512, q * 512 + 512)
            kept = slice(q % 2 * 512, q % 2 * 512 + 512)
            hidden[q // 2, :, kept] += weighted(pick0, pick1, bm[:, 32:64, at].reshape(512, 512))
        picks = [[chosen_rest(slot, 1, right) for slot in (slot0_c, slot1_c)] for right in range(2)]
        for part in range(2):
            for block in (2 * part, 2 * part + 1):
                arrived(rest_in.at[1, pl.ds(0, 15), :, pl.ds(block * 256, 256)], q_recv.at[8 + block])
            kept = slice(part * 512, part * 512 + 512)
            rows = rest_rows(1, kept)
            for right in range(2):
                total = hidden[right, :, kept] + weighted(picks[right][0], picks[right][1], rows)
                out[:, right * 1024 + part * 512 : right * 1024 + part * 512 + 512] = total.astype(bf16)

    with jax.named_scope("s_sent"):
        halo.wait_send()
        arrived(stat.at[pl.ds(0, 3)], stat_sem.at[0])
        arrived(acts.at[pl.ds(0, 3)], act_sem.at[0])
        arrived(cw.at[pl.ds(0, 3), pl.ds(0, 128)], cw_sem.at[0])
        arrived(cw.at[pl.ds(0, 3), pl.ds(0, 128)], cs_sem.at[0])
        arrived(sm.at[pl.ds(0, 15)], d_sent.at[0])
        arrived(sr.at[pl.ds(0, 15)], d_sent.at[1])
        arrived(bm.at[pl.ds(0, 15), pl.ds(0, 32)], r_sent.at[0])
        arrived(rest_in.at[0, pl.ds(0, 15)], r_sent.at[1])
        arrived(bm.at[pl.ds(0, 15), pl.ds(32, 32)], q_sent.at[0])
        arrived(rest_in.at[1, pl.ds(0, 15)], q_sent.at[1])

        @pl.when(dist < 3)
        def _():
            arrived(w.at[0], ring_sent)

        @pl.when(dist == 3)
        def _():
            arrived(w.at[0, 0], ring_sent)

        arrived(w.at[0], sib_sent)


def on_device(
    conv_value,
    conv_gate,
    depth_weight,
    norm_gain,
    norm_shift,
    conv_out_weight,
    moe_input,
    moe_gain,
    route_experts,
    route_scores,
    expert_gate,
    expert_up,
    expert_down,
):
    bf16, f32 = jnp.bfloat16, jnp.float32
    rows, width = moe_input.shape
    span, channels = conv_value.shape
    hbm = pl.BlockSpec(memory_space=pl.ANY)
    vmem = pl.BlockSpec(memory_space=pltpu.VMEM)
    dma = pltpu.SemaphoreType.DMA
    return pl.pallas_call(
        kernel,
        out_shape=(
            pltpu.VMEM((span // NY, width), bf16),
            pltpu.VMEM((rows, width), bf16),
        ),
        in_specs=[hbm] * 13,
        out_specs=(vmem, vmem),
        scratch_shapes=[
            pltpu.VMEM((2, 2, CHUNKS * PIECE, 256), bf16),
            pltpu.VMEM((rows, width), bf16),
            pltpu.VMEM((16, 64, width), bf16),
            pltpu.VMEM((16, 8, width), bf16),
            pltpu.VMEM((16, 64, width), bf16),
            pltpu.VMEM((16, 8, width), bf16),
            pltpu.VMEM((16, 64, width), bf16),
            pltpu.VMEM((2, 16, 8, width // 2), bf16),
            pltpu.VMEM((2, 16, 8, width // 2), bf16),
            pltpu.VMEM((2, 384, 1024), f32),
            pltpu.VMEM((2, 384, 512), bf16),
            pltpu.VMEM((128, width), bf16),
            pltpu.VMEM((128, width), f32),
            pltpu.VMEM((span, channels), bf16),
            pltpu.VMEM((span, channels), bf16),
            pltpu.VMEM((KERNEL, channels), f32),
            pltpu.VMEM((1, channels), f32),
            pltpu.VMEM((1, channels), f32),
            pltpu.VMEM((1, width), f32),
            pltpu.VMEM((2, rows), jnp.int32),
            pltpu.VMEM((2, rows), f32),
            pltpu.VMEM((HALO + span, channels), f32),
            pltpu.VMEM((NY, span // NY, channels), bf16),
            pltpu.VMEM((NY, channels, width), bf16),
            pltpu.VMEM((128 + HALO, channels), f32),
            pltpu.VMEM((HALO, channels), bf16),
            pltpu.VMEM((HALO, channels), bf16),
            pltpu.VMEM((NY, 16, 128), f32),
            pltpu.VMEM((16, 128), f32),
            dma((10,)),
            dma((6,)),
            dma((TOTAL,)),
            dma((24,)),
            dma,
            dma,
            dma((2,)),
            dma((3,)),
            dma((2,)),
            dma((2,)),
            dma((2,)),
            dma((12,)),
            dma((2,)),
            dma((2,)),
            dma((2,)),
            dma((2,)),
            dma((2,)),
        ],
        compiler_params=pltpu.CompilerParams(
            collective_id=0, has_side_effects=True, vmem_limit_bytes=62_000_000
        ),
        name="both",
    )(
        conv_value,
        conv_gate,
        depth_weight,
        norm_gain.reshape(1, CONV),
        norm_shift.reshape(1, CONV),
        conv_out_weight,
        moe_input,
        moe_gain.reshape(1, width),
        route_experts.T,
        route_scores.T,
        expert_gate,
        expert_up,
        expert_down,
    )


def solution(mesh):
    in_specs = (
        P("ep", "tp"),
        P("ep", "tp"),
        P(),
        P(),
        P(),
        P("tp", None),
        P(("ep", "tp"), None),
        P(),
        P(("ep", "tp"), None),
        P(("ep", "tp"), None),
        P("ep", None, None),
        P("ep", None, None),
        P("ep", None, None),
    )
    out_specs = (P(("ep", "tp"), None), P(("ep", "tp"), None))
    return jax.shard_map(
        on_device, mesh=mesh, in_specs=in_specs, out_specs=out_specs, check_vma=False
    )
```

```python
import jax
import jax.numpy as jnp
from jax import lax
from jax.experimental import pallas as pl
from jax.experimental.pallas import tpu as pltpu
from jax.sharding import PartitionSpec as P

MESH = pl.DeviceIdType.MESH
NZ, NX, NC, NY = 8, 4, 2, 4
CONV = 1024
KERNEL = 31
HALO = 32
MAIN = 16
REM = 2
PIECE = 256
CHUNKS = 48
TOTAL = 2 * CHUNKS
HOP = 4
FAR = 3 * HOP + 3
OUTER = 4 * HOP + 2
START = 50
MIDDLE = START + 16
LAST = TOTAL + FAR
OFFSETS = [
    (1, 0), (3, 0), (0, 1), (0, 3), (1, 1), (3, 3), (1, 3), (3, 1),
    (2, 0), (0, 2), (2, 2), (1, 2), (3, 2), (2, 1), (2, 3),
]


def slot_of(expert, rank, z, c):
    high = expert // 8
    yy = high % 4
    block = ((expert // 2) % 4) * NY + yy
    hops = (z - yy + 8) % 4
    below = ((z - hops - yy + 8) % 8) // 4
    other = jnp.where(high // 4 == below, 0, 1)
    flip = (other + jnp.where(hops == 0, c, 0)) % 2
    half = jnp.where(flip == 0, expert % 2, 1 - expert % 2)
    order = half * 2 + other
    main = (block * 64 + order * MAIN).astype(jnp.float32) + rank
    rest = (1024 + block * 8 + order * REM).astype(jnp.float32) + (rank - MAIN)
    return jnp.where(rank < MAIN, main, jnp.where(rank < MAIN + REM, rest, -1.0))


def eye(n):
    return lax.broadcasted_iota(jnp.int32, (n, n), 0) == lax.broadcasted_iota(jnp.int32, (n, n), 1)


def to_column(row, n):
    pieces = []
    for at in range(0, n, 128):
        spread = jnp.where(eye(128), row[:, at : at + 128], 0.0)
        pieces.append(jnp.sum(spread, axis=1, keepdims=True))
    return pieces[0] if len(pieces) == 1 else jnp.concatenate(pieces, axis=0)


def to_row(column):
    return jnp.sum(jnp.where(eye(128), column, 0.0), axis=0, keepdims=True)


def kernel(
    value_hbm, gate_hbm, taps_hbm, gain_c_hbm, shift_c_hbm, cw_hbm,
    x_hbm, gain_hbm, experts_hbm, scores_hbm, wg_hbm, wu_hbm, wd_hbm,
    conv_out, out,
    w, xn, sm, sr, rm, sx, bm, rest_out, rest_in, hidden, inner, rx, orx,
    val, gat, taps, gain_c, shift_c, gain, experts, scores,
    pad, acts, cw, window, halo_out, halo_in, stat, stats,
    load, native, avail, share, ring_sent, sib_sent,
    d_sent, d_recv, r_sent, r_recv, q_sent, q_recv,
    halo_sem, stat_sem, act_sem, cw_sem, cs_sem,
):
    f32, bf16 = jnp.float32, jnp.bfloat16
    ep = lax.axis_index("ep")
    y = lax.axis_index("tp")
    z, x, c = ep // 8, (ep // 2) % 4, ep % 2
    me = x * NY + y
    dd = (z - y + 8) % 4
    dist = jnp.where(c == 0, dd, (4 - dd) % 4)
    h_low = ((z - dd - y + 8) % 8) // 4
    hs = jnp.where((c == 0) | (dd == 0), h_low, 1 - h_low)

    def device(zz, xx, cc):
        return (zz * NX + xx) * NC + cc

    along = jnp.where(c == 0, (z + 1) % NZ, (z + NZ - 1) % NZ)
    ring_to = (device(along, x, c), y)
    sibling = (device(z, x, 1 - c), y)
    my_cols = pl.ds(pl.multiple_of(y * 256, 256), 256)

    loads = [
        pltpu.make_async_copy(value_hbm, val, load.at[0]),
        pltpu.make_async_copy(gate_hbm, gat, load.at[1]),
        pltpu.make_async_copy(x_hbm, xn, load.at[2]),
        pltpu.make_async_copy(taps_hbm.at[:, my_cols], taps, load.at[3]),
        pltpu.make_async_copy(cw_hbm, cw.at[y], load.at[4]),
        pltpu.make_async_copy(gain_c_hbm.at[:, my_cols], gain_c, load.at[5]),
        pltpu.make_async_copy(shift_c_hbm.at[:, my_cols], shift_c, load.at[6]),
        pltpu.make_async_copy(gain_hbm, gain, load.at[7]),
        pltpu.make_async_copy(experts_hbm, experts, load.at[8]),
        pltpu.make_async_copy(scores_hbm, scores, load.at[9]),
    ]

    @pl.when(dist == 0)
    def _():
        for i in range(CHUNKS):
            ref = wg_hbm if i < 16 else wu_hbm if i < 32 else wd_hbm
            block, row = (i // 8 % 2, i % 8) if i < 32 else ((i - 32) // 2, i % 2)
            pltpu.make_async_copy(
                ref.at[0, pl.ds(row * PIECE, PIECE), pl.ds(block * 256, 256)],
                w.at[hs, c, pl.ds(i * PIECE, PIECE)],
                native.at[i // 8],
            ).start()

    for copy in loads:
        copy.start()

    barrier = pltpu.get_barrier_semaphore()
    peers = [(device(z, (x + dx) % NX, c), (y + dy) % NY) for dx, dy in OFFSETS]
    peers += [(device((z + 1) % NZ, x, c), y), (device((z + NZ - 1) % NZ, x, c), y), sibling]
    peers += [((ep + 1) % 64, y), ((ep + 63) % 64, y)]
    for peer in peers:
        pl.semaphore_signal(barrier, inc=1, device_id=peer, device_id_type=MESH)

    def arrived(ref, sem):
        pltpu.make_async_copy(ref, ref, sem).wait()

    def piece(h, i):
        return w.at[h, i // CHUNKS, pl.ds(pl.multiple_of(i % CHUNKS * PIECE, PIECE), PIECE)]

    def ring_copy(i):
        return pltpu.make_async_remote_copy(
            src_ref=piece(hs, i), dst_ref=piece(hs, i), send_sem=ring_sent, recv_sem=avail.at[i],
            device_id=ring_to, device_id_type=MESH,
        )

    def sib_copy(h, i, sem):
        return pltpu.make_async_remote_copy(
            src_ref=piece(h, i), dst_ref=piece(h, i), send_sem=sib_sent, recv_sem=sem,
            device_id=sibling, device_id_type=MESH,
        )

    def share_of(i):
        j = i % CHUNKS
        return share.at[i // CHUNKS * 12 + jnp.where(j < 32, j // 8, 4 + (j - 32) // 2)]

    def expert_at(n):
        return jnp.where(c == 0, n, (n + CHUNKS) % TOTAL)

    def own(n):
        i = expert_at(n)
        mine = (dist == 0) & (i // CHUNKS == c)

        @pl.when(mine & (i % 8 == 0))
        def _():
            arrived(w.at[hs, c, pl.ds(0, 8 * PIECE)], native.at[i % CHUNKS // 8])

        @pl.when(jnp.logical_not(mine))
        def _():
            ring_copy(i).wait_recv()

        @pl.when((dist < 3) | (n < CHUNKS))
        def _():
            ring_copy(i).start()

        @pl.when(dist > 0)
        def _():
            sib_copy(hs, i, share_of(i)).start()

        @pl.when(mine)
        def _():
            sib_copy(hs, i, avail.at[i]).start()

    def step(p):
        n = p - HOP * dist
        m = p - OUTER

        @pl.when((n >= 0) & (n < TOTAL))
        def _():
            own(n)

        @pl.when((dist == 0) & (m >= 0) & (m < CHUNKS))
        def _():
            i = expert_at(m)
            ring_copy(i).wait_recv()
            sib_copy(1 - hs, i, share_of(i)).start()

    with jax.named_scope("s_gated"):
        loads[0].wait()
        loads[1].wait()

        def gated(b, carry):
            rows = pl.ds(pl.multiple_of(b * 128, 128), 128)
            wide = val[rows, :].astype(f32) * jax.nn.sigmoid(gat[rows, :].astype(f32))
            pad[pl.ds(pl.multiple_of(HALO + b * 128, 32), 128), :] = wide.astype(bf16).astype(f32)
            return carry

        lax.fori_loop(0, 8, gated, 0)
        halo_out[...] = pad[1024 : 1024 + HALO, :].astype(bf16)

        halo = pltpu.make_async_remote_copy(
            src_ref=halo_out, dst_ref=halo_in, send_sem=halo_sem.at[0], recv_sem=halo_sem.at[1],
            device_id=((ep + 1) % 64, y), device_id_type=MESH,
        )
    with jax.named_scope("s_route"):
        tokens = xn.shape[0]
        loads[8].wait()
        loads[9].wait()
        first, second = experts[0:1, :], experts[1:2, :]
        ids = lax.broadcasted_iota(jnp.int32, (64, tokens), 0)
        hit0, hit1 = ids == first, ids == second
        both = jnp.where(hit0 | hit1, 1.0, 0.0).astype(bf16)
        row_t = lax.broadcasted_iota(jnp.int32, (tokens, tokens), 0)
        col_t = lax.broadcasted_iota(jnp.int32, (tokens, tokens), 1)
        earlier = jnp.where(row_t < col_t, 1.0, 0.0).astype(bf16)
        counts = jnp.dot(both, earlier, preferred_element_type=f32)
        slot0 = slot_of(first, jnp.sum(jnp.where(hit0, counts, 0.0), axis=0, keepdims=True), z, c)
        slot1 = slot_of(second, jnp.sum(jnp.where(hit1, counts, 0.0), axis=0, keepdims=True), z, c)

    with jax.named_scope("s_norm"):
        loads[2].wait()
        loads[7].wait()

        def norm(b, carry):
            rows = pl.ds(pl.multiple_of(b * 64, 64), 64)
            wide = xn[rows, :].astype(f32)
            square = jnp.mean(wide * wide, axis=-1, keepdims=True)
            xn[rows, :] = (wide * lax.rsqrt(square + 1e-06) * gain[...]).astype(bf16)
            return carry

        lax.fori_loop(0, 6, norm, 0)

    with jax.named_scope("s_barrier"):
        pl.semaphore_wait(barrier, len(peers))
    halo.start()
    step(0)

    def picked(base, count):
        at = (lax.broadcasted_iota(jnp.int32, (count, tokens), 0) + base).astype(f32)
        return jnp.where((at == slot0) | (at == slot1), 1.0, 0.0).astype(bf16)

    def gather(g, carry):
        choose = picked(g * 256, 256)

        def cols(q, carry):
            at = pl.ds(pl.multiple_of(q * 512, 512), 512)
            rows = jnp.dot(choose, xn[:, at], preferred_element_type=f32).astype(bf16)
            sm[pl.ds(g * 4, 4), :, at] = rows.reshape(4, 64, 512)
            return carry

        lax.fori_loop(0, 4, cols, 0)

        step(1 + g)
        return carry

    with jax.named_scope("s_gather"):
        lax.fori_loop(0, 4, gather, 0)
        choose = picked(1024, 128)

        def gather_rest(q, carry):
            at = pl.ds(pl.multiple_of(q * 512, 512), 512)
            rows = jnp.dot(choose, xn[:, at], preferred_element_type=f32)
            sr[:, :, at] = rows.reshape(16, 8, 512).astype(bf16)
            return carry

        lax.fori_loop(0, 4, gather_rest, 0)

    def block_at(k, sign):
        dx, dy = OFFSETS[k]
        xx, yy = (x + sign * dx + NX) % NX, (y + sign * dy + NY) % NY
        return xx * NY + yy, (device(z, xx, c), yy)

    def dispatch(k, part):
        block, peer = block_at(k, 1)
        if part < 2:
            src, dst = sm.at[block, pl.ds(part * 32, 32)], rm.at[me, pl.ds(part * 32, 32)]
        else:
            src, dst = sr.at[block], sx.at[me]
        return pltpu.make_async_remote_copy(
            src_ref=src, dst_ref=dst, send_sem=d_sent.at[part // 2], recv_sem=d_recv.at[part],
            device_id=peer, device_id_type=MESH,
        )

    with jax.named_scope("s_dispatch"):
        for part in range(3):
            for k in range(15):
                dispatch(k, part).start()
        rm[me] = sm[me]
        sx[me] = sr[me]

    with jax.named_scope("s_filter"):
        halo.wait_recv()
        pad[0:HALO, :] = jnp.where(ep > 0, halo_in[...].astype(f32), 0.0)
        loads[3].wait()

        def filter_block(b, carry):
            step(5 + 2 * b)
            step(6 + 2 * b)
            base = pl.multiple_of(b * 128, 128)
            window[...] = pad[pl.ds(base, 128 + HALO), :]
            total = None
            for k in range(KERNEL):
                low = HALO - KERNEL + 1 + k
                term = taps[k : k + 1, :] * window[low : low + 128, :]
                total = term if total is None else total + term
            pad[pl.ds(base, 128), :] = total
            stat[y, pl.ds(b, 1), :] = to_row(jnp.sum(total, axis=1, keepdims=True))
            stat[y, pl.ds(8 + b, 1), :] = to_row(jnp.sum(total * total, axis=1, keepdims=True))
            return carry

        lax.fori_loop(0, 8, filter_block, 0)

    def near(k):
        yy = (y + k) % NY
        return yy, (ep, yy)

    def stat_copy(k):
        return pltpu.make_async_remote_copy(
            src_ref=stat.at[y], dst_ref=stat.at[y], send_sem=stat_sem.at[0], recv_sem=stat_sem.at[1],
            device_id=near(k)[1], device_id_type=MESH,
        )

    def act_copy(k):
        yy, peer = near(k)
        return pltpu.make_async_remote_copy(
            src_ref=val.at[pl.ds(pl.multiple_of(yy * 256, 256), 256)], dst_ref=acts.at[y],
            send_sem=act_sem.at[0], recv_sem=act_sem.at[1], device_id=peer, device_id_type=MESH,
        )

    half = pl.ds(pl.multiple_of(c * 128, 128), 128)

    def cw_copy(k):
        return pltpu.make_async_remote_copy(
            src_ref=cw.at[y, half], dst_ref=cw.at[y, half], send_sem=cw_sem.at[0],
            recv_sem=cw_sem.at[1], device_id=near(k)[1], device_id_type=MESH,
        )

    def cs_copy(k):
        yy = (y + NY - k) % NY
        return pltpu.make_async_remote_copy(
            src_ref=cw.at[yy, half], dst_ref=cw.at[yy, half], send_sem=cs_sem.at[0],
            recv_sem=cs_sem.at[1], device_id=sibling, device_id_type=MESH,
        )

    loads[4].wait()
    for k in (1, 3, 2):
        stat_copy(k).start()
    for k in (1, 3, 2):
        cw_copy(k).start()

    def only_step(p, carry):
        step(p)
        return carry

    with jax.named_scope("s_pumps"):
        lax.fori_loop(21, START, only_step, 0)

    with jax.named_scope("s_wait_rows"):
        for part in range(2):
            arrived(rm.at[pl.ds(0, 15), pl.ds(0, 32)], d_recv.at[part])
        arrived(sx.at[pl.ds(0, 15)], d_recv.at[2])
        rx[...] = sx[...].astype(f32).reshape(128, 2048).astype(bf16)

    with jax.named_scope("s_wait_stat"):
        arrived(stat.at[pl.ds(0, 3)], stat_sem.at[1])
        loads[5].wait()
        loads[6].wait()
        stats[...] = (stat[0] + stat[1]) + (stat[2] + stat[3])

    order_in_rest = (lax.broadcasted_iota(jnp.int32, (128, 256), 0) % 8) // REM

    def of_half(half, s):
        e_low = jnp.where((dist == 0) & (c == 1), 1 - half, half)
        return jnp.where(s == 0, h_low, 1 - h_low), jnp.where(s == 0, e_low, 1 - e_low)

    def shared(half, s, low, count):
        e = of_half(half, s)[1]

        @pl.when(jnp.where(dist > 0, s != c, (s == 1) & (half == 0)))
        def _():
            arrived(w.at[hs, 0, pl.ds(0, count * PIECE)], share_of(e * CHUNKS + low))

    def rows_at(half, s):
        return pl.ds(pl.multiple_of(half * 32 + s * MAIN, MAIN), MAIN)

    def gate_up(half, block, s):
        shared(half, s, block * 8, 8)
        h, e = of_half(half, s)
        rows = jnp.concatenate([rm[:, rows_at(half, s), :].reshape(256, 2048), rx[...]], axis=0)
        weight = w[h, e, pl.ds(pl.multiple_of(block * 2048, 2048), 2048), :]
        at = pl.ds(pl.multiple_of(block * 256, 256), 256)
        hidden[s, :, at] = jnp.dot(rows, weight, preferred_element_type=f32)

        @pl.when(block == 3)
        def _():
            inner[s] = (jax.nn.silu(hidden[s, :, 0:512]) * hidden[s, :, 512:1024]).astype(bf16)

    def down(half, block, s):
        shared(half, s, 32 + block * 2, 2)
        at = pl.ds(pl.multiple_of(block * 256, 256), 256)
        h, e = of_half(half, s)
        weight = w[h, e, pl.ds(pl.multiple_of(8192 + block * 512, 512), 512), :]
        rows = jnp.dot(inner[s], weight, preferred_element_type=f32)
        rm[:, rows_at(half, s), at] = rows[:256].astype(bf16).reshape(16, MAIN, 256)
        here = order_in_rest == half * 2 + s
        orx[:, at] = jnp.where(here, rows[256:], orx[:, at])

    def activate(b):
        rows = pl.ds(pl.multiple_of(b * 128, 128), 128)
        center = to_column(stats[pl.ds(b, 1), :], 128) / CONV
        spread = to_column(stats[pl.ds(8 + b, 1), :], 128) / CONV - center * center
        normed = (pad[rows, :] - center) * lax.rsqrt(spread + 1e-05) * gain_c[...] + shift_c[...]
        val[rows, :] = jax.nn.silu(normed).astype(bf16)

    def phase0(p, carry):
        step(p)

        @pl.when(p < START + 8)
        def _():
            activate(p - START)
            gate_up(0, (p - START) // 2, (p - START) % 2)

        @pl.when(p == START + 8)
        def _():
            for k in (1, 3, 2):
                act_copy(k).start()
            acts[y] = val[my_cols, :]

        @pl.when(p >= START + 8)
        def _():
            for s in range(2):
                down(0, p - START - 8, s)

        return carry

    with jax.named_scope("s_phase0"):
        lax.fori_loop(START, MIDDLE, phase0, 0)

    def back(k, main):
        block, peer = block_at(k, -1)
        if main:
            src, dst = rm.at[block, pl.ds(0, 32)], bm.at[me, pl.ds(0, 32)]
        else:
            src, dst = rest_out.at[0, block], rest_in.at[0, me]
        return pltpu.make_async_remote_copy(
            src_ref=src, dst_ref=dst, send_sem=r_sent.at[1 - main], recv_sem=r_recv.at[1 - main],
            device_id=peer, device_id_type=MESH,
        )

    low_rows = lax.broadcasted_iota(jnp.int32, (128, 256), 0) % 8 < 4

    def fold(half, block):
        left = slice(block * 256, block * 256 + 256)
        right = slice(1024 + block * 256, 1280 + block * 256)
        if half == 0:
            rows = jnp.where(low_rows, orx[:, left], pltpu.roll(orx[:, right], 4, 0))
        else:
            rows = jnp.where(low_rows, pltpu.roll(orx[:, left], 124, 0), orx[:, right])
        rest_out[half, :, :, left] = rows.reshape(16, 8, 256).astype(bf16)

    with jax.named_scope("s_back0"):
        for k in range(15):
            back(k, 1).start()
        for block in range(4):
            fold(0, block)
        for k in range(15):
            back(k, 0).start()
        bm[me, 0:32] = rm[me, 0:32]
        rest_in[0, me] = rest_out[0, me]

    def conv_part(q):
        at = pl.ds(pl.multiple_of(q * 512, 512), 512)
        total = None
        for b in range(4):
            term = jnp.dot(acts[b], cw[b, :, at], preferred_element_type=f32).astype(bf16).astype(f32)
            total = term if total is None else total + term
        conv_out[:, at] = total.astype(bf16)

    slot0_c, slot1_c = to_column(slot0, tokens), to_column(slot1, tokens)
    group = jax.nn.sigmoid(scores[0:1, :])
    weight0 = to_column(group * jax.nn.sigmoid(scores[1:2, :]), tokens)
    weight1 = to_column(group * jax.nn.sigmoid(-scores[1:2, :]), tokens)

    def chosen_main(slot, half):
        at = lax.broadcasted_iota(jnp.int32, (tokens, 512), 1)
        main = ((at // 32) * 64 + half * 32 + at % 32).astype(f32)
        return jnp.where(main == slot, 1.0, 0.0).astype(bf16)

    def chosen_rest(slot, half, right):
        at = lax.broadcasted_iota(jnp.int32, (tokens, 128), 1)
        name = 1024 + at + 4 * (half - right)
        here = (at % 8 >= 4) == (right > 0)
        return jnp.where(here & (name.astype(f32) == slot), 1.0, 0.0).astype(bf16)

    def rest_rows(half, at):
        return rest_in[half, :, :, at].astype(f32).reshape(128, 512).astype(bf16)

    def weighted(pick0, pick1, rows):
        return weight0 * jnp.dot(pick0, rows, preferred_element_type=f32) + weight1 * jnp.dot(
            pick1, rows, preferred_element_type=f32
        )

    def combine0(q):
        at = pl.ds(pl.multiple_of(q * 512, 512), 512)
        kept = pl.ds(pl.multiple_of(q % 2 * 512, 512), 512)
        rows = jnp.concatenate([bm[:, 0:32, at].reshape(512, 512), rest_rows(0, kept)], axis=0)
        picks = [
            jnp.concatenate([chosen_main(slot, 0), chosen_rest(slot, 0, q // 2)], axis=1)
            for slot in (slot0_c, slot1_c)
        ]
        hidden[q // 2, :, kept] = weighted(picks[0], picks[1], rows)

    def column(k, q, s):
        source, peer = block_at(k, -1)
        at = pl.ds(pl.multiple_of(q * 512, 512), 512)
        rows = pl.ds(32 + s * MAIN, MAIN)
        return pltpu.make_async_remote_copy(
            src_ref=rm.at[source, rows, at], dst_ref=bm.at[me, rows, at], send_sem=q_sent.at[0],
            recv_sem=q_recv.at[s * 4 + q], device_id=peer, device_id_type=MESH,
        )

    def rest_column(k, q):
        source, peer = block_at(k, -1)
        at = pl.ds(q * 512, 512)
        return pltpu.make_async_remote_copy(
            src_ref=rest_out.at[1, source, :, at], dst_ref=rest_in.at[1, me, :, at],
            send_sem=q_sent.at[1], recv_sem=q_recv.at[8 + q], device_id=peer, device_id_type=MESH,
        )

    def leave(q, s):
        at = pl.ds(pl.multiple_of(q * 512, 512), 512)
        rows = pl.ds(32 + s * MAIN, MAIN)
        for k in range(15):
            column(k, q, s).start()
        bm[me, rows, at] = rm[me, rows, at]

    def rest_leave(q):
        fold(1, 2 * q)
        fold(1, 2 * q + 1)
        for k in range(15):
            rest_column(k, q).start()
        at = slice(q * 512, q * 512 + 512)
        rest_in[1, me, :, at] = rest_out[1, me, :, at]

    def phase1(p, carry):
        step(p)

        @pl.when(p == MIDDLE + 14)
        def _():
            arrived(cw.at[pl.ds(0, 3), pl.ds(0, 128)], cw_sem.at[1])
            for k in (1, 3, 2):
                cs_copy(k).start()

        @pl.when(p == MIDDLE + 20)
        def _():
            arrived(acts.at[pl.ds(0, 3)], act_sem.at[1])
            arrived(cw.at[pl.ds(0, 3), pl.ds(0, 128)], cs_sem.at[1])

        @pl.when((p >= MIDDLE + 20) & (p < MIDDLE + 24))
        def _():
            conv_part(p - MIDDLE - 20)

        ready = p - FAR - CHUNKS + 1

        for s in range(2):
            handed = jnp.where(c == s, HOP * dist, HOP * (4 - dist) + 3)
            lag = jnp.where(dist == 0, 0, handed)

            def pieces(p, lag=lag):
                return jnp.minimum(2 * (p - MIDDLE), p - lag - CHUNKS + 1)

            old, new = pieces(p - 1), pieces(p)

            @pl.when((new >= 8) & (new < 34) & (new // 8 != old // 8))
            def _(s=s, new=new):
                gate_up(1, new // 8 - 1, s)

            @pl.when((new >= 34) & (new < 50) & (new // 2 != old // 2))
            def _(s=s, new=new):
                block = (new - 34) // 2
                down(1, block, s)

                @pl.when(block % 2 == 1)
                def _():
                    leave(block // 2, s)

        @pl.when(ready == 35)
        def _():
            arrived(bm.at[pl.ds(0, 15), pl.ds(0, 32)], r_recv.at[0])
            arrived(rest_in.at[0, pl.ds(0, 15)], r_recv.at[1])

        @pl.when((ready >= 35) & (ready % 2 == 1) & (ready < 43))
        def _():
            combine0((ready - 35) // 2)

        for q in range(2):

            @pl.when(p == LAST - 5 + 4 * q)
            def _(q=q):
                rest_leave(q)

        return carry

    with jax.named_scope("s_phase1"):
        lax.fori_loop(MIDDLE, LAST, phase1, 0)

    with jax.named_scope("s_combine1"):
        pick0, pick1 = chosen_main(slot0_c, 1), chosen_main(slot1_c, 1)
        for q in range(4):
            for s in range(2):
                arrived(
                    bm.at[pl.ds(0, 15), pl.ds(32 + s * MAIN, MAIN), pl.ds(q * 512, 512)],
                    q_recv.at[s * 4 + q],
                )
            at = slice(q * 512, q * 512 + 512)
            kept = slice(q % 2 * 512, q % 2 * 512 + 512)
            hidden[q // 2, :, kept] += weighted(pick0, pick1, bm[:, 32:64, at].reshape(512, 512))
        picks = [[chosen_rest(slot, 1, right) for slot in (slot0_c, slot1_c)] for right in range(2)]
        for part in range(2):
            arrived(rest_in.at[1, pl.ds(0, 15), :, pl.ds(part * 512, 512)], q_recv.at[8 + part])
            kept = slice(part * 512, part * 512 + 512)
            rows = rest_rows(1, kept)
            for right in range(2):
                total = hidden[right, :, kept] + weighted(picks[right][0], picks[right][1], rows)
                out[:, right * 1024 + part * 512 : right * 1024 + part * 512 + 512] = total.astype(bf16)

    with jax.named_scope("s_sent"):
        halo.wait_send()
        arrived(stat.at[pl.ds(0, 3)], stat_sem.at[0])
        arrived(acts.at[pl.ds(0, 3)], act_sem.at[0])
        arrived(cw.at[pl.ds(0, 3), pl.ds(0, 128)], cw_sem.at[0])
        arrived(cw.at[pl.ds(0, 3), pl.ds(0, 128)], cs_sem.at[0])
        arrived(sm.at[pl.ds(0, 15)], d_sent.at[0])
        arrived(sr.at[pl.ds(0, 15)], d_sent.at[1])
        arrived(bm.at[pl.ds(0, 15), pl.ds(0, 32)], r_sent.at[0])
        arrived(rest_in.at[0, pl.ds(0, 15)], r_sent.at[1])
        arrived(bm.at[pl.ds(0, 15), pl.ds(32, 32)], q_sent.at[0])
        arrived(rest_in.at[1, pl.ds(0, 15)], q_sent.at[1])

        @pl.when(dist < 3)
        def _():
            arrived(w.at[0], ring_sent)

        @pl.when(dist == 3)
        def _():
            arrived(w.at[0, 0], ring_sent)

        arrived(w.at[0], sib_sent)


def on_device(
    conv_value,
    conv_gate,
    depth_weight,
    norm_gain,
    norm_shift,
    conv_out_weight,
    moe_input,
    moe_gain,
    route_experts,
    route_scores,
    expert_gate,
    expert_up,
    expert_down,
):
    bf16, f32 = jnp.bfloat16, jnp.float32
    rows, width = moe_input.shape
    span, channels = conv_value.shape
    hbm = pl.BlockSpec(memory_space=pl.ANY)
    vmem = pl.BlockSpec(memory_space=pltpu.VMEM)
    dma = pltpu.SemaphoreType.DMA
    return pl.pallas_call(
        kernel,
        out_shape=(
            pltpu.VMEM((span // NY, width), bf16),
            pltpu.VMEM((rows, width), bf16),
        ),
        in_specs=[hbm] * 13,
        out_specs=(vmem, vmem),
        scratch_shapes=[
            pltpu.VMEM((2, 2, CHUNKS * PIECE, 256), bf16),
            pltpu.VMEM((rows, width), bf16),
            pltpu.VMEM((16, 64, width), bf16),
            pltpu.VMEM((16, 8, width), bf16),
            pltpu.VMEM((16, 64, width), bf16),
            pltpu.VMEM((16, 8, width), bf16),
            pltpu.VMEM((16, 64, width), bf16),
            pltpu.VMEM((2, 16, 8, width // 2), bf16),
            pltpu.VMEM((2, 16, 8, width // 2), bf16),
            pltpu.VMEM((2, 384, 1024), f32),
            pltpu.VMEM((2, 384, 512), bf16),
            pltpu.VMEM((128, width), bf16),
            pltpu.VMEM((128, width), f32),
            pltpu.VMEM((span, channels), bf16),
            pltpu.VMEM((span, channels), bf16),
            pltpu.VMEM((KERNEL, channels), f32),
            pltpu.VMEM((1, channels), f32),
            pltpu.VMEM((1, channels), f32),
            pltpu.VMEM((1, width), f32),
            pltpu.VMEM((2, rows), jnp.int32),
            pltpu.VMEM((2, rows), f32),
            pltpu.VMEM((HALO + span, channels), f32),
            pltpu.VMEM((NY, span // NY, channels), bf16),
            pltpu.VMEM((NY, channels, width), bf16),
            pltpu.VMEM((128 + HALO, channels), f32),
            pltpu.VMEM((HALO, channels), bf16),
            pltpu.VMEM((HALO, channels), bf16),
            pltpu.VMEM((NY, 16, 128), f32),
            pltpu.VMEM((16, 128), f32),
            dma((10,)),
            dma((6,)),
            dma((TOTAL,)),
            dma((24,)),
            dma,
            dma,
            dma((2,)),
            dma((3,)),
            dma((2,)),
            dma((2,)),
            dma((2,)),
            dma((10,)),
            dma((2,)),
            dma((2,)),
            dma((2,)),
            dma((2,)),
            dma((2,)),
        ],
        compiler_params=pltpu.CompilerParams(
            collective_id=0, has_side_effects=True, vmem_limit_bytes=62_000_000
        ),
        name="both",
    )(
        conv_value,
        conv_gate,
        depth_weight,
        norm_gain.reshape(1, CONV),
        norm_shift.reshape(1, CONV),
        conv_out_weight,
        moe_input,
        moe_gain.reshape(1, width),
        route_experts.T,
        route_scores.T,
        expert_gate,
        expert_up,
        expert_down,
    )


def solution(mesh):
    in_specs = (
        P("ep", "tp"),
        P("ep", "tp"),
        P(),
        P(),
        P(),
        P("tp", None),
        P(("ep", "tp"), None),
        P(),
        P(("ep", "tp"), None),
        P(("ep", "tp"), None),
        P("ep", None, None),
        P("ep", None, None),
        P("ep", None, None),
    )
    out_specs = (P(("ep", "tp"), None), P(("ep", "tp"), None))
    return jax.shard_map(
        on_device, mesh=mesh, in_specs=in_specs, out_specs=out_specs, check_vma=False
    )
```

```python
import jax
import jax.numpy as jnp
from jax import lax
from jax.experimental import pallas as pl
from jax.experimental.pallas import tpu as pltpu
from jax.sharding import PartitionSpec as P

MESH = pl.DeviceIdType.MESH
NZ, NX, NC, NY = 8, 4, 2, 4
CONV = 1024
KERNEL = 31
HALO = 32
MAIN = 16
REM = 2
PIECE = 256
CHUNKS = 48
TOTAL = 2 * CHUNKS
HOP = 2
AHEAD = 4
SHARE = 4
OUTER = 12
START = 48
MIDDLE = START + 16
LAST = TOTAL + 3 * HOP + SHARE
OFFSETS = [
    (1, 0), (3, 0), (0, 1), (0, 3), (1, 1), (3, 3), (1, 3), (3, 1),
    (2, 0), (0, 2), (2, 2), (1, 2), (3, 2), (2, 1), (2, 3),
]

TAIL_ORDER = tuple(reversed(range(15)))


def slot_of(expert, rank, z, c):
    high = expert // 8
    yy = high % 4
    block = ((expert // 2) % 4) * NY + yy
    hops = (z - yy + 8) % 4
    below = ((z - hops - yy + 8) % 8) // 4
    other = jnp.where(high // 4 == below, 0, 1)
    flip = (other + jnp.where(hops == 0, c, 0)) % 2
    half = jnp.where(flip == 0, expert % 2, 1 - expert % 2)
    order = half * 2 + other
    main = (block * 64 + order * MAIN).astype(jnp.float32) + rank
    rest = (1024 + block * 8 + order * REM).astype(jnp.float32) + (rank - MAIN)
    return jnp.where(rank < MAIN, main, jnp.where(rank < MAIN + REM, rest, -1.0))


def eye(n):
    return lax.broadcasted_iota(jnp.int32, (n, n), 0) == lax.broadcasted_iota(jnp.int32, (n, n), 1)


def to_column(row, n):
    pieces = []
    for at in range(0, n, 128):
        spread = jnp.where(eye(128), row[:, at : at + 128], 0.0)
        pieces.append(jnp.sum(spread, axis=1, keepdims=True))
    return pieces[0] if len(pieces) == 1 else jnp.concatenate(pieces, axis=0)


def to_row(column):
    return jnp.sum(jnp.where(eye(128), column, 0.0), axis=0, keepdims=True)


def kernel(
    value_hbm, gate_hbm, taps_hbm, gain_c_hbm, shift_c_hbm, cw_hbm,
    x_hbm, gain_hbm, experts_hbm, scores_hbm, wg_hbm, wu_hbm, wd_hbm,
    conv_out, out,
    w, xn, sm, sr, rm, sx, bm, rest_out, rest_in, hidden, sums, inner, rx, orx,
    val, gat, taps, gain_c, shift_c, gain, experts, scores,
    pad, acts, cw, window, halo_out, halo_in, stat, stats,
    load, native, avail, share, ring_sent, sib_sent,
    d_sent, d_recv, r_sent, r_recv, q_sent, q_recv,
    halo_sem, stat_sem, act_sem, cw_sem, cs_sem,
):
    f32, bf16 = jnp.float32, jnp.bfloat16
    ep = lax.axis_index("ep")
    y = lax.axis_index("tp")
    z, x, c = ep // 8, (ep // 2) % 4, ep % 2
    me = x * NY + y
    dd = (z - y + 8) % 4
    dist = jnp.where(c == 0, dd, (4 - dd) % 4)
    h_low = ((z - dd - y + 8) % 8) // 4
    hs = jnp.where((c == 0) | (dd == 0), h_low, 1 - h_low)

    def device(zz, xx, cc):
        return (zz * NX + xx) * NC + cc

    along = jnp.where(c == 0, (z + 1) % NZ, (z + NZ - 1) % NZ)
    ring_to = (device(along, x, c), y)
    sibling = (device(z, x, 1 - c), y)
    my_cols = pl.ds(pl.multiple_of(y * 256, 256), 256)

    loads = [
        pltpu.make_async_copy(value_hbm, val, load.at[0]),
        pltpu.make_async_copy(gate_hbm, gat, load.at[1]),
        pltpu.make_async_copy(x_hbm, xn, load.at[2]),
        pltpu.make_async_copy(taps_hbm.at[:, my_cols], taps, load.at[3]),
        pltpu.make_async_copy(cw_hbm, cw.at[y], load.at[4]),
        pltpu.make_async_copy(gain_c_hbm.at[:, my_cols], gain_c, load.at[5]),
        pltpu.make_async_copy(shift_c_hbm.at[:, my_cols], shift_c, load.at[6]),
        pltpu.make_async_copy(gain_hbm, gain, load.at[7]),
        pltpu.make_async_copy(experts_hbm, experts, load.at[8]),
        pltpu.make_async_copy(scores_hbm, scores, load.at[9]),
    ]

    @pl.when(dist == 0)
    def _():
        for i in range(CHUNKS):
            ref = wg_hbm if i < 16 else wu_hbm if i < 32 else wd_hbm
            block, row = (i // 8 % 2, i % 8) if i < 32 else ((i - 32) // 2, i % 2)
            pltpu.make_async_copy(
                ref.at[0, pl.ds(row * PIECE, PIECE), pl.ds(block * 256, 256)],
                w.at[hs, c, pl.ds(i * PIECE, PIECE)],
                native.at[i // 8],
            ).start()

    for copy in loads:
        copy.start()

    barrier = pltpu.get_barrier_semaphore()
    peers = [(device(z, (x + dx) % NX, c), (y + dy) % NY) for dx, dy in OFFSETS]
    peers += [(device((z + 1) % NZ, x, c), y), (device((z + NZ - 1) % NZ, x, c), y), sibling]
    peers += [((ep + 1) % 64, y), ((ep + 63) % 64, y)]
    for peer in peers:
        pl.semaphore_signal(barrier, inc=1, device_id=peer, device_id_type=MESH)

    def arrived(ref, sem):
        pltpu.make_async_copy(ref, ref, sem).wait()

    def piece(h, i):
        return w.at[h, i // CHUNKS, pl.ds(pl.multiple_of(i % CHUNKS * PIECE, PIECE), PIECE)]

    def ring_copy(i):
        return pltpu.make_async_remote_copy(
            src_ref=piece(hs, i), dst_ref=piece(hs, i), send_sem=ring_sent, recv_sem=avail.at[i],
            device_id=ring_to, device_id_type=MESH,
        )

    def sib_copy(h, i, sem):
        return pltpu.make_async_remote_copy(
            src_ref=piece(h, i), dst_ref=piece(h, i), send_sem=sib_sent, recv_sem=sem,
            device_id=sibling, device_id_type=MESH,
        )

    def share_of(i):
        j = i % CHUNKS
        return share.at[i // CHUNKS * 12 + jnp.where(j < 32, j // 8, 4 + (j - 32) // 2)]

    def expert_at(n):
        return jnp.where(c == 0, n, (n + CHUNKS) % TOTAL)

    def own(n):
        i = expert_at(n)
        mine = (dist == 0) & (i // CHUNKS == c)

        @pl.when(mine & (i % 8 == 0))
        def _():
            arrived(w.at[hs, c, pl.ds(0, 8 * PIECE)], native.at[i % CHUNKS // 8])

        @pl.when(jnp.logical_not(mine))
        def _():
            ring_copy(i).wait_recv()

        @pl.when((dist < 3) | (n < CHUNKS))
        def _():
            ring_copy(i).start()

        @pl.when(dist > 0)
        def _():
            sib_copy(hs, i, share_of(i)).start()

        @pl.when(mine)
        def _():
            sib_copy(hs, i, avail.at[i]).start()

    def step(p):
        n = p + jnp.where(dist == 0, AHEAD, -HOP * dist)
        m = p - OUTER

        @pl.when((n >= 0) & (n < TOTAL))
        def _():
            own(n)

        @pl.when((dist == 0) & (m >= 0) & (m < CHUNKS))
        def _():
            i = expert_at(m)
            ring_copy(i).wait_recv()
            sib_copy(1 - hs, i, share_of(i)).start()

    with jax.named_scope("s_gated"):
        loads[0].wait()
        loads[1].wait()

        def gated(b, carry):
            rows = pl.ds(pl.multiple_of(b * 128, 128), 128)
            wide = val[rows, :].astype(f32) * jax.nn.sigmoid(gat[rows, :].astype(f32))
            pad[pl.ds(pl.multiple_of(HALO + b * 128, 32), 128), :] = wide.astype(bf16).astype(f32)
            return carry

        lax.fori_loop(0, 8, gated, 0)
        halo_out[...] = pad[1024 : 1024 + HALO, :].astype(bf16)

        halo = pltpu.make_async_remote_copy(
            src_ref=halo_out, dst_ref=halo_in, send_sem=halo_sem.at[0], recv_sem=halo_sem.at[1],
            device_id=((ep + 1) % 64, y), device_id_type=MESH,
        )
    with jax.named_scope("s_route"):
        tokens = xn.shape[0]
        loads[8].wait()
        loads[9].wait()
        first, second = experts[0:1, :], experts[1:2, :]
        ids = lax.broadcasted_iota(jnp.int32, (64, tokens), 0)
        hit0, hit1 = ids == first, ids == second
        both = jnp.where(hit0 | hit1, 1.0, 0.0).astype(bf16)
        row_t = lax.broadcasted_iota(jnp.int32, (tokens, tokens), 0)
        col_t = lax.broadcasted_iota(jnp.int32, (tokens, tokens), 1)
        earlier = jnp.where(row_t < col_t, 1.0, 0.0).astype(bf16)
        counts = jnp.dot(both, earlier, preferred_element_type=f32)
        slot0 = slot_of(first, jnp.sum(jnp.where(hit0, counts, 0.0), axis=0, keepdims=True), z, c)
        slot1 = slot_of(second, jnp.sum(jnp.where(hit1, counts, 0.0), axis=0, keepdims=True), z, c)

    with jax.named_scope("s_norm"):
        loads[2].wait()
        loads[7].wait()

        def norm(b, carry):
            rows = pl.ds(pl.multiple_of(b * 64, 64), 64)
            wide = xn[rows, :].astype(f32)
            square = jnp.mean(wide * wide, axis=-1, keepdims=True)
            xn[rows, :] = (wide * lax.rsqrt(square + 1e-06) * gain[...]).astype(bf16)
            return carry

        lax.fori_loop(0, 6, norm, 0)

    with jax.named_scope("s_barrier"):
        pl.semaphore_wait(barrier, len(peers))
    halo.start()

    @pl.when(dist == 0)
    def _():
        for n in range(AHEAD):
            own(n)

    step(0)

    def picked(base, count):
        at = (lax.broadcasted_iota(jnp.int32, (count, tokens), 0) + base).astype(f32)
        return jnp.where((at == slot0) | (at == slot1), 1.0, 0.0).astype(bf16)

    def dispatch(xx, yy, part):
        block = xx * NY + yy
        if part < 2:
            src, dst = sm.at[block, pl.ds(part * 32, 32)], rm.at[me, pl.ds(part * 32, 32)]
        else:
            src, dst = sr.at[block], sx.at[me]
        return pltpu.make_async_remote_copy(
            src_ref=src, dst_ref=dst, send_sem=d_sent.at[part // 2], recv_sem=d_recv.at[part],
            device_id=(device(z, xx, c), yy), device_id_type=MESH,
        )

    def column_of(g):
        return (x + jnp.where(g == 0, 1, jnp.where(g == 1, 3, jnp.where(g == 2, 2, 0)))) % NX

    def send_group(g):
        xx = column_of(g)
        for part in range(2):
            for dy in (1, 3, 2, 0):
                copy = dispatch(xx, (y + dy) % NY, part)
                if dy > 0:
                    copy.start()
                else:

                    @pl.when(g < 3)
                    def _(copy=copy):
                        copy.start()

    def gather(g, carry):
        xx = column_of(g)
        choose = picked(xx * 256, 256)

        def cols(q, carry):
            at = pl.ds(pl.multiple_of(q * 512, 512), 512)
            rows = jnp.dot(choose, xn[:, at], preferred_element_type=f32).astype(bf16)
            sm[pl.ds(xx * 4, 4), :, at] = rows.reshape(4, 64, 512)
            return carry

        lax.fori_loop(0, 4, cols, 0)
        step(1 + g)

        @pl.when(g > 0)
        def _():
            send_group(g - 1)

        return carry

    with jax.named_scope("s_gather"):
        lax.fori_loop(0, 4, gather, 0)
        choose = picked(1024, 128)

        def gather_rest(q, carry):
            at = pl.ds(pl.multiple_of(q * 512, 512), 512)
            rows = jnp.dot(choose, xn[:, at], preferred_element_type=f32)
            sr[:, :, at] = rows.reshape(16, 8, 512).astype(bf16)
            return carry

        lax.fori_loop(0, 4, gather_rest, 0)

    def block_at(k, sign):
        dx, dy = OFFSETS[k]
        xx, yy = (x + sign * dx + NX) % NX, (y + sign * dy + NY) % NY
        return xx * NY + yy, (device(z, xx, c), yy)

    with jax.named_scope("s_dispatch"):
        send_group(3)
        for dx, dy in OFFSETS:
            dispatch((x + dx) % NX, (y + dy) % NY, 2).start()
        rm[me] = sm[me]
        sx[me] = sr[me]

    with jax.named_scope("s_filter"):
        halo.wait_recv()
        pad[0:HALO, :] = jnp.where(ep > 0, halo_in[...].astype(f32), 0.0)
        loads[3].wait()

        def filter_block(b, carry):
            step(5 + 2 * b)
            step(6 + 2 * b)
            base = pl.multiple_of(b * 128, 128)
            window[...] = pad[pl.ds(base, 128 + HALO), :]
            total = None
            for k in range(KERNEL):
                low = HALO - KERNEL + 1 + k
                term = taps[k : k + 1, :] * window[low : low + 128, :]
                total = term if total is None else total + term
            pad[pl.ds(base, 128), :] = total
            stat[y, pl.ds(b, 1), :] = to_row(jnp.sum(total, axis=1, keepdims=True))
            stat[y, pl.ds(8 + b, 1), :] = to_row(jnp.sum(total * total, axis=1, keepdims=True))
            return carry

        lax.fori_loop(0, 8, filter_block, 0)

    def near(k):
        yy = (y + k) % NY
        return yy, (ep, yy)

    def stat_copy(k):
        return pltpu.make_async_remote_copy(
            src_ref=stat.at[y], dst_ref=stat.at[y], send_sem=stat_sem.at[0], recv_sem=stat_sem.at[1],
            device_id=near(k)[1], device_id_type=MESH,
        )

    def act_copy(k):
        yy, peer = near(k)
        return pltpu.make_async_remote_copy(
            src_ref=val.at[pl.ds(pl.multiple_of(yy * 256, 256), 256)], dst_ref=acts.at[y],
            send_sem=act_sem.at[0], recv_sem=act_sem.at[1], device_id=peer, device_id_type=MESH,
        )

    half = pl.ds(pl.multiple_of(c * 128, 128), 128)

    def cw_copy(k):
        return pltpu.make_async_remote_copy(
            src_ref=cw.at[y, half], dst_ref=cw.at[y, half], send_sem=cw_sem.at[0],
            recv_sem=cw_sem.at[1], device_id=near(k)[1], device_id_type=MESH,
        )

    def cs_copy(k):
        yy = (y + NY - k) % NY
        return pltpu.make_async_remote_copy(
            src_ref=cw.at[yy, half], dst_ref=cw.at[yy, half], send_sem=cs_sem.at[0],
            recv_sem=cs_sem.at[1], device_id=sibling, device_id_type=MESH,
        )

    loads[4].wait()
    for k in (1, 3, 2):
        stat_copy(k).start()
    for k in (1, 3, 2):
        cw_copy(k).start()

    def only_step(p, carry):
        step(p)
        return carry

    with jax.named_scope("s_pumps"):
        lax.fori_loop(21, START, only_step, 0)

    with jax.named_scope("s_wait_rows"):
        for part in range(2):
            arrived(rm.at[pl.ds(0, 15), pl.ds(0, 32)], d_recv.at[part])
        arrived(sx.at[pl.ds(0, 15)], d_recv.at[2])
        rx[...] = sx[...].astype(f32).reshape(128, 2048).astype(bf16)

    with jax.named_scope("s_wait_stat"):
        arrived(stat.at[pl.ds(0, 3)], stat_sem.at[1])
        loads[5].wait()
        loads[6].wait()
        stats[...] = (stat[0] + stat[1]) + (stat[2] + stat[3])

    order_in_rest = (lax.broadcasted_iota(jnp.int32, (128, 256), 0) % 8) // REM

    def of_half(half, s):
        e_low = jnp.where((dist == 0) & (c == 1), 1 - half, half)
        return jnp.where(s == 0, h_low, 1 - h_low), jnp.where(s == 0, e_low, 1 - e_low)

    def shared(half, s, low, count):
        e = of_half(half, s)[1]

        @pl.when(jnp.where(dist > 0, s != c, (s == 1) & (half == 0)))
        def _():
            arrived(w.at[hs, 0, pl.ds(0, count * PIECE)], share_of(e * CHUNKS + low))

    def rows_at(half, s):
        return pl.ds(pl.multiple_of(half * 32 + s * MAIN, MAIN), MAIN)

    def gate_up(half, block, s):
        shared(half, s, block * 8, 8)
        h, e = of_half(half, s)
        rows = jnp.concatenate([rm[:, rows_at(half, s), :].reshape(256, 2048), rx[...]], axis=0)
        weight = w[h, e, pl.ds(pl.multiple_of(block * 2048, 2048), 2048), :]
        at = pl.ds(pl.multiple_of(block * 256, 256), 256)
        hidden[s, :, at] = jnp.dot(rows, weight, preferred_element_type=f32)

        @pl.when(block == 3)
        def _():
            inner[s] = (jax.nn.silu(hidden[s, :, 0:512]) * hidden[s, :, 512:1024]).astype(bf16)

    def down(half, block, s):
        shared(half, s, 32 + block * 2, 2)
        at = pl.ds(pl.multiple_of(block * 256, 256), 256)
        h, e = of_half(half, s)
        weight = w[h, e, pl.ds(pl.multiple_of(8192 + block * 512, 512), 512), :]
        rows = jnp.dot(inner[s], weight, preferred_element_type=f32)
        rm[:, rows_at(half, s), at] = rows[:256].astype(bf16).reshape(16, MAIN, 256)
        here = order_in_rest == half * 2 + s
        orx[:, at] = jnp.where(here, rows[256:], orx[:, at])

    def activate(b):
        rows = pl.ds(pl.multiple_of(b * 128, 128), 128)
        center = to_column(stats[pl.ds(b, 1), :], 128) / CONV
        spread = to_column(stats[pl.ds(8 + b, 1), :], 128) / CONV - center * center
        normed = (pad[rows, :] - center) * lax.rsqrt(spread + 1e-05) * gain_c[...] + shift_c[...]
        val[rows, :] = jax.nn.silu(normed).astype(bf16)

    def phase0(p):
        @pl.when(p < START + 8)
        def _():
            activate(p - START)

        @pl.when(p == START + 8)
        def _():
            for k in (1, 3, 2):
                act_copy(k).start()
            acts[y] = val[my_cols, :]

        q = p - START

        @pl.when((q >= 0) & (q < 8))
        def _():
            gate_up(0, q // 2, q % 2)

        @pl.when((q >= 8) & (q < 16))
        def _():
            for s in range(2):
                down(0, q - 8, s)

    def back(k, main):
        block, peer = block_at(k, -1)
        if main:
            src, dst = rm.at[block, pl.ds(0, 32)], bm.at[me, pl.ds(0, 32)]
        else:
            src, dst = rest_out.at[0, block], rest_in.at[0, me]
        return pltpu.make_async_remote_copy(
            src_ref=src, dst_ref=dst, send_sem=r_sent.at[1 - main], recv_sem=r_recv.at[1 - main],
            device_id=peer, device_id_type=MESH,
        )

    low_rows = lax.broadcasted_iota(jnp.int32, (128, 256), 0) % 8 < 4

    def fold(half, block):
        left = slice(block * 256, block * 256 + 256)
        right = slice(1024 + block * 256, 1280 + block * 256)
        if half == 0:
            rows = jnp.where(low_rows, orx[:, left], pltpu.roll(orx[:, right], 4, 0))
        else:
            rows = jnp.where(low_rows, pltpu.roll(orx[:, left], 124, 0), orx[:, right])
        rest_out[half, :, :, left] = rows.reshape(16, 8, 256).astype(bf16)

    def first_leave():
        for k in range(15):
            back(k, 1).start()
        for block in range(4):
            fold(0, block)
        for k in range(15):
            back(k, 0).start()
        bm[me, 0:32] = rm[me, 0:32]
        rest_in[0, me] = rest_out[0, me]

    def conv_part(q):
        at = pl.ds(pl.multiple_of(q * 512, 512), 512)
        total = None
        for b in range(4):
            term = jnp.dot(acts[b], cw[b, :, at], preferred_element_type=f32).astype(bf16).astype(f32)
            total = term if total is None else total + term
        conv_out[:, at] = total.astype(bf16)

    slot0_c, slot1_c = to_column(slot0, tokens), to_column(slot1, tokens)
    group = jax.nn.sigmoid(scores[0:1, :])
    weight0 = to_column(group * jax.nn.sigmoid(scores[1:2, :]), tokens)
    weight1 = to_column(group * jax.nn.sigmoid(-scores[1:2, :]), tokens)

    def chosen_main(slot, half):
        at = lax.broadcasted_iota(jnp.int32, (tokens, 512), 1)
        main = ((at // 32) * 64 + half * 32 + at % 32).astype(f32)
        return jnp.where(main == slot, 1.0, 0.0).astype(bf16)

    def chosen_rest(slot, half, right):
        at = lax.broadcasted_iota(jnp.int32, (tokens, 128), 1)
        name = 1024 + at + 4 * (half - right)
        here = (at % 8 >= 4) == (right > 0)
        return jnp.where(here & (name.astype(f32) == slot), 1.0, 0.0).astype(bf16)

    def rest_rows(half, at):
        return rest_in[half, :, :, at].astype(f32).reshape(128, 256).astype(bf16)

    def weighted(pick0, pick1, rows):
        return weight0 * jnp.dot(pick0, rows, preferred_element_type=f32) + weight1 * jnp.dot(
            pick1, rows, preferred_element_type=f32
        )

    def combine0(block):
        at = slice(block * 256, block * 256 + 256)
        folded = slice(block % 4 * 256, block % 4 * 256 + 256)
        rows = jnp.concatenate([bm[:, 0:32, at].reshape(512, 256), rest_rows(0, folded)], axis=0)
        picks = [
            jnp.concatenate([chosen_main(slot, 0), chosen_rest(slot, 0, block // 4)], axis=1)
            for slot in (slot0_c, slot1_c)
        ]
        sums[:, at] = weighted(picks[0], picks[1], rows)

    def column(k, block, s):
        source, peer = block_at(k, -1)
        at = pl.ds(pl.multiple_of(block * 256, 256), 256)
        rows = pl.ds(32 + s * MAIN, MAIN)
        return pltpu.make_async_remote_copy(
            src_ref=rm.at[source, rows, at], dst_ref=bm.at[me, rows, at], send_sem=q_sent.at[0],
            recv_sem=q_recv.at[block], device_id=peer, device_id_type=MESH,
        )

    def rest_column(k, block):
        source, peer = block_at(k, -1)
        at = pl.ds(block * 256, 256)
        return pltpu.make_async_remote_copy(
            src_ref=rest_out.at[1, source, :, at], dst_ref=rest_in.at[1, me, :, at],
            send_sem=q_sent.at[1], recv_sem=q_recv.at[8 + block], device_id=peer,
            device_id_type=MESH,
        )

    def leave(block, s):
        at = pl.ds(pl.multiple_of(block * 256, 256), 256)
        rows = pl.ds(32 + s * MAIN, MAIN)
        for k in TAIL_ORDER:
            column(k, block, s).start()
        bm[me, rows, at] = rm[me, rows, at]

    def rest_leave(block):
        fold(1, block)
        for k in TAIL_ORDER:
            rest_column(k, block).start()
        at = slice(block * 256, block * 256 + 256)
        rest_in[1, me, :, at] = rest_out[1, me, :, at]

    def phases(p, carry):
        step(p)
        phase0(p)

        @pl.when(p == MIDDLE)
        def _():
            first_leave()

        @pl.when(p == MIDDLE + 10)
        def _():
            arrived(cw.at[pl.ds(0, 3), pl.ds(0, 128)], cw_sem.at[1])
            for k in (1, 3, 2):
                cs_copy(k).start()

        @pl.when(p == MIDDLE + 18)
        def _():
            arrived(acts.at[pl.ds(0, 3)], act_sem.at[1])
            arrived(cw.at[pl.ds(0, 3), pl.ds(0, 128)], cs_sem.at[1])

        @pl.when((p >= MIDDLE + 18) & (p < MIDDLE + 22))
        def _():
            conv_part(p - MIDDLE - 18)

        there = []
        for s in range(2):
            handed = jnp.where(c == s, HOP * dist, HOP * (4 - dist) + SHARE)
            lag = jnp.where(dist == 0, -AHEAD, handed)

            def pieces(p, lag=lag):
                return jnp.minimum(2 * (p - MIDDLE), p - lag - CHUNKS + 1)

            old, new = pieces(p - 1), pieces(p)

            @pl.when((new >= 8) & (new < 34) & (new // 8 != old // 8))
            def _(s=s, new=new):
                gate_up(1, new // 8 - 1, s)

            @pl.when((new >= 34) & (new < 50) & (new // 2 != old // 2))
            def _(s=s, new=new):
                block = (new - 34) // 2
                down(1, block, s)
                leave(block, s)

            there.append((old, new))

        old, new = [jnp.minimum(there[0][i], there[1][i]) for i in range(2)]
        for block in range(4):
            due = 42 + 2 * block

            @pl.when((old < due) & (new >= due))
            def _(block=block):
                rest_leave(block)

        return carry

    with jax.named_scope("s_phase1"):
        lax.fori_loop(START, LAST, phases, 0)

    with jax.named_scope("s_combine0"):
        arrived(bm.at[pl.ds(0, 15), pl.ds(0, 32)], r_recv.at[0])
        arrived(rest_in.at[0, pl.ds(0, 15)], r_recv.at[1])
        for block in range(8):
            combine0(block)

    with jax.named_scope("s_combine1"):
        pick0, pick1 = chosen_main(slot0_c, 1), chosen_main(slot1_c, 1)
        picks = [[chosen_rest(slot, 1, right) for slot in (slot0_c, slot1_c)] for right in range(2)]
        for block in range(8):
            at = slice(block * 256, block * 256 + 256)
            arrived(bm.at[pl.ds(0, 15), pl.ds(32, 32), pl.ds(block * 256, 256)], q_recv.at[block])
            sums[:, at] += weighted(pick0, pick1, bm[:, 32:64, at].reshape(512, 256))
            if block >= 4:
                low = block * 256 - 1024
                arrived(rest_in.at[1, pl.ds(0, 15), :, pl.ds(low, 256)], q_recv.at[4 + block])
                rows = rest_rows(1, slice(low, low + 256))
                for right in range(2):
                    at = slice(low + right * 1024, low + right * 1024 + 256)
                    last = weighted(picks[right][0], picks[right][1], rows)
                    out[:, at] = (sums[:, at] + last).astype(bf16)

    with jax.named_scope("s_sent"):
        halo.wait_send()
        arrived(stat.at[pl.ds(0, 3)], stat_sem.at[0])
        arrived(acts.at[pl.ds(0, 3)], act_sem.at[0])
        arrived(cw.at[pl.ds(0, 3), pl.ds(0, 128)], cw_sem.at[0])
        arrived(cw.at[pl.ds(0, 3), pl.ds(0, 128)], cs_sem.at[0])
        arrived(sm.at[pl.ds(0, 15)], d_sent.at[0])
        arrived(sr.at[pl.ds(0, 15)], d_sent.at[1])
        arrived(bm.at[pl.ds(0, 15), pl.ds(0, 32)], r_sent.at[0])
        arrived(rest_in.at[0, pl.ds(0, 15)], r_sent.at[1])
        arrived(bm.at[pl.ds(0, 15), pl.ds(32, 32)], q_sent.at[0])
        arrived(rest_in.at[1, pl.ds(0, 15)], q_sent.at[1])

        @pl.when(dist < 3)
        def _():
            arrived(w.at[0], ring_sent)

        @pl.when(dist == 3)
        def _():
            arrived(w.at[0, 0], ring_sent)

        arrived(w.at[0], sib_sent)


def write_out(conv_ref, moe_ref, conv_out, moe_out, sems):
    copies = []
    for source, target in ((moe_ref, moe_out), (conv_ref, conv_out)):
        for low in range(0, source.shape[0], 128):
            rows = pl.ds(low, 128)
            copies.append(
                pltpu.make_async_copy(source.at[rows], target.at[rows], sems.at[len(copies)])
            )
            copies[-1].start()
    for copy in copies:
        copy.wait()


def on_device(
    conv_value,
    conv_gate,
    depth_weight,
    norm_gain,
    norm_shift,
    conv_out_weight,
    moe_input,
    moe_gain,
    route_experts,
    route_scores,
    expert_gate,
    expert_up,
    expert_down,
):
    bf16, f32 = jnp.bfloat16, jnp.float32
    rows, width = moe_input.shape
    span, channels = conv_value.shape
    hbm = pl.BlockSpec(memory_space=pl.ANY)
    vmem = pl.BlockSpec(memory_space=pltpu.VMEM)
    dma = pltpu.SemaphoreType.DMA
    both = pl.pallas_call(
        kernel,
        out_shape=(
            pltpu.VMEM((span // NY, width), bf16),
            pltpu.VMEM((rows, width), bf16),
        ),
        in_specs=[hbm] * 13,
        out_specs=(vmem, vmem),
        scratch_shapes=[
            pltpu.VMEM((2, 2, CHUNKS * PIECE, 256), bf16),
            pltpu.VMEM((rows, width), bf16),
            pltpu.VMEM((16, 64, width), bf16),
            pltpu.VMEM((16, 8, width), bf16),
            pltpu.VMEM((16, 64, width), bf16),
            pltpu.VMEM((16, 8, width), bf16),
            pltpu.VMEM((16, 64, width), bf16),
            pltpu.VMEM((2, 16, 8, width // 2), bf16),
            pltpu.VMEM((2, 16, 8, width // 2), bf16),
            pltpu.VMEM((2, 384, 1024), f32),
            pltpu.VMEM((rows, width), f32),
            pltpu.VMEM((2, 384, 512), bf16),
            pltpu.VMEM((128, width), bf16),
            pltpu.VMEM((128, width), f32),
            pltpu.VMEM((span, channels), bf16),
            pltpu.VMEM((span, channels), bf16),
            pltpu.VMEM((KERNEL, channels), f32),
            pltpu.VMEM((1, channels), f32),
            pltpu.VMEM((1, channels), f32),
            pltpu.VMEM((1, width), f32),
            pltpu.VMEM((2, rows), jnp.int32),
            pltpu.VMEM((2, rows), f32),
            pltpu.VMEM((HALO + span, channels), f32),
            pltpu.VMEM((NY, span // NY, channels), bf16),
            pltpu.VMEM((NY, channels, width), bf16),
            pltpu.VMEM((128 + HALO, channels), f32),
            pltpu.VMEM((HALO, channels), bf16),
            pltpu.VMEM((HALO, channels), bf16),
            pltpu.VMEM((NY, 16, 128), f32),
            pltpu.VMEM((16, 128), f32),
            dma((10,)),
            dma((6,)),
            dma((TOTAL,)),
            dma((24,)),
            dma,
            dma,
            dma((2,)),
            dma((3,)),
            dma((2,)),
            dma((2,)),
            dma((2,)),
            dma((12,)),
            dma((2,)),
            dma((2,)),
            dma((2,)),
            dma((2,)),
            dma((2,)),
        ],
        compiler_params=pltpu.CompilerParams(
            collective_id=0, has_side_effects=True, vmem_limit_bytes=64_300_000
        ),
        name="both",
    )(
        conv_value,
        conv_gate,
        depth_weight,
        norm_gain.reshape(1, CONV),
        norm_shift.reshape(1, CONV),
        conv_out_weight,
        moe_input,
        moe_gain.reshape(1, width),
        route_experts.T,
        route_scores.T,
        expert_gate,
        expert_up,
        expert_down,
    )
    outs = [jax.ShapeDtypeStruct(out.shape, out.dtype) for out in both]
    return pl.pallas_call(
        write_out,
        out_shape=tuple(outs),
        in_specs=[vmem, vmem],
        out_specs=(hbm, hbm),
        scratch_shapes=[dma((sum(out.shape[0] for out in outs) // 128,))],
        name="write_out",
    )(*(pltpu.with_memory_space_constraint(out, pltpu.VMEM) for out in both))


def solution(mesh):
    in_specs = (
        P("ep", "tp"),
        P("ep", "tp"),
        P(),
        P(),
        P(),
        P("tp", None),
        P(("ep", "tp"), None),
        P(),
        P(("ep", "tp"), None),
        P(("ep", "tp"), None),
        P("ep", None, None),
        P("ep", None, None),
        P("ep", None, None),
    )
    out_specs = (P(("ep", "tp"), None), P(("ep", "tp"), None))
    return jax.shard_map(
        on_device, mesh=mesh, in_specs=in_specs, out_specs=out_specs, check_vma=False
    )
```

```python
import jax
import jax.numpy as jnp
from jax import lax
from jax.experimental import pallas as pl
from jax.experimental.pallas import tpu as pltpu
from jax.sharding import PartitionSpec as P

MESH = pl.DeviceIdType.MESH
OUT_ROWS = 128
NZ, NX, NC, NY = 8, 4, 2, 4
CONV = 1024
KERNEL = 31
HALO = 32
MAIN = 16
REM = 2
PIECE = 256
CHUNKS = 48
TOTAL = 2 * CHUNKS
HOP = 2
AHEAD = 4
SHARE = 4
OUTER = 12
START = 48
MIDDLE = START + 16
LAST = TOTAL + 3 * HOP + SHARE
OFFSETS = [
    (1, 0), (3, 0), (0, 1), (0, 3), (1, 1), (3, 3), (1, 3), (3, 1),
    (2, 0), (0, 2), (2, 2), (1, 2), (3, 2), (2, 1), (2, 3),
]

TAIL_ORDER = tuple(reversed(range(15)))


def slot_of(expert, rank, z, c):
    high = expert // 8
    yy = high % 4
    block = ((expert // 2) % 4) * NY + yy
    hops = (z - yy + 8) % 4
    below = ((z - hops - yy + 8) % 8) // 4
    other = jnp.where(high // 4 == below, 0, 1)
    flip = (other + jnp.where(hops == 0, c, 0)) % 2
    half = jnp.where(flip == 0, expert % 2, 1 - expert % 2)
    order = half * 2 + other
    main = (block * 64 + order * MAIN).astype(jnp.float32) + rank
    rest = (1024 + block * 8 + order * REM).astype(jnp.float32) + (rank - MAIN)
    return jnp.where(rank < MAIN, main, jnp.where(rank < MAIN + REM, rest, -1.0))


def eye(n):
    return lax.broadcasted_iota(jnp.int32, (n, n), 0) == lax.broadcasted_iota(jnp.int32, (n, n), 1)


def to_column(row, n):
    pieces = []
    for at in range(0, n, 128):
        spread = jnp.where(eye(128), row[:, at : at + 128], 0.0)
        pieces.append(jnp.sum(spread, axis=1, keepdims=True))
    return pieces[0] if len(pieces) == 1 else jnp.concatenate(pieces, axis=0)


def to_row(column):
    return jnp.sum(jnp.where(eye(128), column, 0.0), axis=0, keepdims=True)


def kernel(
    value_hbm, gate_hbm, taps_hbm, gain_c_hbm, shift_c_hbm, cw_hbm,
    x_hbm, gain_hbm, experts_hbm, scores_hbm, wg_hbm, wu_hbm, wd_hbm,
    conv_out, out,
    w, xn, sm, sr, rm, sx, bm, rest_out, rest_in, hidden, sums, inner, rx, orx,
    val, gat, taps, gain_c, shift_c, gain, experts, scores,
    pad, acts, cw, window, halo_out, halo_in, stat, stats,
    load, native, avail, share, ring_sent, sib_sent,
    sent, d_recv, r_recv, q_recv,
    halo_sem, stat_sem, act_sem, cw_sem, cs_sem,
):
    f32, bf16 = jnp.float32, jnp.bfloat16
    ep = lax.axis_index("ep")
    y = lax.axis_index("tp")
    z, x, c = ep // 8, (ep // 2) % 4, ep % 2
    me = x * NY + y
    dd = (z - y + 8) % 4
    dist = jnp.where(c == 0, dd, (4 - dd) % 4)
    h_low = ((z - dd - y + 8) % 8) // 4
    hs = jnp.where((c == 0) | (dd == 0), h_low, 1 - h_low)

    def device(zz, xx, cc):
        return (zz * NX + xx) * NC + cc

    along = jnp.where(c == 0, (z + 1) % NZ, (z + NZ - 1) % NZ)
    ring_to = (device(along, x, c), y)
    sibling = (device(z, x, 1 - c), y)
    my_cols = pl.ds(pl.multiple_of(y * 256, 256), 256)

    loads = [
        pltpu.make_async_copy(value_hbm, val, load.at[0]),
        pltpu.make_async_copy(gate_hbm, gat, load.at[0]),
        pltpu.make_async_copy(x_hbm, xn, load.at[2]),
        pltpu.make_async_copy(taps_hbm.at[:, my_cols], taps, load.at[3]),
        pltpu.make_async_copy(cw_hbm, cw.at[y], load.at[4]),
        pltpu.make_async_copy(gain_c_hbm.at[:, my_cols], gain_c, load.at[3]),
        pltpu.make_async_copy(shift_c_hbm.at[:, my_cols], shift_c, load.at[3]),
        pltpu.make_async_copy(gain_hbm, gain, load.at[2]),
        pltpu.make_async_copy(experts_hbm, experts, load.at[1]),
        pltpu.make_async_copy(scores_hbm, scores, load.at[1]),
    ]

    @pl.when(dist == 0)
    def _():
        for i in range(CHUNKS):
            ref = wg_hbm if i < 16 else wu_hbm if i < 32 else wd_hbm
            block, row = (i // 8 % 2, i % 8) if i < 32 else ((i - 32) // 2, i % 2)
            pltpu.make_async_copy(
                ref.at[0, pl.ds(row * PIECE, PIECE), pl.ds(block * 256, 256)],
                w.at[hs, c, pl.ds(i * PIECE, PIECE)],
                native.at[i // 8],
            ).start()

    for copy in loads:
        copy.start()

    barrier = pltpu.get_barrier_semaphore()
    peers = [(device(z, (x + dx) % NX, c), (y + dy) % NY) for dx, dy in OFFSETS]
    peers += [(device((z + 1) % NZ, x, c), y), (device((z + NZ - 1) % NZ, x, c), y), sibling]
    peers += [((ep + 1) % 64, y), ((ep + 63) % 64, y)]
    for peer in peers:
        pl.semaphore_signal(barrier, inc=1, device_id=peer, device_id_type=MESH)

    def arrived(ref, sem):
        pltpu.make_async_copy(ref, ref, sem).wait()

    def piece(h, i):
        return w.at[h, i // CHUNKS, pl.ds(pl.multiple_of(i % CHUNKS * PIECE, PIECE), PIECE)]

    def ring_copy(i):
        return pltpu.make_async_remote_copy(
            src_ref=piece(hs, i), dst_ref=piece(hs, i), send_sem=ring_sent, recv_sem=avail.at[i],
            device_id=ring_to, device_id_type=MESH,
        )

    def sib_copy(h, i, sem):
        return pltpu.make_async_remote_copy(
            src_ref=piece(h, i), dst_ref=piece(h, i), send_sem=sib_sent, recv_sem=sem,
            device_id=sibling, device_id_type=MESH,
        )

    def share_of(i):
        j = i % CHUNKS
        return share.at[i // CHUNKS * 12 + jnp.where(j < 32, j // 8, 4 + (j - 32) // 2)]

    def expert_at(n):
        return jnp.where(c == 0, n, (n + CHUNKS) % TOTAL)

    def own(n):
        i = expert_at(n)
        mine = (dist == 0) & (i // CHUNKS == c)

        @pl.when(mine & (i % 8 == 0))
        def _():
            arrived(w.at[hs, c, pl.ds(0, 8 * PIECE)], native.at[i % CHUNKS // 8])

        @pl.when(jnp.logical_not(mine))
        def _():
            ring_copy(i).wait_recv()

        @pl.when((dist < 3) | (n < CHUNKS))
        def _():
            ring_copy(i).start()

        @pl.when(dist > 0)
        def _():
            sib_copy(hs, i, share_of(i)).start()

        @pl.when(mine)
        def _():
            sib_copy(hs, i, avail.at[i]).start()

    def step(p):
        n = p + jnp.where(dist == 0, AHEAD, -HOP * dist)
        m = p - OUTER

        @pl.when((n >= 0) & (n < TOTAL))
        def _():
            own(n)

        @pl.when((dist == 0) & (m >= 0) & (m < CHUNKS))
        def _():
            i = expert_at(m)
            ring_copy(i).wait_recv()
            sib_copy(1 - hs, i, share_of(i)).start()

    with jax.named_scope("s_gated"):
        loads[0].wait()
        loads[1].wait()

        def gated(b, carry):
            rows = pl.ds(pl.multiple_of(b * 128, 128), 128)
            wide = val[rows, :].astype(f32) * jax.nn.sigmoid(gat[rows, :].astype(f32))
            pad[pl.ds(pl.multiple_of(HALO + b * 128, 32), 128), :] = wide.astype(bf16).astype(f32)
            return carry

        lax.fori_loop(0, 8, gated, 0)
        halo_out[...] = pad[1024 : 1024 + HALO, :].astype(bf16)

        halo = pltpu.make_async_remote_copy(
            src_ref=halo_out, dst_ref=halo_in, send_sem=sent, recv_sem=halo_sem,
            device_id=((ep + 1) % 64, y), device_id_type=MESH,
        )
    with jax.named_scope("s_route"):
        tokens = xn.shape[0]
        loads[8].wait()
        loads[9].wait()
        first, second = experts[0:1, :], experts[1:2, :]
        ids = lax.broadcasted_iota(jnp.int32, (64, tokens), 0)
        hit0, hit1 = ids == first, ids == second
        both = jnp.where(hit0 | hit1, 1.0, 0.0).astype(bf16)
        row_t = lax.broadcasted_iota(jnp.int32, (tokens, tokens), 0)
        col_t = lax.broadcasted_iota(jnp.int32, (tokens, tokens), 1)
        earlier = jnp.where(row_t < col_t, 1.0, 0.0).astype(bf16)
        counts = jnp.dot(both, earlier, preferred_element_type=f32)
        slot0 = slot_of(first, jnp.sum(jnp.where(hit0, counts, 0.0), axis=0, keepdims=True), z, c)
        slot1 = slot_of(second, jnp.sum(jnp.where(hit1, counts, 0.0), axis=0, keepdims=True), z, c)

    with jax.named_scope("s_norm"):
        loads[2].wait()
        loads[7].wait()

        def norm(b, carry):
            rows = pl.ds(pl.multiple_of(b * 64, 64), 64)
            wide = xn[rows, :].astype(f32)
            square = jnp.mean(wide * wide, axis=-1, keepdims=True)
            xn[rows, :] = (wide * lax.rsqrt(square + 1e-06) * gain[...]).astype(bf16)
            return carry

        lax.fori_loop(0, 6, norm, 0)

    with jax.named_scope("s_barrier"):
        pl.semaphore_wait(barrier, len(peers))
    halo.start()

    @pl.when(dist == 0)
    def _():
        for n in range(AHEAD):
            own(n)

    step(0)

    def picked(base, count):
        at = (lax.broadcasted_iota(jnp.int32, (count, tokens), 0) + base).astype(f32)
        return jnp.where((at == slot0) | (at == slot1), 1.0, 0.0).astype(bf16)

    def dispatch(xx, yy, part):
        block = xx * NY + yy
        if part < 2:
            src, dst = sm.at[block, pl.ds(part * 32, 32)], rm.at[me, pl.ds(part * 32, 32)]
        else:
            src, dst = sr.at[block], sx.at[me]
        return pltpu.make_async_remote_copy(
            src_ref=src, dst_ref=dst, send_sem=sent, recv_sem=d_recv.at[part],
            device_id=(device(z, xx, c), yy), device_id_type=MESH,
        )

    def column_of(g):
        return (x + jnp.where(g == 0, 1, jnp.where(g == 1, 3, jnp.where(g == 2, 2, 0)))) % NX

    def send_group(g):
        xx = column_of(g)
        for part in range(2):
            for dy in (1, 3, 2, 0):
                copy = dispatch(xx, (y + dy) % NY, part)
                if dy > 0:
                    copy.start()
                else:

                    @pl.when(g < 3)
                    def _(copy=copy):
                        copy.start()

    def gather(g, carry):
        xx = column_of(g)
        choose = picked(xx * 256, 256)

        def cols(q, carry):
            at = pl.ds(pl.multiple_of(q * 512, 512), 512)
            rows = jnp.dot(choose, xn[:, at], preferred_element_type=f32).astype(bf16)
            sm[pl.ds(xx * 4, 4), :, at] = rows.reshape(4, 64, 512)
            return carry

        lax.fori_loop(0, 4, cols, 0)
        step(1 + g)

        @pl.when(g > 0)
        def _():
            send_group(g - 1)

        return carry

    with jax.named_scope("s_gather"):
        lax.fori_loop(0, 4, gather, 0)
        choose = picked(1024, 128)

        def gather_rest(q, carry):
            at = pl.ds(pl.multiple_of(q * 512, 512), 512)
            rows = jnp.dot(choose, xn[:, at], preferred_element_type=f32)
            sr[:, :, at] = rows.reshape(16, 8, 512).astype(bf16)
            return carry

        lax.fori_loop(0, 4, gather_rest, 0)

    def block_at(k, sign):
        dx, dy = OFFSETS[k]
        xx, yy = (x + sign * dx + NX) % NX, (y + sign * dy + NY) % NY
        return xx * NY + yy, (device(z, xx, c), yy)

    with jax.named_scope("s_dispatch"):
        send_group(3)
        for dx, dy in OFFSETS:
            dispatch((x + dx) % NX, (y + dy) % NY, 2).start()
        rm[me] = sm[me]
        sx[me] = sr[me]

    with jax.named_scope("s_filter"):
        halo.wait_recv()
        pad[0:HALO, :] = jnp.where(ep > 0, halo_in[...].astype(f32), 0.0)
        for k in (3, 5, 6):
            loads[k].wait()

        def filter_block(b, carry):
            step(5 + 2 * b)
            step(6 + 2 * b)
            base = pl.multiple_of(b * 128, 128)
            window[...] = pad[pl.ds(base, 128 + HALO), :]
            total = None
            for k in range(KERNEL):
                low = HALO - KERNEL + 1 + k
                term = taps[k : k + 1, :] * window[low : low + 128, :]
                total = term if total is None else total + term
            pad[pl.ds(base, 128), :] = total
            stat[y, pl.ds(b, 1), :] = to_row(jnp.sum(total, axis=1, keepdims=True))
            stat[y, pl.ds(8 + b, 1), :] = to_row(jnp.sum(total * total, axis=1, keepdims=True))
            return carry

        lax.fori_loop(0, 8, filter_block, 0)

    def near(k):
        yy = (y + k) % NY
        return yy, (ep, yy)

    def stat_copy(k):
        return pltpu.make_async_remote_copy(
            src_ref=stat.at[y], dst_ref=stat.at[y], send_sem=sent, recv_sem=stat_sem,
            device_id=near(k)[1], device_id_type=MESH,
        )

    def act_copy(k):
        yy, peer = near(k)
        return pltpu.make_async_remote_copy(
            src_ref=val.at[pl.ds(pl.multiple_of(yy * 256, 256), 256)], dst_ref=acts.at[y],
            send_sem=sent, recv_sem=act_sem, device_id=peer, device_id_type=MESH,
        )

    half = pl.ds(pl.multiple_of(c * 128, 128), 128)

    def cw_copy(k):
        return pltpu.make_async_remote_copy(
            src_ref=cw.at[y, half], dst_ref=cw.at[y, half], send_sem=sent,
            recv_sem=cw_sem, device_id=near(k)[1], device_id_type=MESH,
        )

    def cs_copy(k):
        yy = (y + NY - k) % NY
        return pltpu.make_async_remote_copy(
            src_ref=cw.at[yy, half], dst_ref=cw.at[yy, half], send_sem=sent,
            recv_sem=cs_sem, device_id=sibling, device_id_type=MESH,
        )

    loads[4].wait()
    for k in (1, 3, 2):
        stat_copy(k).start()
    for k in (1, 3, 2):
        cw_copy(k).start()

    def only_step(p, carry):
        step(p)
        return carry

    with jax.named_scope("s_pumps"):
        lax.fori_loop(21, START, only_step, 0)

    with jax.named_scope("s_wait_rows"):
        for part in range(2):
            arrived(rm.at[pl.ds(0, 15), pl.ds(0, 32)], d_recv.at[part])
        arrived(sx.at[pl.ds(0, 15)], d_recv.at[2])
        rx[...] = sx[...].astype(f32).reshape(128, 2048).astype(bf16)

    with jax.named_scope("s_wait_stat"):
        arrived(stat.at[pl.ds(0, 3)], stat_sem)
        stats[...] = (stat[0] + stat[1]) + (stat[2] + stat[3])

    order_in_rest = (lax.broadcasted_iota(jnp.int32, (128, 256), 0) % 8) // REM

    def of_half(half, s):
        e_low = jnp.where((dist == 0) & (c == 1), 1 - half, half)
        return jnp.where(s == 0, h_low, 1 - h_low), jnp.where(s == 0, e_low, 1 - e_low)

    def shared(half, s, low, count):
        e = of_half(half, s)[1]

        @pl.when(jnp.where(dist > 0, s != c, (s == 1) & (half == 0)))
        def _():
            arrived(w.at[hs, 0, pl.ds(0, count * PIECE)], share_of(e * CHUNKS + low))

    def rows_at(half, s):
        return pl.ds(pl.multiple_of(half * 32 + s * MAIN, MAIN), MAIN)

    def gate_up(half, block, s):
        shared(half, s, block * 8, 8)
        h, e = of_half(half, s)
        rows = jnp.concatenate([rm[:, rows_at(half, s), :].reshape(256, 2048), rx[...]], axis=0)
        weight = w[h, e, pl.ds(pl.multiple_of(block * 2048, 2048), 2048), :]
        at = pl.ds(pl.multiple_of(block * 256, 256), 256)
        hidden[s, :, at] = jnp.dot(rows, weight, preferred_element_type=f32)

        @pl.when(block == 3)
        def _():
            inner[s] = (jax.nn.silu(hidden[s, :, 0:512]) * hidden[s, :, 512:1024]).astype(bf16)

    def down(half, block, s):
        shared(half, s, 32 + block * 2, 2)
        at = pl.ds(pl.multiple_of(block * 256, 256), 256)
        h, e = of_half(half, s)
        weight = w[h, e, pl.ds(pl.multiple_of(8192 + block * 512, 512), 512), :]
        rows = jnp.dot(inner[s], weight, preferred_element_type=f32)
        rm[:, rows_at(half, s), at] = rows[:256].astype(bf16).reshape(16, MAIN, 256)
        here = order_in_rest == half * 2 + s
        orx[:, at] = jnp.where(here, rows[256:], orx[:, at])

    def activate(b):
        rows = pl.ds(pl.multiple_of(b * 128, 128), 128)
        center = to_column(stats[pl.ds(b, 1), :], 128) / CONV
        spread = to_column(stats[pl.ds(8 + b, 1), :], 128) / CONV - center * center
        normed = (pad[rows, :] - center) * lax.rsqrt(spread + 1e-05) * gain_c[...] + shift_c[...]
        val[rows, :] = jax.nn.silu(normed).astype(bf16)

    def phase0(p):
        @pl.when(p < START + 8)
        def _():
            activate(p - START)

        @pl.when(p == START + 8)
        def _():
            for k in (1, 3, 2):
                act_copy(k).start()
            acts[y] = val[my_cols, :]

        q = p - START

        @pl.when((q >= 0) & (q < 8))
        def _():
            gate_up(0, q // 2, q % 2)

        @pl.when((q >= 8) & (q < 16))
        def _():
            for s in range(2):
                down(0, q - 8, s)

    def back(k, main):
        block, peer = block_at(k, -1)
        if main:
            src, dst = rm.at[block, pl.ds(0, 32)], bm.at[me, pl.ds(0, 32)]
        else:
            src, dst = rest_out.at[0, block], rest_in.at[0, me]
        return pltpu.make_async_remote_copy(
            src_ref=src, dst_ref=dst, send_sem=sent, recv_sem=r_recv.at[1 - main],
            device_id=peer, device_id_type=MESH,
        )

    low_rows = lax.broadcasted_iota(jnp.int32, (128, 256), 0) % 8 < 4

    def fold(half, block):
        left = slice(block * 256, block * 256 + 256)
        right = slice(1024 + block * 256, 1280 + block * 256)
        if half == 0:
            rows = jnp.where(low_rows, orx[:, left], pltpu.roll(orx[:, right], 4, 0))
        else:
            rows = jnp.where(low_rows, pltpu.roll(orx[:, left], 124, 0), orx[:, right])
        rest_out[half, :, :, left] = rows.reshape(16, 8, 256).astype(bf16)

    def first_leave():
        for k in range(15):
            back(k, 1).start()
        for block in range(4):
            fold(0, block)
        for k in range(15):
            back(k, 0).start()
        bm[me, 0:32] = rm[me, 0:32]
        rest_in[0, me] = rest_out[0, me]

    def conv_part(q):
        at = pl.ds(pl.multiple_of(q * 512, 512), 512)
        total = None
        for b in range(4):
            term = jnp.dot(acts[b], cw[b, :, at], preferred_element_type=f32).astype(bf16).astype(f32)
            total = term if total is None else total + term
        conv_out[:, at] = total.astype(bf16)

    slot0_c, slot1_c = to_column(slot0, tokens), to_column(slot1, tokens)
    group = jax.nn.sigmoid(scores[0:1, :])
    weight0 = to_column(group * jax.nn.sigmoid(scores[1:2, :]), tokens)
    weight1 = to_column(group * jax.nn.sigmoid(-scores[1:2, :]), tokens)

    def chosen_main(slot, half):
        at = lax.broadcasted_iota(jnp.int32, (tokens, 512), 1)
        main = ((at // 32) * 64 + half * 32 + at % 32).astype(f32)
        return jnp.where(main == slot, 1.0, 0.0).astype(bf16)

    def chosen_rest(slot, half, right):
        at = lax.broadcasted_iota(jnp.int32, (tokens, 128), 1)
        name = 1024 + at + 4 * (half - right)
        here = (at % 8 >= 4) == (right > 0)
        return jnp.where(here & (name.astype(f32) == slot), 1.0, 0.0).astype(bf16)

    def rest_rows(half, at):
        return rest_in[half, :, :, at].astype(f32).reshape(128, 256).astype(bf16)

    def weighted(pick0, pick1, rows):
        return weight0 * jnp.dot(pick0, rows, preferred_element_type=f32) + weight1 * jnp.dot(
            pick1, rows, preferred_element_type=f32
        )

    def combine0(block):
        at = slice(block * 256, block * 256 + 256)
        folded = slice(block % 4 * 256, block % 4 * 256 + 256)
        rows = jnp.concatenate([bm[:, 0:32, at].reshape(512, 256), rest_rows(0, folded)], axis=0)
        picks = [
            jnp.concatenate([chosen_main(slot, 0), chosen_rest(slot, 0, block // 4)], axis=1)
            for slot in (slot0_c, slot1_c)
        ]
        sums[:, at] = weighted(picks[0], picks[1], rows)

    def column(k, block, s):
        source, peer = block_at(k, -1)
        at = pl.ds(pl.multiple_of(block * 256, 256), 256)
        rows = pl.ds(32 + s * MAIN, MAIN)
        return pltpu.make_async_remote_copy(
            src_ref=rm.at[source, rows, at], dst_ref=bm.at[me, rows, at], send_sem=sent,
            recv_sem=q_recv.at[block], device_id=peer, device_id_type=MESH,
        )

    def rest_column(k, block):
        source, peer = block_at(k, -1)
        at = pl.ds(block * 256, 256)
        return pltpu.make_async_remote_copy(
            src_ref=rest_out.at[1, source, :, at], dst_ref=rest_in.at[1, me, :, at],
            send_sem=sent, recv_sem=q_recv.at[8 + block], device_id=peer,
            device_id_type=MESH,
        )

    def leave(block, s):
        at = pl.ds(pl.multiple_of(block * 256, 256), 256)
        rows = pl.ds(32 + s * MAIN, MAIN)
        for k in TAIL_ORDER:
            column(k, block, s).start()
        bm[me, rows, at] = rm[me, rows, at]

    def rest_leave(block):
        fold(1, block)
        for k in TAIL_ORDER:
            rest_column(k, block).start()
        at = slice(block * 256, block * 256 + 256)
        rest_in[1, me, :, at] = rest_out[1, me, :, at]

    def phases(p, carry):
        step(p)
        phase0(p)

        @pl.when(p == MIDDLE)
        def _():
            first_leave()

        @pl.when(p == MIDDLE + 10)
        def _():
            arrived(cw.at[pl.ds(0, 3), pl.ds(0, 128)], cw_sem)
            for k in (1, 3, 2):
                cs_copy(k).start()

        @pl.when(p == MIDDLE + 18)
        def _():
            arrived(acts.at[pl.ds(0, 3)], act_sem)
            arrived(cw.at[pl.ds(0, 3), pl.ds(0, 128)], cs_sem)

        @pl.when((p >= MIDDLE + 18) & (p < MIDDLE + 22))
        def _():
            conv_part(p - MIDDLE - 18)

        there = []
        for s in range(2):
            handed = jnp.where(c == s, HOP * dist, HOP * (4 - dist) + SHARE)
            lag = jnp.where(dist == 0, -AHEAD, handed)

            def pieces(p, lag=lag):
                return jnp.minimum(2 * (p - MIDDLE), p - lag - CHUNKS + 1)

            old, new = pieces(p - 1), pieces(p)

            @pl.when((new >= 8) & (new < 34) & (new // 8 != old // 8))
            def _(s=s, new=new):
                gate_up(1, new // 8 - 1, s)

            @pl.when((new >= 34) & (new < 50) & (new // 2 != old // 2))
            def _(s=s, new=new):
                block = (new - 34) // 2
                down(1, block, s)
                leave(block, s)

            there.append((old, new))

        old, new = [jnp.minimum(there[0][i], there[1][i]) for i in range(2)]
        for block in range(4):
            due = 42 + 2 * block

            @pl.when((old < due) & (new >= due))
            def _(block=block):
                rest_leave(block)

        return carry

    with jax.named_scope("s_phase1"):
        lax.fori_loop(START, LAST, phases, 0)

    with jax.named_scope("s_combine0"):
        arrived(bm.at[pl.ds(0, 15), pl.ds(0, 32)], r_recv.at[0])
        arrived(rest_in.at[0, pl.ds(0, 15)], r_recv.at[1])
        for block in range(8):
            combine0(block)

    with jax.named_scope("s_combine1"):
        pick0, pick1 = chosen_main(slot0_c, 1), chosen_main(slot1_c, 1)
        picks = [[chosen_rest(slot, 1, right) for slot in (slot0_c, slot1_c)] for right in range(2)]
        for block in range(8):
            at = slice(block * 256, block * 256 + 256)
            arrived(bm.at[pl.ds(0, 15), pl.ds(32, 32), pl.ds(block * 256, 256)], q_recv.at[block])
            sums[:, at] += weighted(pick0, pick1, bm[:, 32:64, at].reshape(512, 256))
            if block >= 4:
                low = block * 256 - 1024
                arrived(rest_in.at[1, pl.ds(0, 15), :, pl.ds(low, 256)], q_recv.at[4 + block])
                rows = rest_rows(1, slice(low, low + 256))
                for right in range(2):
                    at = slice(low + right * 1024, low + right * 1024 + 256)
                    last = weighted(picks[right][0], picks[right][1], rows)
                    out[:, at] = (sums[:, at] + last).astype(bf16)

    with jax.named_scope("s_sent"):
        halo.wait_send()
        arrived(stat.at[pl.ds(0, 3)], sent)
        arrived(acts.at[pl.ds(0, 3)], sent)
        arrived(cw.at[pl.ds(0, 3), pl.ds(0, 128)], sent)
        arrived(cw.at[pl.ds(0, 3), pl.ds(0, 128)], sent)
        arrived(sm.at[pl.ds(0, 15)], sent)
        arrived(sr.at[pl.ds(0, 15)], sent)
        arrived(bm.at[pl.ds(0, 15), pl.ds(0, 32)], sent)
        arrived(rest_in.at[0, pl.ds(0, 15)], sent)
        arrived(bm.at[pl.ds(0, 15), pl.ds(32, 32)], sent)
        arrived(rest_in.at[1, pl.ds(0, 15)], sent)

        @pl.when(dist < 3)
        def _():
            arrived(w.at[0], ring_sent)

        @pl.when(dist == 3)
        def _():
            arrived(w.at[0, 0], ring_sent)

        arrived(w.at[0], sib_sent)


def write_out(conv_ref, moe_ref, conv_out, moe_out, sems):
    copies = []
    for source, target in ((moe_ref, moe_out), (conv_ref, conv_out)):
        for low in range(0, source.shape[0], OUT_ROWS):
            rows = pl.ds(low, OUT_ROWS)
            copies.append(
                pltpu.make_async_copy(source.at[rows], target.at[rows], sems.at[len(copies)])
            )
            copies[-1].start()
    for copy in copies:
        copy.wait()


def on_device(
    conv_value,
    conv_gate,
    depth_weight,
    norm_gain,
    norm_shift,
    conv_out_weight,
    moe_input,
    moe_gain,
    route_experts,
    route_scores,
    expert_gate,
    expert_up,
    expert_down,
):
    bf16, f32 = jnp.bfloat16, jnp.float32
    rows, width = moe_input.shape
    span, channels = conv_value.shape
    hbm = pl.BlockSpec(memory_space=pl.ANY)
    vmem = pl.BlockSpec(memory_space=pltpu.VMEM)
    dma = pltpu.SemaphoreType.DMA
    both = pl.pallas_call(
        kernel,
        out_shape=(
            pltpu.VMEM((span // NY, width), bf16),
            pltpu.VMEM((rows, width), bf16),
        ),
        in_specs=[hbm] * 13,
        out_specs=(vmem, vmem),
        scratch_shapes=[
            pltpu.VMEM((2, 2, CHUNKS * PIECE, 256), bf16),
            pltpu.VMEM((rows, width), bf16),
            pltpu.VMEM((16, 64, width), bf16),
            pltpu.VMEM((16, 8, width), bf16),
            pltpu.VMEM((16, 64, width), bf16),
            pltpu.VMEM((16, 8, width), bf16),
            pltpu.VMEM((16, 64, width), bf16),
            pltpu.VMEM((2, 16, 8, width // 2), bf16),
            pltpu.VMEM((2, 16, 8, width // 2), bf16),
            pltpu.VMEM((2, 384, 1024), f32),
            pltpu.VMEM((rows, width), f32),
            pltpu.VMEM((2, 384, 512), bf16),
            pltpu.VMEM((128, width), bf16),
            pltpu.VMEM((128, width), f32),
            pltpu.VMEM((span, channels), bf16),
            pltpu.VMEM((span, channels), bf16),
            pltpu.VMEM((KERNEL, channels), f32),
            pltpu.VMEM((1, channels), f32),
            pltpu.VMEM((1, channels), f32),
            pltpu.VMEM((1, width), f32),
            pltpu.VMEM((2, rows), jnp.int32),
            pltpu.VMEM((2, rows), f32),
            pltpu.VMEM((HALO + span, channels), f32),
            pltpu.VMEM((NY, span // NY, channels), bf16),
            pltpu.VMEM((NY, channels, width), bf16),
            pltpu.VMEM((128 + HALO, channels), f32),
            pltpu.VMEM((HALO, channels), bf16),
            pltpu.VMEM((HALO, channels), bf16),
            pltpu.VMEM((NY, 16, 128), f32),
            pltpu.VMEM((16, 128), f32),
            dma((5,)),
            dma((6,)),
            dma((TOTAL,)),
            dma((24,)),
            dma,
            dma,
            dma,
            dma((3,)),
            dma((2,)),
            dma((12,)),
            dma,
            dma,
            dma,
            dma,
            dma,
        ],
        compiler_params=pltpu.CompilerParams(
            collective_id=0, has_side_effects=True, vmem_limit_bytes=64_300_000
        ),
        name="both",
    )(
        conv_value,
        conv_gate,
        depth_weight,
        norm_gain.reshape(1, CONV),
        norm_shift.reshape(1, CONV),
        conv_out_weight,
        moe_input,
        moe_gain.reshape(1, width),
        route_experts.T,
        route_scores.T,
        expert_gate,
        expert_up,
        expert_down,
    )
    outs = [jax.ShapeDtypeStruct(out.shape, out.dtype) for out in both]
    return pl.pallas_call(
        write_out,
        out_shape=tuple(outs),
        in_specs=[vmem, vmem],
        out_specs=(hbm, hbm),
        scratch_shapes=[dma((sum(out.shape[0] for out in outs) // OUT_ROWS,))],
        name="write_out",
    )(*(pltpu.with_memory_space_constraint(out, pltpu.VMEM) for out in both))


def solution(mesh):
    in_specs = (
        P("ep", "tp"),
        P("ep", "tp"),
        P(),
        P(),
        P(),
        P("tp", None),
        P(("ep", "tp"), None),
        P(),
        P(("ep", "tp"), None),
        P(("ep", "tp"), None),
        P("ep", None, None),
        P("ep", None, None),
        P("ep", None, None),
    )
    out_specs = (P(("ep", "tp"), None), P(("ep", "tp"), None))
    return jax.shard_map(
        on_device, mesh=mesh, in_specs=in_specs, out_specs=out_specs, check_vma=False
    )
```

```python
import jax
import jax.numpy as jnp
from jax import lax
from jax.experimental import pallas as pl
from jax.experimental.pallas import tpu as pltpu
from jax.sharding import PartitionSpec as P

MESH = pl.DeviceIdType.MESH
OUT_ROWS = 128
NZ, NX, NC, NY = 8, 4, 2, 4
CONV = 1024
KERNEL = 31
HALO = 32
MAIN = 16
REM = 2
PIECE = 256
CHUNKS = 48
TOTAL = 2 * CHUNKS
HOP = 2
AHEAD = 4
SHARE = 4
OUTER = 12
START = 48
MIDDLE = START + 16
LAST = TOTAL + 3 * HOP + SHARE
OFFSETS = [
    (1, 0), (3, 0), (0, 1), (0, 3), (1, 1), (3, 3), (1, 3), (3, 1),
    (2, 0), (0, 2), (2, 2), (1, 2), (3, 2), (2, 1), (2, 3),
]

TAIL_ORDER = tuple(reversed(range(15)))


def slot_of(expert, rank, z, c):
    high = expert // 8
    yy = high % 4
    block = ((expert // 2) % 4) * NY + yy
    hops = (z - yy + 8) % 4
    below = ((z - hops - yy + 8) % 8) // 4
    other = jnp.where(high // 4 == below, 0, 1)
    flip = (other + jnp.where(hops == 0, c, 0)) % 2
    half = jnp.where(flip == 0, expert % 2, 1 - expert % 2)
    order = half * 2 + other
    main = (block * 64 + order * MAIN).astype(jnp.float32) + rank
    rest = (1024 + block * 8 + order * REM).astype(jnp.float32) + (rank - MAIN)
    return jnp.where(rank < MAIN, main, jnp.where(rank < MAIN + REM, rest, -1.0))


def eye(n):
    return lax.broadcasted_iota(jnp.int32, (n, n), 0) == lax.broadcasted_iota(jnp.int32, (n, n), 1)


def to_column(row, n):
    pieces = []
    for at in range(0, n, 128):
        spread = jnp.where(eye(128), row[:, at : at + 128], 0.0)
        pieces.append(jnp.sum(spread, axis=1, keepdims=True))
    return pieces[0] if len(pieces) == 1 else jnp.concatenate(pieces, axis=0)


def to_row(column):
    return jnp.sum(jnp.where(eye(128), column, 0.0), axis=0, keepdims=True)


def kernel(
    value_hbm, gate_hbm, taps_hbm, gain_c_hbm, shift_c_hbm, cw_hbm,
    x_hbm, gain_hbm, experts_hbm, scores_hbm, wg_hbm, wu_hbm, wd_hbm,
    conv_out, out,
    w, xn, sm, sr, rm, sx, bm, rest_out, rest_in, hidden, sums, inner, rx, orx,
    val, gat, taps, gain_c, shift_c, gain, experts, scores,
    pad, acts, cw, window, halo_out, halo_in, stat, stats,
    load, native, avail, share, ring_sent, sib_sent,
    sent, d_recv, r_recv, q_recv,
    halo_sem, stat_sem, act_sem, cw_sem, cs_sem,
):
    f32, bf16 = jnp.float32, jnp.bfloat16
    ep = lax.axis_index("ep")
    y = lax.axis_index("tp")
    z, x, c = ep // 8, (ep // 2) % 4, ep % 2
    me = x * NY + y
    dd = (z - y + 8) % 4
    dist = jnp.where(c == 0, dd, (4 - dd) % 4)
    h_low = ((z - dd - y + 8) % 8) // 4
    hs = jnp.where((c == 0) | (dd == 0), h_low, 1 - h_low)

    def device(zz, xx, cc):
        return (zz * NX + xx) * NC + cc

    along = jnp.where(c == 0, (z + 1) % NZ, (z + NZ - 1) % NZ)
    ring_to = (device(along, x, c), y)
    sibling = (device(z, x, 1 - c), y)
    my_cols = pl.ds(pl.multiple_of(y * 256, 256), 256)

    loads = [
        pltpu.make_async_copy(value_hbm, val, load.at[0]),
        pltpu.make_async_copy(gate_hbm, gat, load.at[0]),
        pltpu.make_async_copy(x_hbm, xn, load.at[2]),
        pltpu.make_async_copy(taps_hbm.at[:, my_cols], taps, load.at[3]),
        pltpu.make_async_copy(cw_hbm, cw.at[y], load.at[4]),
        pltpu.make_async_copy(gain_c_hbm.at[:, my_cols], gain_c, load.at[3]),
        pltpu.make_async_copy(shift_c_hbm.at[:, my_cols], shift_c, load.at[3]),
        pltpu.make_async_copy(gain_hbm, gain, load.at[2]),
        pltpu.make_async_copy(experts_hbm, experts, load.at[1]),
        pltpu.make_async_copy(scores_hbm, scores, load.at[1]),
    ]

    @pl.when(dist == 0)
    def _():
        for i in range(CHUNKS):
            ref = wg_hbm if i < 16 else wu_hbm if i < 32 else wd_hbm
            block, row = (i // 8 % 2, i % 8) if i < 32 else ((i - 32) // 2, i % 2)
            pltpu.make_async_copy(
                ref.at[0, pl.ds(row * PIECE, PIECE), pl.ds(block * 256, 256)],
                w.at[hs, c, pl.ds(i * PIECE, PIECE)],
                native.at[i // 16],
            ).start()

    for copy in loads:
        copy.start()

    barrier = pltpu.get_barrier_semaphore()
    peers = [(device(z, (x + dx) % NX, c), (y + dy) % NY) for dx, dy in OFFSETS]
    peers += [(device((z + 1) % NZ, x, c), y), (device((z + NZ - 1) % NZ, x, c), y), sibling]
    peers += [((ep + 1) % 64, y), ((ep + 63) % 64, y)]
    for peer in peers:
        pl.semaphore_signal(barrier, inc=1, device_id=peer, device_id_type=MESH)

    def arrived(ref, sem):
        pltpu.make_async_copy(ref, ref, sem).wait()

    def piece(h, i):
        return w.at[h, i // CHUNKS, pl.ds(pl.multiple_of(i % CHUNKS * PIECE, PIECE), PIECE)]

    def ring_copy(i):
        return pltpu.make_async_remote_copy(
            src_ref=piece(hs, i), dst_ref=piece(hs, i), send_sem=ring_sent, recv_sem=avail.at[i],
            device_id=ring_to, device_id_type=MESH,
        )

    def sib_copy(h, i, sem):
        return pltpu.make_async_remote_copy(
            src_ref=piece(h, i), dst_ref=piece(h, i), send_sem=sib_sent, recv_sem=sem,
            device_id=sibling, device_id_type=MESH,
        )

    def share_of(i):
        j = i % CHUNKS
        return share.at[i // CHUNKS * 12 + jnp.where(j < 32, j // 8, 4 + (j - 32) // 2)]

    def expert_at(n):
        return jnp.where(c == 0, n, (n + CHUNKS) % TOTAL)

    def own(n):
        i = expert_at(n)
        mine = (dist == 0) & (i // CHUNKS == c)

        @pl.when(mine & (i % 16 == 0))
        def _():
            arrived(w.at[hs, c, pl.ds(0, 16 * PIECE)], native.at[i % CHUNKS // 16])

        @pl.when(jnp.logical_not(mine))
        def _():
            ring_copy(i).wait_recv()

        @pl.when((dist < 3) | (n < CHUNKS))
        def _():
            ring_copy(i).start()

        @pl.when(dist > 0)
        def _():
            sib_copy(hs, i, share_of(i)).start()

        @pl.when(mine)
        def _():
            sib_copy(hs, i, avail.at[i]).start()

    def step(p):
        n = p + jnp.where(dist == 0, AHEAD, -HOP * dist)
        m = p - OUTER

        @pl.when((n >= 0) & (n < TOTAL))
        def _():
            own(n)

        @pl.when((dist == 0) & (m >= 0) & (m < CHUNKS))
        def _():
            i = expert_at(m)
            ring_copy(i).wait_recv()
            sib_copy(1 - hs, i, share_of(i)).start()

    with jax.named_scope("s_gated"):
        loads[0].wait()
        loads[1].wait()

        def gated(b, carry):
            rows = pl.ds(pl.multiple_of(b * 128, 128), 128)
            wide = val[rows, :].astype(f32) * jax.nn.sigmoid(gat[rows, :].astype(f32))
            pad[pl.ds(pl.multiple_of(HALO + b * 128, 32), 128), :] = wide.astype(bf16).astype(f32)
            return carry

        lax.fori_loop(0, 8, gated, 0)
        halo_out[...] = pad[1024 : 1024 + HALO, :].astype(bf16)

        halo = pltpu.make_async_remote_copy(
            src_ref=halo_out, dst_ref=halo_in, send_sem=sent, recv_sem=halo_sem,
            device_id=((ep + 1) % 64, y), device_id_type=MESH,
        )
    with jax.named_scope("s_route"):
        tokens = xn.shape[0]
        loads[8].wait()
        loads[9].wait()
        first, second = experts[0:1, :], experts[1:2, :]
        ids = lax.broadcasted_iota(jnp.int32, (64, tokens), 0)
        hit0, hit1 = ids == first, ids == second
        both = jnp.where(hit0 | hit1, 1.0, 0.0).astype(bf16)
        row_t = lax.broadcasted_iota(jnp.int32, (tokens, tokens), 0)
        col_t = lax.broadcasted_iota(jnp.int32, (tokens, tokens), 1)
        earlier = jnp.where(row_t < col_t, 1.0, 0.0).astype(bf16)
        counts = jnp.dot(both, earlier, preferred_element_type=f32)
        slot0 = slot_of(first, jnp.sum(jnp.where(hit0, counts, 0.0), axis=0, keepdims=True), z, c)
        slot1 = slot_of(second, jnp.sum(jnp.where(hit1, counts, 0.0), axis=0, keepdims=True), z, c)

    with jax.named_scope("s_norm"):
        loads[2].wait()
        loads[7].wait()

        def norm(b, carry):
            rows = pl.ds(pl.multiple_of(b * 64, 64), 64)
            wide = xn[rows, :].astype(f32)
            square = jnp.mean(wide * wide, axis=-1, keepdims=True)
            xn[rows, :] = (wide * lax.rsqrt(square + 1e-06) * gain[...]).astype(bf16)
            return carry

        lax.fori_loop(0, 6, norm, 0)

    with jax.named_scope("s_barrier"):
        pl.semaphore_wait(barrier, len(peers))
    halo.start()

    @pl.when(dist == 0)
    def _():
        for n in range(AHEAD):
            own(n)

    step(0)

    def picked(base, count):
        at = (lax.broadcasted_iota(jnp.int32, (count, tokens), 0) + base).astype(f32)
        return jnp.where((at == slot0) | (at == slot1), 1.0, 0.0).astype(bf16)

    def dispatch(xx, yy, part):
        block = xx * NY + yy
        if part < 2:
            src, dst = sm.at[block, pl.ds(part * 32, 32)], rm.at[me, pl.ds(part * 32, 32)]
        else:
            src, dst = sr.at[block], sx.at[me]
        return pltpu.make_async_remote_copy(
            src_ref=src, dst_ref=dst, send_sem=sent, recv_sem=d_recv.at[part // 2],
            device_id=(device(z, xx, c), yy), device_id_type=MESH,
        )

    def column_of(g):
        return (x + jnp.where(g == 0, 1, jnp.where(g == 1, 3, jnp.where(g == 2, 2, 0)))) % NX

    def send_group(g):
        xx = column_of(g)
        for part in range(2):
            for dy in (1, 3, 2, 0):
                copy = dispatch(xx, (y + dy) % NY, part)
                if dy > 0:
                    copy.start()
                else:

                    @pl.when(g < 3)
                    def _(copy=copy):
                        copy.start()

    def gather(g, carry):
        xx = column_of(g)
        choose = picked(xx * 256, 256)

        def cols(q, carry):
            at = pl.ds(pl.multiple_of(q * 512, 512), 512)
            rows = jnp.dot(choose, xn[:, at], preferred_element_type=f32).astype(bf16)
            sm[pl.ds(xx * 4, 4), :, at] = rows.reshape(4, 64, 512)
            return carry

        lax.fori_loop(0, 4, cols, 0)
        step(1 + g)

        @pl.when(g > 0)
        def _():
            send_group(g - 1)

        return carry

    with jax.named_scope("s_gather"):
        lax.fori_loop(0, 4, gather, 0)
        choose = picked(1024, 128)

        def gather_rest(q, carry):
            at = pl.ds(pl.multiple_of(q * 512, 512), 512)
            rows = jnp.dot(choose, xn[:, at], preferred_element_type=f32)
            sr[:, :, at] = rows.reshape(16, 8, 512).astype(bf16)
            return carry

        lax.fori_loop(0, 4, gather_rest, 0)

    def block_at(k, sign):
        dx, dy = OFFSETS[k]
        xx, yy = (x + sign * dx + NX) % NX, (y + sign * dy + NY) % NY
        return xx * NY + yy, (device(z, xx, c), yy)

    with jax.named_scope("s_dispatch"):
        send_group(3)
        for dx, dy in OFFSETS:
            dispatch((x + dx) % NX, (y + dy) % NY, 2).start()
        rm[me] = sm[me]
        sx[me] = sr[me]

    with jax.named_scope("s_filter"):
        halo.wait_recv()
        pad[0:HALO, :] = jnp.where(ep > 0, halo_in[...].astype(f32), 0.0)
        for k in (3, 5, 6):
            loads[k].wait()

        def filter_block(b, carry):
            step(5 + 2 * b)
            step(6 + 2 * b)
            base = pl.multiple_of(b * 128, 128)
            window[...] = pad[pl.ds(base, 128 + HALO), :]
            total = None
            for k in range(KERNEL):
                low = HALO - KERNEL + 1 + k
                term = taps[k : k + 1, :] * window[low : low + 128, :]
                total = term if total is None else total + term
            pad[pl.ds(base, 128), :] = total
            stat[y, pl.ds(b, 1), :] = to_row(jnp.sum(total, axis=1, keepdims=True))
            stat[y, pl.ds(8 + b, 1), :] = to_row(jnp.sum(total * total, axis=1, keepdims=True))
            return carry

        lax.fori_loop(0, 8, filter_block, 0)

    def near(k):
        yy = (y + k) % NY
        return yy, (ep, yy)

    def stat_copy(k):
        return pltpu.make_async_remote_copy(
            src_ref=stat.at[y], dst_ref=stat.at[y], send_sem=sent, recv_sem=stat_sem,
            device_id=near(k)[1], device_id_type=MESH,
        )

    def act_copy(k):
        yy, peer = near(k)
        return pltpu.make_async_remote_copy(
            src_ref=val.at[pl.ds(pl.multiple_of(yy * 256, 256), 256)], dst_ref=acts.at[y],
            send_sem=sent, recv_sem=act_sem, device_id=peer, device_id_type=MESH,
        )

    half = pl.ds(pl.multiple_of(c * 128, 128), 128)

    def cw_copy(k):
        return pltpu.make_async_remote_copy(
            src_ref=cw.at[y, half], dst_ref=cw.at[y, half], send_sem=sent,
            recv_sem=cw_sem, device_id=near(k)[1], device_id_type=MESH,
        )

    def cs_copy(k):
        yy = (y + NY - k) % NY
        return pltpu.make_async_remote_copy(
            src_ref=cw.at[yy, half], dst_ref=cw.at[yy, half], send_sem=sent,
            recv_sem=cs_sem, device_id=sibling, device_id_type=MESH,
        )

    loads[4].wait()
    for k in (1, 3, 2):
        stat_copy(k).start()
    for k in (1, 3, 2):
        cw_copy(k).start()

    def only_step(p, carry):
        step(p)
        return carry

    with jax.named_scope("s_pumps"):
        lax.fori_loop(21, START, only_step, 0)

    with jax.named_scope("s_wait_rows"):
        arrived(rm.at[pl.ds(0, 15)], d_recv.at[0])
        arrived(sx.at[pl.ds(0, 15)], d_recv.at[1])
        rx[...] = sx[...].astype(f32).reshape(128, 2048).astype(bf16)

    with jax.named_scope("s_wait_stat"):
        arrived(stat.at[pl.ds(0, 3)], stat_sem)
        stats[...] = (stat[0] + stat[1]) + (stat[2] + stat[3])

    order_in_rest = (lax.broadcasted_iota(jnp.int32, (128, 256), 0) % 8) // REM

    def of_half(half, s):
        e_low = jnp.where((dist == 0) & (c == 1), 1 - half, half)
        return jnp.where(s == 0, h_low, 1 - h_low), jnp.where(s == 0, e_low, 1 - e_low)

    def shared(half, s, low, count):
        e = of_half(half, s)[1]

        @pl.when(jnp.where(dist > 0, s != c, (s == 1) & (half == 0)))
        def _():
            arrived(w.at[hs, 0, pl.ds(0, count * PIECE)], share_of(e * CHUNKS + low))

    def rows_at(half, s):
        return pl.ds(pl.multiple_of(half * 32 + s * MAIN, MAIN), MAIN)

    def gate_up(half, block, s):
        shared(half, s, block * 8, 8)
        h, e = of_half(half, s)
        rows = jnp.concatenate([rm[:, rows_at(half, s), :].reshape(256, 2048), rx[...]], axis=0)
        weight = w[h, e, pl.ds(pl.multiple_of(block * 2048, 2048), 2048), :]
        at = pl.ds(pl.multiple_of(block * 256, 256), 256)
        hidden[s, :, at] = jnp.dot(rows, weight, preferred_element_type=f32)

        @pl.when(block == 3)
        def _():
            inner[s] = (jax.nn.silu(hidden[s, :, 0:512]) * hidden[s, :, 512:1024]).astype(bf16)

    def down(half, block, s):
        shared(half, s, 32 + block * 2, 2)
        at = pl.ds(pl.multiple_of(block * 256, 256), 256)
        h, e = of_half(half, s)
        weight = w[h, e, pl.ds(pl.multiple_of(8192 + block * 512, 512), 512), :]
        rows = jnp.dot(inner[s], weight, preferred_element_type=f32)
        rm[:, rows_at(half, s), at] = rows[:256].astype(bf16).reshape(16, MAIN, 256)
        here = order_in_rest == half * 2 + s
        orx[:, at] = jnp.where(here, rows[256:], orx[:, at])

    def activate(b):
        rows = pl.ds(pl.multiple_of(b * 128, 128), 128)
        center = to_column(stats[pl.ds(b, 1), :], 128) / CONV
        spread = to_column(stats[pl.ds(8 + b, 1), :], 128) / CONV - center * center
        normed = (pad[rows, :] - center) * lax.rsqrt(spread + 1e-05) * gain_c[...] + shift_c[...]
        val[rows, :] = jax.nn.silu(normed).astype(bf16)

    def phase0(p):
        @pl.when(p < START + 8)
        def _():
            activate(p - START)

        @pl.when(p == START + 8)
        def _():
            for k in (1, 3, 2):
                act_copy(k).start()
            acts[y] = val[my_cols, :]

        q = p - START

        @pl.when((q >= 0) & (q < 8))
        def _():
            gate_up(0, q // 2, q % 2)

        @pl.when((q >= 8) & (q < 16))
        def _():
            for s in range(2):
                down(0, q - 8, s)

    def back(k, main):
        block, peer = block_at(k, -1)
        if main:
            src, dst = rm.at[block, pl.ds(0, 32)], bm.at[me, pl.ds(0, 32)]
        else:
            src, dst = rest_out.at[0, block], rest_in.at[0, me]
        return pltpu.make_async_remote_copy(
            src_ref=src, dst_ref=dst, send_sem=sent, recv_sem=r_recv.at[1 - main],
            device_id=peer, device_id_type=MESH,
        )

    low_rows = lax.broadcasted_iota(jnp.int32, (128, 256), 0) % 8 < 4

    def fold(half, block):
        left = slice(block * 256, block * 256 + 256)
        right = slice(1024 + block * 256, 1280 + block * 256)
        if half == 0:
            rows = jnp.where(low_rows, orx[:, left], pltpu.roll(orx[:, right], 4, 0))
        else:
            rows = jnp.where(low_rows, pltpu.roll(orx[:, left], 124, 0), orx[:, right])
        rest_out[half, :, :, left] = rows.reshape(16, 8, 256).astype(bf16)

    def first_leave():
        for k in range(15):
            back(k, 1).start()
        for block in range(4):
            fold(0, block)
        for k in range(15):
            back(k, 0).start()
        bm[me, 0:32] = rm[me, 0:32]
        rest_in[0, me] = rest_out[0, me]

    def conv_part(q):
        at = pl.ds(pl.multiple_of(q * 512, 512), 512)
        total = None
        for b in range(4):
            term = jnp.dot(acts[b], cw[b, :, at], preferred_element_type=f32).astype(bf16).astype(f32)
            total = term if total is None else total + term
        conv_out[:, at] = total.astype(bf16)

    slot0_c, slot1_c = to_column(slot0, tokens), to_column(slot1, tokens)
    group = jax.nn.sigmoid(scores[0:1, :])
    weight0 = to_column(group * jax.nn.sigmoid(scores[1:2, :]), tokens)
    weight1 = to_column(group * jax.nn.sigmoid(-scores[1:2, :]), tokens)

    def chosen_main(slot, half):
        at = lax.broadcasted_iota(jnp.int32, (tokens, 512), 1)
        main = ((at // 32) * 64 + half * 32 + at % 32).astype(f32)
        return jnp.where(main == slot, 1.0, 0.0).astype(bf16)

    def chosen_rest(slot, half, right):
        at = lax.broadcasted_iota(jnp.int32, (tokens, 128), 1)
        name = 1024 + at + 4 * (half - right)
        here = (at % 8 >= 4) == (right > 0)
        return jnp.where(here & (name.astype(f32) == slot), 1.0, 0.0).astype(bf16)

    def rest_rows(half, at):
        return rest_in[half, :, :, at].astype(f32).reshape(128, 256).astype(bf16)

    def weighted(pick0, pick1, rows):
        return weight0 * jnp.dot(pick0, rows, preferred_element_type=f32) + weight1 * jnp.dot(
            pick1, rows, preferred_element_type=f32
        )

    def combine0(block):
        at = slice(block * 256, block * 256 + 256)
        folded = slice(block % 4 * 256, block % 4 * 256 + 256)
        rows = jnp.concatenate([bm[:, 0:32, at].reshape(512, 256), rest_rows(0, folded)], axis=0)
        picks = [
            jnp.concatenate([chosen_main(slot, 0), chosen_rest(slot, 0, block // 4)], axis=1)
            for slot in (slot0_c, slot1_c)
        ]
        sums[:, at] = weighted(picks[0], picks[1], rows)

    def column(k, block, s):
        source, peer = block_at(k, -1)
        at = pl.ds(pl.multiple_of(block * 256, 256), 256)
        rows = pl.ds(32 + s * MAIN, MAIN)
        return pltpu.make_async_remote_copy(
            src_ref=rm.at[source, rows, at], dst_ref=bm.at[me, rows, at], send_sem=sent,
            recv_sem=q_recv.at[block], device_id=peer, device_id_type=MESH,
        )

    def rest_column(k, block):
        source, peer = block_at(k, -1)
        at = pl.ds(block * 256, 256)
        return pltpu.make_async_remote_copy(
            src_ref=rest_out.at[1, source, :, at], dst_ref=rest_in.at[1, me, :, at],
            send_sem=sent, recv_sem=q_recv.at[8 + block], device_id=peer,
            device_id_type=MESH,
        )

    def leave(block, s):
        at = pl.ds(pl.multiple_of(block * 256, 256), 256)
        rows = pl.ds(32 + s * MAIN, MAIN)
        for k in TAIL_ORDER:
            column(k, block, s).start()
        bm[me, rows, at] = rm[me, rows, at]

    def rest_leave(block):
        fold(1, block)
        for k in TAIL_ORDER:
            rest_column(k, block).start()
        at = slice(block * 256, block * 256 + 256)
        rest_in[1, me, :, at] = rest_out[1, me, :, at]

    def phases(p, carry):
        step(p)
        phase0(p)

        @pl.when(p == MIDDLE)
        def _():
            first_leave()

        @pl.when(p == MIDDLE + 10)
        def _():
            arrived(cw.at[pl.ds(0, 3), pl.ds(0, 128)], cw_sem)
            for k in (1, 3, 2):
                cs_copy(k).start()

        @pl.when(p == MIDDLE + 18)
        def _():
            arrived(acts.at[pl.ds(0, 3)], act_sem)
            arrived(cw.at[pl.ds(0, 3), pl.ds(0, 128)], cs_sem)

        @pl.when((p >= MIDDLE + 18) & (p < MIDDLE + 22))
        def _():
            conv_part(p - MIDDLE - 18)

        there = []
        for s in range(2):
            handed = jnp.where(c == s, HOP * dist, HOP * (4 - dist) + SHARE)
            lag = jnp.where(dist == 0, -AHEAD, handed)

            def pieces(p, lag=lag):
                return jnp.minimum(2 * (p - MIDDLE), p - lag - CHUNKS + 1)

            old, new = pieces(p - 1), pieces(p)

            @pl.when((new >= 8) & (new < 34) & (new // 8 != old // 8))
            def _(s=s, new=new):
                gate_up(1, new // 8 - 1, s)

            @pl.when((new >= 34) & (new < 50) & (new // 2 != old // 2))
            def _(s=s, new=new):
                block = (new - 34) // 2
                down(1, block, s)
                leave(block, s)

            there.append((old, new))

        old, new = [jnp.minimum(there[0][i], there[1][i]) for i in range(2)]
        for block in range(4):
            due = 42 + 2 * block

            @pl.when((old < due) & (new >= due))
            def _(block=block):
                rest_leave(block)

        return carry

    with jax.named_scope("s_phase1"):
        lax.fori_loop(START, LAST, phases, 0)

    with jax.named_scope("s_combine0"):
        arrived(bm.at[pl.ds(0, 15), pl.ds(0, 32)], r_recv.at[0])
        arrived(rest_in.at[0, pl.ds(0, 15)], r_recv.at[1])
        for block in range(8):
            combine0(block)

    with jax.named_scope("s_combine1"):
        pick0, pick1 = chosen_main(slot0_c, 1), chosen_main(slot1_c, 1)
        picks = [[chosen_rest(slot, 1, right) for slot in (slot0_c, slot1_c)] for right in range(2)]
        for block in range(8):
            at = slice(block * 256, block * 256 + 256)
            arrived(bm.at[pl.ds(0, 15), pl.ds(32, 32), pl.ds(block * 256, 256)], q_recv.at[block])
            sums[:, at] += weighted(pick0, pick1, bm[:, 32:64, at].reshape(512, 256))
            if block >= 4:
                low = block * 256 - 1024
                arrived(rest_in.at[1, pl.ds(0, 15), :, pl.ds(low, 256)], q_recv.at[4 + block])
                rows = rest_rows(1, slice(low, low + 256))
                for right in range(2):
                    at = slice(low + right * 1024, low + right * 1024 + 256)
                    last = weighted(picks[right][0], picks[right][1], rows)
                    out[:, at] = (sums[:, at] + last).astype(bf16)

    with jax.named_scope("s_sent"):
        halo.wait_send()
        arrived(stat.at[pl.ds(0, 3)], sent)
        arrived(acts.at[pl.ds(0, 3)], sent)
        arrived(cw.at[pl.ds(0, 3), pl.ds(0, 128)], sent)
        arrived(cw.at[pl.ds(0, 3), pl.ds(0, 128)], sent)
        arrived(sm.at[pl.ds(0, 15)], sent)
        arrived(sr.at[pl.ds(0, 15)], sent)
        arrived(bm.at[pl.ds(0, 15), pl.ds(0, 32)], sent)
        arrived(rest_in.at[0, pl.ds(0, 15)], sent)
        arrived(bm.at[pl.ds(0, 15), pl.ds(32, 32)], sent)
        arrived(rest_in.at[1, pl.ds(0, 15)], sent)

        @pl.when(dist < 3)
        def _():
            arrived(w.at[0], ring_sent)

        @pl.when(dist == 3)
        def _():
            arrived(w.at[0, 0], ring_sent)

        arrived(w.at[0], sib_sent)


def write_out(conv_ref, moe_ref, conv_out, moe_out, sems):
    copies = []
    for source, target in ((moe_ref, moe_out), (conv_ref, conv_out)):
        for low in range(0, source.shape[0], OUT_ROWS):
            rows = pl.ds(low, OUT_ROWS)
            copies.append(
                pltpu.make_async_copy(source.at[rows], target.at[rows], sems.at[len(copies)])
            )
            copies[-1].start()
    for copy in copies:
        copy.wait()


def on_device(
    conv_value,
    conv_gate,
    depth_weight,
    norm_gain,
    norm_shift,
    conv_out_weight,
    moe_input,
    moe_gain,
    route_experts,
    route_scores,
    expert_gate,
    expert_up,
    expert_down,
):
    bf16, f32 = jnp.bfloat16, jnp.float32
    rows, width = moe_input.shape
    span, channels = conv_value.shape
    hbm = pl.BlockSpec(memory_space=pl.ANY)
    vmem = pl.BlockSpec(memory_space=pltpu.VMEM)
    dma = pltpu.SemaphoreType.DMA
    both = pl.pallas_call(
        kernel,
        out_shape=(
            pltpu.VMEM((span // NY, width), bf16),
            pltpu.VMEM((rows, width), bf16),
        ),
        in_specs=[hbm] * 13,
        out_specs=(vmem, vmem),
        scratch_shapes=[
            pltpu.VMEM((2, 2, CHUNKS * PIECE, 256), bf16),
            pltpu.VMEM((rows, width), bf16),
            pltpu.VMEM((16, 64, width), bf16),
            pltpu.VMEM((16, 8, width), bf16),
            pltpu.VMEM((16, 64, width), bf16),
            pltpu.VMEM((16, 8, width), bf16),
            pltpu.VMEM((16, 64, width), bf16),
            pltpu.VMEM((2, 16, 8, width // 2), bf16),
            pltpu.VMEM((2, 16, 8, width // 2), bf16),
            pltpu.VMEM((2, 384, 1024), f32),
            pltpu.VMEM((rows, width), f32),
            pltpu.VMEM((2, 384, 512), bf16),
            pltpu.VMEM((128, width), bf16),
            pltpu.VMEM((128, width), f32),
            pltpu.VMEM((span, channels), bf16),
            pltpu.VMEM((span, channels), bf16),
            pltpu.VMEM((KERNEL, channels), f32),
            pltpu.VMEM((1, channels), f32),
            pltpu.VMEM((1, channels), f32),
            pltpu.VMEM((1, width), f32),
            pltpu.VMEM((2, rows), jnp.int32),
            pltpu.VMEM((2, rows), f32),
            pltpu.VMEM((HALO + span, channels), f32),
            pltpu.VMEM((NY, span // NY, channels), bf16),
            pltpu.VMEM((NY, channels, width), bf16),
            pltpu.VMEM((128 + HALO, channels), f32),
            pltpu.VMEM((HALO, channels), bf16),
            pltpu.VMEM((HALO, channels), bf16),
            pltpu.VMEM((NY, 16, 128), f32),
            pltpu.VMEM((16, 128), f32),
            dma((5,)),
            dma((3,)),
            dma((TOTAL,)),
            dma((24,)),
            dma,
            dma,
            dma,
            dma((2,)),
            dma((2,)),
            dma((12,)),
            dma,
            dma,
            dma,
            dma,
            dma,
        ],
        compiler_params=pltpu.CompilerParams(
            collective_id=0, has_side_effects=True, vmem_limit_bytes=64_300_000
        ),
        name="both",
    )(
        conv_value,
        conv_gate,
        depth_weight,
        norm_gain.reshape(1, CONV),
        norm_shift.reshape(1, CONV),
        conv_out_weight,
        moe_input,
        moe_gain.reshape(1, width),
        route_experts.T,
        route_scores.T,
        expert_gate,
        expert_up,
        expert_down,
    )
    outs = [jax.ShapeDtypeStruct(out.shape, out.dtype) for out in both]
    return pl.pallas_call(
        write_out,
        out_shape=tuple(outs),
        in_specs=[vmem, vmem],
        out_specs=(hbm, hbm),
        scratch_shapes=[dma((sum(out.shape[0] for out in outs) // OUT_ROWS,))],
        name="write_out",
    )(*(pltpu.with_memory_space_constraint(out, pltpu.VMEM) for out in both))


def solution(mesh):
    in_specs = (
        P("ep", "tp"),
        P("ep", "tp"),
        P(),
        P(),
        P(),
        P("tp", None),
        P(("ep", "tp"), None),
        P(),
        P(("ep", "tp"), None),
        P(("ep", "tp"), None),
        P("ep", None, None),
        P("ep", None, None),
        P("ep", None, None),
    )
    out_specs = (P(("ep", "tp"), None), P(("ep", "tp"), None))
    return jax.shard_map(
        on_device, mesh=mesh, in_specs=in_specs, out_specs=out_specs, check_vma=False
    )
```
